32 devices in a mesh: sp: 8 (over z, core), tp: 4 (over y, x).
Axes of the slice: x: 2, y: 2, z: 4, core: 2. Of those that a mesh axis runs over, the one named last changes fastest.
Arguments:
- queries: bfloat16 [1024, 4096], P('sp', 'tp'), may hold values from -6 to 6
- keys: bfloat16 [1024, 4096], P('sp', 'tp'), may hold values from -6 to 6
- values: bfloat16 [1024, 8192], P('sp', 'tp'), may hold values from -6 to 6
- output_gate_logits: bfloat16 [1024, 8192], P('sp', 'tp'), may hold values from -6 to 6
- input_gate_log: float32 [1024, 16], P('sp', 'tp'), may hold values from -6 to 130
- forget_gate_logits: float32 [1024, 16], P('sp', 'tp'), may hold values from -3 to 20
- extra_log_decay: float32 [1024, 16], P('sp', 'tp'), may hold values from -0.7 to 0
- cell_output_weight: bfloat16 [8192, 4096], P('tp', 'sp'), may hold values from -0.0625 to 0.0625
- residual_input: bfloat16 [1024, 4096], P(('sp', 'tp')), may hold values from -6 to 6
- cell_norm_gain: float32 [4096], replicated, may hold values from 0.1 to 1.9
- expert_before_gain: float32 [4096], replicated, may hold values from 0.1 to 1.9
- expert_after_gain: float32 [4096], replicated, may hold values from 0.1 to 1.9
- routes: int32 [1024, 4], P('sp'), may hold values from 0 to 7, all different within a row; in each aligned block of 128 rows (0 to 127, 128 to 255, ...) at most 80 rows name the same one
- chosen_expert_weight: float32 [1024, 4], P('sp'), may hold values from 0.1 to 1
- expert_gate_weight: bfloat16 [8, 4096, 2048], P('sp', None, 'tp'), may hold values from -0.09375 to 0.09375
- expert_up_weight: bfloat16 [8, 4096, 2048], P('sp', None, 'tp'), may hold values from -0.09375 to 0.09375
- expert_down_weight: bfloat16 [8, 2048, 4096], P('sp', None, 'tp'), may hold values from -0.125 to 0.125
Outputs:
- result: bfloat16 [1024, 4096], P(('sp', 'tp'))
The draws below stay inside these ranges and needn't reach their ends.
Inputs may be any that keep to these rules, and one draw needn't show every extreme that they name: `routes`: within the rows of one index of sp (aligned blocks of 128 positions) no expert is named by more than 80 positions, a bound that some block reaches; a position names 4 different experts.
All inputs are finite; a program needn't handle non-finite values.
Results may differ from the reference program's by a relative error of at most 0.019.
Values may be sent and summed in bfloat16 or wider, within the bound.
No kernel may reach another device: no remote copies, remote signals or barrier semaphores. Data moves between devices by JAX's collectives and lax.ppermute only.
A program may use at most 128 MiB of HBM per device.

```python
import math
import jax
import jax.numpy as jnp
import numpy as np
from jax import lax

D = 4096
CELL_HEADS = 16
DQK = 256
DV = 512
FE = 2048
TOP = 4
BLOCK = 128
SEG = 128
SEQUENCE_TOKENS = 1024
HV = 8192
EXPERTS = 8
CAP = 80
N_SP = 8
N_TP = 4


def draw_input_gate_log(key, part):
    normal_draw = jnp.clip(jax.random.normal(key, (SEQUENCE_TOKENS, CELL_HEADS), jnp.float32), -6.0, 6.0)
    return normal_draw


def draw_forget_gate_logits(key, part):
    ranking = jax.random.permutation(jax.random.fold_in(key, 1), CELL_HEADS)
    is_fast = ranking < CELL_HEADS // 2
    slow_level = jnp.log(jnp.float32(SEQUENCE_TOKENS) / 0.4)
    fast_level = jax.random.uniform(jax.random.fold_in(key, 2), (CELL_HEADS,), jnp.float32, 3.2, 4.2)
    level_base = jnp.where(is_fast, fast_level, slow_level)
    block_shift = jax.random.uniform(jax.random.fold_in(key, 3), (SEQUENCE_TOKENS // BLOCK, CELL_HEADS), jnp.float32, -0.7, 0.7)
    block_shift = jnp.repeat(block_shift, BLOCK, axis=0)
    jitter = 0.6 * jnp.clip(jax.random.normal(jax.random.fold_in(key, 4), (SEQUENCE_TOKENS, CELL_HEADS), jnp.float32), -4.0, 4.0)
    return level_base[None, :] + block_shift + jitter


def draw_extra_log_decay(key, part):
    spike_position = jax.random.randint(jax.random.fold_in(key, 1), (3, CELL_HEADS), 0, SEQUENCE_TOKENS)
    loss_history = jax.random.uniform(jax.random.fold_in(key, 2), (3, CELL_HEADS), jnp.float32, -0.69, -0.22)
    token_position = lax.broadcasted_iota(jnp.int32, (SEQUENCE_TOKENS, CELL_HEADS), 0)
    spike_list = jnp.zeros((SEQUENCE_TOKENS, CELL_HEADS), jnp.float32)
    for spike_index in range(3):
        spike_list = spike_list + jnp.where(token_position == spike_position[spike_index][None, :], loss_history[spike_index][None, :], 0.0)
    return jnp.maximum(spike_list, -0.7)


def shard_levels(rng, dims, cuts, least, high):
    def one(axis_at, blocks):
        draws = jax.random.uniform(jax.random.fold_in(jax.random.fold_in(rng, 6), axis_at), (blocks,), jnp.float32, least / len(cuts), high / len(cuts))
        return jnp.repeat(jnp.exp(draws), dims[axis_at] // blocks).reshape((-1,) + (1,) * (len(dims) - axis_at - 1))

    factor_of = one(*cuts[0])
    for cut in cuts[1:]:
        factor_of = factor_of * one(*cut)
    return factor_of


def shared_out(own_key, own, number, rows, amount, top, bound, skew):
    order = jax.random.permutation(own_key, amount)
    packed, ordinary = portions_of(amount, rows * top, bound, skew, True), portions_of(amount, rows * top, bound, skew, False)
    places = jnp.arange(amount)

    def named(tallies, turn):
        used = int((tallies > 0).sum())
        fixed = max(1, used // 4)
        shifted = fixed + (places - fixed + turn * (used - fixed)) % max(1, amount - fixed)
        return jnp.zeros((amount,), jnp.int32).at[order[jnp.where(places < fixed, places, shifted)]].set(jnp.asarray(tallies, jnp.int32))

    tallies = jnp.where(number % 4 == 0, named(packed, number // 4), named(ordinary, number - number // 4 - 1))
    mixed = jax.random.permutation(jax.random.fold_in(own, 3), amount)
    source_of, receiver = mixed[0:amount // 2 * 2:2], mixed[1:amount // 2 * 2:2]
    margin = jnp.minimum(tallies[source_of] - 1, bound - tallies[receiver]) // 2
    margin = jnp.where((source_of == order[0]) | (receiver == order[0]) | (tallies[receiver] == 0), 0, jnp.maximum(margin, 0))
    shifted = jax.random.randint(jax.random.fold_in(own, 4), (amount // 2,), 0, 1 << 20) % (margin + 1)
    tallies = tallies.at[source_of].add(-shifted).at[receiver].add(shifted)
    items = jnp.searchsorted(jnp.cumsum(tallies), jnp.arange(rows * top), side="right").astype(jnp.int32)
    grid = items.reshape(top, rows).T
    grid = grid[jax.random.permutation(jax.random.fold_in(own, 1), rows)]
    turn = jax.random.randint(jax.random.fold_in(own, 2), (rows, 1), 0, top)
    return jnp.take_along_axis(grid, (jnp.arange(top)[None, :] + turn) % top, axis=1)


def portions_of(amount, total, bound, skew, full):
    weights = [(1 << 20) // math.isqrt(standing ** skew) + 1 for standing in range(1, amount + 1)]
    largest = bound if full else min(bound, max(-(-total // amount), total * weights[0] // sum(weights)))
    least = 1 if total - largest >= amount - 1 else 0
    counts, spare = [largest] + [least] * (amount - 1), total - largest - least * (amount - 1)
    while spare > 0:
        candidates = [i for i in range(1, amount) if counts[i] < largest] or [i for i in range(1, amount) if counts[i] < bound]
        whole, remaining = sum([weights[i] for i in candidates]), spare
        for i in candidates:
            extra = min(bound - counts[i], max(1, remaining * weights[i] // whole), spare)
            counts[i] = counts[i] + extra
            spare = spare - extra
    return np.array(counts)


def noise(key, shape, spread, limit, split=(), held_as=jnp.bfloat16):
    entries = spread * jax.random.normal(key, shape, jnp.float32)
    if split:
        entries = entries * shard_levels(key, shape, split, -0.22, 0.18)
    return jnp.clip(entries, -limit, limit).astype(held_as)


def setup_inputs(seed: int = 0) -> dict:
    seeds = jax.random.split(jax.random.key(seed), 18)
    queries = noise(seeds[0], (SEQUENCE_TOKENS, CELL_HEADS * DQK), 1.0, 6.0, ((0, 8), (1, 4)))
    keys = noise(seeds[1], (SEQUENCE_TOKENS, CELL_HEADS * DQK), 1.0, 6.0, ((0, 8), (1, 4)))
    values = noise(seeds[2], (SEQUENCE_TOKENS, HV), 1.0, 6.0, ((0, 8), (1, 4)))
    output_gate_logits = noise(seeds[3], (SEQUENCE_TOKENS, HV), 1.0, 6.0, ((0, 8), (1, 4)))
    input_gate_log = draw_input_gate_log(jax.random.fold_in(seeds[17], 71), 0)
    forget_gate_logits = draw_forget_gate_logits(jax.random.fold_in(seeds[17], 71), 0)
    extra_log_decay = draw_extra_log_decay(jax.random.fold_in(seeds[17], 71), 0)
    cell_output_weight = noise(seeds[7], (HV, D), HV ** -0.5, 0.0625, ((0, 4), (1, 8)))
    residual_input = noise(seeds[8], (SEQUENCE_TOKENS, D), 1.0, 6.0, ((0, 32),))
    cell_norm_gain = jnp.clip(1.0 + 0.18 * jax.random.normal(seeds[9], (D,), jnp.float32), 0.1, 1.9)
    expert_before_gain = jnp.clip(1.0 + 0.18 * jax.random.normal(seeds[10], (D,), jnp.float32), 0.1, 1.9)
    expert_after_gain = jnp.clip(1.0 + 0.18 * jax.random.normal(seeds[11], (D,), jnp.float32), 0.1, 1.9)
    routes_keys = jax.random.split(jax.random.fold_in(seeds[12], 1), SEQUENCE_TOKENS // SEG)
    routes_turns = jax.random.permutation(jax.random.fold_in(seeds[12], 3), SEQUENCE_TOKENS // SEG)
    routes = jax.vmap(lambda own, number: shared_out(jax.random.fold_in(seeds[12], 2), own, number, SEG, EXPERTS, TOP, CAP, 2))(routes_keys, routes_turns).reshape((SEQUENCE_TOKENS, TOP))
    chosen_expert_weight = jnp.clip(0.1 + 0.9 * jax.random.uniform(seeds[13], (SEQUENCE_TOKENS, TOP), jnp.float32) ** shard_levels(seeds[13], (SEQUENCE_TOKENS, TOP), ((0, 8),), -0.2, 0.2), 0.1, 1.0)
    expert_gate_weight = noise(seeds[14], (EXPERTS, D, FE), D ** -0.5, 0.09375, ((0, 8), (2, 4)))
    expert_up_weight = noise(seeds[15], (EXPERTS, D, FE), D ** -0.5, 0.09375, ((0, 8), (2, 4)))
    expert_down_weight = noise(seeds[16], (EXPERTS, FE, D), FE ** -0.5, 0.125, ((0, 8), (2, 4)))
    return {"queries": queries, "keys": keys, "values": values, "output_gate_logits": output_gate_logits, "input_gate_log": input_gate_log, "forget_gate_logits": forget_gate_logits, "extra_log_decay": extra_log_decay, "cell_output_weight": cell_output_weight, "residual_input": residual_input, "cell_norm_gain": cell_norm_gain, "expert_before_gain": expert_before_gain, "expert_after_gain": expert_after_gain, "routes": routes, "chosen_expert_weight": chosen_expert_weight, "expert_gate_weight": expert_gate_weight, "expert_up_weight": expert_up_weight, "expert_down_weight": expert_down_weight}


norm_eps = 1e-06
den_floor = 8.0

def rms_scale(inputs, gain):
    return inputs * lax.rsqrt(lax.optimization_barrier(jnp.mean(inputs * inputs, axis=-1, keepdims=True)) + norm_eps) * gain

def block_local(query_blk, key_blk, value_blk, gate_blk, forget_blk):
    key_scale = DQK ** (-0.5)
    running = jnp.cumsum(forget_blk, axis=-1)
    length = running.shape[-1]
    lower = lax.broadcasted_iota(jnp.int32, (length, length), 0) >= lax.broadcasted_iota(jnp.int32, (length, length), 1)
    offsets = jnp.where(lower, running[:, :, None] - running[:, None, :] + gate_blk[:, None, :], -jnp.inf)
    local_top = lax.optimization_barrier(jnp.max(offsets, axis=-1))
    scores = jnp.einsum('htd,hsd->hts', query_blk.astype(jnp.float32), key_blk.astype(jnp.float32), precision=lax.Precision.HIGHEST) * key_scale
    weights = scores * jnp.exp(offsets - local_top[:, :, None])
    rounded = lax.optimization_barrier(weights.astype(jnp.bfloat16))
    numerator = jnp.einsum('hts,hsv->htv', rounded.astype(jnp.float32), value_blk.astype(jnp.float32), precision=lax.Precision.HIGHEST)
    denominator = lax.optimization_barrier(jnp.sum(weights, axis=-1))
    return (running, local_top, numerator, denominator)

def read_out(query_blk, memory, running, local_top, numerator, denominator):
    matrix, vector, peak = memory
    query_wide = query_blk.astype(jnp.float32)
    carried = running + peak[:, None]
    highest = jnp.maximum(local_top, carried)
    inner_w = jnp.exp(local_top - highest)
    carried_w = jnp.exp(carried - highest)
    numer_all = inner_w[:, :, None] * numerator + carried_w[:, :, None] * jnp.einsum('htd,hdv->htv', query_wide, matrix, precision=lax.Precision.HIGHEST)
    denom_all = inner_w * denominator + carried_w * jnp.einsum('htd,hd->ht', query_wide, vector, precision=lax.Precision.HIGHEST)
    return numer_all / jnp.maximum(jnp.abs(denom_all), den_floor)[:, :, None]

def advance(memory, key_blk, value_blk, gate_blk, running):
    matrix, vector, peak = memory
    key_wide = key_blk.astype(jnp.float32) * DQK ** (-0.5)
    block_sum = running[:, -1]
    growth = block_sum[:, None] - running + gate_blk
    peak_new = jnp.maximum(block_sum + peak, lax.optimization_barrier(jnp.max(growth, axis=-1)))
    fading = jnp.exp(block_sum + peak - peak_new)
    writes = jnp.exp(growth - peak_new[:, None])
    weighted = lax.optimization_barrier((key_wide * writes[:, :, None]).astype(jnp.bfloat16))
    matrix_new = fading[:, None, None] * matrix + jnp.einsum('hsd,hsv->hdv', weighted.astype(jnp.float32), value_blk.astype(jnp.float32), precision=lax.Precision.HIGHEST)
    vector_new = fading[:, None] * vector + jnp.einsum('hs,hsd->hd', writes, key_wide, precision=lax.Precision.HIGHEST)
    return (matrix_new, vector_new, peak_new)

def reference(queries, keys, values, output_gate_logits, input_gate_log, forget_gate_logits, extra_log_decay, cell_output_weight, residual_input, cell_norm_gain, expert_before_gain, expert_after_gain, routes, chosen_expert_weight, expert_gate_weight, expert_up_weight, expert_down_weight):
    block_count = SEQUENCE_TOKENS // BLOCK

    def split_heads(array, width):
        return array.reshape(block_count, BLOCK, CELL_HEADS, width).transpose(0, 2, 1, 3)
    query_blocks = split_heads(queries, DQK)
    key_blocks = split_heads(keys, DQK)
    value_blocks = split_heads(values, DV)
    forget_log_value = jax.nn.log_sigmoid(forget_gate_logits) + extra_log_decay
    gate_blocks = input_gate_log.reshape(block_count, BLOCK, CELL_HEADS).transpose(0, 2, 1)
    forget_blocks = forget_log_value.reshape(block_count, BLOCK, CELL_HEADS).transpose(0, 2, 1)

    def step(memory, inputs):
        query_blk, key_blk, value_blk, gate_blk, forget_blk = inputs
        running, local_top, numerator, denominator = block_local(query_blk, key_blk, value_blk, gate_blk, forget_blk)
        outcome = read_out(query_blk, memory, running, local_top, numerator, denominator)
        return (advance(memory, key_blk, value_blk, gate_blk, running), outcome)
    start_state = (jnp.zeros((CELL_HEADS, DQK, DV), jnp.float32), jnp.zeros((CELL_HEADS, DQK), jnp.float32), jnp.zeros((CELL_HEADS,), jnp.float32))
    unused, heads_out = lax.scan(step, start_state, (query_blocks, key_blocks, value_blocks, gate_blocks, forget_blocks))
    cell_out = heads_out.transpose(0, 2, 1, 3).reshape(SEQUENCE_TOKENS, HV)
    gated = (cell_out * jax.nn.sigmoid(output_gate_logits.astype(jnp.float32))).astype(jnp.bfloat16)
    group_width = HV // N_TP

    def group_sum(accum_sum, group_idx):
        partial_value = lax.dynamic_slice_in_dim(gated, group_idx * group_width, group_width, 1)
        weight_rows = lax.dynamic_slice_in_dim(cell_output_weight, group_idx * group_width, group_width, 0)
        product = jnp.dot(partial_value, weight_rows, preferred_element_type=jnp.float32).astype(jnp.bfloat16)
        product = lax.optimization_barrier(product)
        return (accum_sum + product.astype(jnp.float32), None)
    mixed, unused = lax.scan(group_sum, jnp.zeros((SEQUENCE_TOKENS, D), jnp.float32), jnp.arange(N_TP, dtype=jnp.int32))
    stream = (residual_input.astype(jnp.float32) + rms_scale(mixed, cell_norm_gain)).astype(jnp.bfloat16)
    normed = rms_scale(stream.astype(jnp.float32), expert_before_gain).astype(jnp.bfloat16)
    most_rows = N_SP * CAP

    def expert_step(accum_sum, expert_idx):
        weight_gate = lax.dynamic_index_in_dim(expert_gate_weight, expert_idx, 0, keepdims=False)
        weight_up = lax.dynamic_index_in_dim(expert_up_weight, expert_idx, 0, keepdims=False)
        weight_down = lax.dynamic_index_in_dim(expert_down_weight, expert_idx, 0, keepdims=False)
        chosen = routes == expert_idx
        picked = jnp.any(chosen, axis=1)
        positions = jnp.nonzero(picked, size=most_rows, fill_value=0)[0].astype(jnp.int32)
        filled = (jnp.arange(most_rows, dtype=jnp.int32) < jnp.sum(picked.astype(jnp.int32))).astype(jnp.float32)
        rows_in = normed[positions]
        gate_proj = jnp.dot(rows_in, weight_gate, preferred_element_type=jnp.float32)
        up_proj = jnp.dot(rows_in, weight_up, preferred_element_type=jnp.float32)
        hidden = lax.optimization_barrier((jax.nn.silu(gate_proj) * up_proj).astype(jnp.bfloat16))
        expert_out = jnp.dot(hidden, weight_down, preferred_element_type=jnp.float32).astype(jnp.bfloat16)
        expert_out = lax.optimization_barrier(expert_out)
        weight = lax.optimization_barrier(jnp.sum(jnp.where(chosen, chosen_expert_weight, jnp.float32(0.0)), axis=1))[positions] * filled
        return (accum_sum.at[positions].add(expert_out.astype(jnp.float32) * weight[:, None]), None)
    routed_sum, unused = lax.scan(expert_step, jnp.zeros((SEQUENCE_TOKENS, D), jnp.float32), jnp.arange(EXPERTS, dtype=jnp.int32))
    moe = lax.optimization_barrier(routed_sum.astype(jnp.bfloat16))
    return (stream.astype(jnp.float32) + rms_scale(moe.astype(jnp.float32), expert_after_gain)).astype(jnp.bfloat16)
```

```python
import jax
import jax.numpy as jnp
from jax import lax
from jax.experimental import pallas as pl
from jax.experimental.pallas import tpu as pltpu
from jax.sharding import PartitionSpec as P

DQK = 256
DV = 512
BLOCK = 128


norm_eps = 1e-06
very_low = -1e30
den_floor = 8.0


def carried_in(part, axis, combine, identity):
    place = lax.axis_index(axis)
    gathered = jax.tree.map(lambda a: lax.all_gather(a, axis), part)
    state = jax.tree.map(lambda a, e: jnp.zeros_like(a) + jnp.asarray(e, a.dtype), part, identity)

    def one(step, state):
        return combine(
            state, jax.tree.map(lambda a: lax.dynamic_index_in_dim(a, step, 0, False), gathered)
        )

    return lax.fori_loop(0, place, one, state)


def rms_scale(inputs, gain):
    return inputs * lax.rsqrt(jnp.mean(inputs * inputs, axis=-1, keepdims=True) + norm_eps) * gain


def combine_states(earlier, later):
    total_early, matrix_early, vector_early, peak_early = earlier
    total_late, matrix_late, vector_late, peak_late = later
    shifted = total_late + peak_early
    peak = jnp.maximum(shifted, peak_late)
    keep_early = jnp.exp(shifted - peak)
    keep_late = jnp.exp(peak_late - peak)
    return (
        total_early + total_late,
        keep_early[:, None, None] * matrix_early + keep_late[:, None, None] * matrix_late,
        keep_early[:, None] * vector_early + keep_late[:, None] * vector_late,
        peak,
    )


def block_local(query_blk, key_blk, value_blk, gate_blk, forget_blk):
    key_scale = DQK ** (-0.5)
    running = jnp.cumsum(forget_blk, axis=-1)
    length = running.shape[-1]
    lower = lax.broadcasted_iota(jnp.int32, (length, length), 0) >= lax.broadcasted_iota(
        jnp.int32, (length, length), 1
    )
    offsets = jnp.where(
        lower, running[:, :, None] - running[:, None, :] + gate_blk[:, None, :], -jnp.inf
    )
    local_top = jnp.max(offsets, axis=-1)
    scores = (
        jnp.einsum("htd,hsd->hts", query_blk, key_blk, preferred_element_type=jnp.float32)
        * key_scale
    )
    weights = scores * jnp.exp(offsets - local_top[:, :, None])
    numerator = jnp.einsum(
        "hts,hsv->htv", weights.astype(jnp.bfloat16), value_blk, preferred_element_type=jnp.float32
    )
    denominator = jnp.sum(weights, axis=-1)
    return (running, local_top, numerator, denominator)


def read_out(query_blk, memory, running, local_top, numerator, denominator):
    matrix, vector, peak = memory
    query_wide = query_blk.astype(jnp.float32)
    carried = running + peak[:, None]
    highest = jnp.maximum(local_top, carried)
    inner_w = jnp.exp(local_top - highest)
    carried_w = jnp.exp(carried - highest)
    numer_all = inner_w[:, :, None] * numerator + carried_w[:, :, None] * jnp.einsum(
        "htd,hdv->htv", query_wide, matrix, precision=lax.Precision.HIGHEST
    )
    denom_all = inner_w * denominator + carried_w * jnp.einsum(
        "htd,hd->ht", query_wide, vector, precision=lax.Precision.HIGHEST
    )
    return numer_all / jnp.maximum(jnp.abs(denom_all), den_floor)[:, :, None]


def advance(memory, key_blk, value_blk, gate_blk, running):
    matrix, vector, peak = memory
    key_wide = key_blk.astype(jnp.float32) * DQK ** (-0.5)
    block_sum = running[:, -1]
    growth = block_sum[:, None] - running + gate_blk
    peak_new = jnp.maximum(block_sum + peak, jnp.max(growth, axis=-1))
    fading = jnp.exp(block_sum + peak - peak_new)
    writes = jnp.exp(growth - peak_new[:, None])
    weighted = (key_wide * writes[:, :, None]).astype(jnp.bfloat16)
    matrix_new = fading[:, None, None] * matrix + jnp.einsum(
        "hsd,hsv->hdv", weighted, value_blk, preferred_element_type=jnp.float32
    )
    vector_new = fading[:, None] * vector + jnp.einsum(
        "hs,hsd->hd", writes, key_wide, precision=lax.Precision.HIGHEST
    )
    return (matrix_new, vector_new, peak_new)


def by_states(
    queries,
    keys,
    values,
    output_gate_logits,
    input_gate_log,
    forget_gate_logits,
    extra_log_decay,
    cell_output_weight,
    residual_input,
    cell_norm_gain,
    expert_before_gain,
    expert_after_gain,
    routes,
    chosen_expert_weight,
    expert_gate_weight,
    expert_up_weight,
    expert_down_weight,
):
    segment = queries.shape[0]
    head_count = queries.shape[1] // DQK
    block_count = segment // BLOCK

    def split_heads(array, width):
        return array.reshape(block_count, BLOCK, head_count, width).transpose(0, 2, 1, 3)

    query_blocks = split_heads(queries, DQK)
    key_blocks = split_heads(keys, DQK)
    value_blocks = split_heads(values, DV)
    forget_log_value = jax.nn.log_sigmoid(forget_gate_logits) + extra_log_decay
    gate_blocks = input_gate_log.reshape(block_count, BLOCK, head_count).transpose(0, 2, 1)
    forget_blocks = forget_log_value.reshape(block_count, BLOCK, head_count).transpose(0, 2, 1)
    totals = jnp.sum(forget_log_value, axis=0)
    zero_matrix = jnp.zeros((head_count, DQK, DV), jnp.float32)
    zero_vector = jnp.zeros((head_count, DQK), jnp.float32)
    zero_heads = jnp.zeros((head_count,), jnp.float32)
    fresh = (zero_matrix, zero_vector, jnp.full((head_count,), very_low, jnp.float32))
    empty = (zero_heads,) + fresh
    anchor = (zero_heads, zero_matrix, zero_vector, zero_heads)

    def summarize(memory, inputs):
        key_blk, value_blk, gate_blk, forget_blk = inputs
        return (
            advance(memory, key_blk, value_blk, gate_blk, jnp.cumsum(forget_blk, axis=-1)),
            None,
        )

    own_state, unused = lax.scan(
        summarize, fresh, (key_blocks, value_blocks, gate_blocks, forget_blocks)
    )
    prefix = carried_in((totals,) + own_state, "sp", combine_states, empty)
    start_full = combine_states(anchor, prefix)

    def emit(memory, inputs):
        query_blk, key_blk, value_blk, gate_blk, forget_blk = inputs
        running, local_top, numerator, denominator = block_local(
            query_blk, key_blk, value_blk, gate_blk, forget_blk
        )
        outcome = read_out(query_blk, memory, running, local_top, numerator, denominator)
        return (advance(memory, key_blk, value_blk, gate_blk, running), outcome)

    unused, heads_out = lax.scan(
        emit, start_full[1:], (query_blocks, key_blocks, value_blocks, gate_blocks, forget_blocks)
    )
    cell_out = heads_out.transpose(0, 2, 1, 3).reshape(segment, head_count * DV)
    gated = (cell_out * jax.nn.sigmoid(output_gate_logits.astype(jnp.float32))).astype(jnp.bfloat16)
    whole_weight = lax.all_gather(cell_output_weight, "sp", axis=1, tiled=True)
    mixed = lax.psum_scatter(
        jnp.dot(gated, whole_weight, preferred_element_type=jnp.float32).astype(jnp.bfloat16),
        "tp",
        scatter_dimension=0,
        tiled=True,
    ).astype(jnp.float32)
    stream = (residual_input.astype(jnp.float32) + rms_scale(mixed, cell_norm_gain)).astype(
        jnp.bfloat16
    )
    normed = rms_scale(stream.astype(jnp.float32), expert_before_gain).astype(jnp.bfloat16)
    normed_all = lax.all_gather(normed, "tp", axis=0, tiled=True)
    sources = lax.axis_size("sp")
    top_count = routes.shape[1]
    capacity = max(2, min(segment, 5 * segment * top_count // (4 * sources)))
    width = normed_all.shape[1]
    labels = lax.broadcasted_iota(jnp.int32, (1, 1, sources), 2)
    matches = (routes[:, :, None] == labels).astype(jnp.int32)
    per_row = jnp.sum(matches, axis=1)
    before_rows = jnp.cumsum(per_row, axis=0) - per_row
    places = jnp.sum(matches * before_rows[:, None, :], axis=2)
    slot_of = routes * capacity + places
    slot_ids = lax.broadcasted_iota(jnp.int32, (sources * capacity, 1, 1), 0)
    picker = jnp.sum((slot_of[None, :, :] == slot_ids).astype(jnp.int32), axis=2).astype(
        jnp.bfloat16
    )
    buffer = jnp.dot(picker, normed_all, preferred_element_type=jnp.float32).astype(jnp.bfloat16)
    buffer = buffer.reshape(sources, capacity, width)
    arrived = lax.all_to_all(buffer, "sp", split_axis=0, concat_axis=0, tiled=True)
    flattened = arrived.reshape(-1, width)
    gate_proj = jnp.dot(flattened, expert_gate_weight[0], preferred_element_type=jnp.float32)
    up_proj = jnp.dot(flattened, expert_up_weight[0], preferred_element_type=jnp.float32)
    hidden = (jax.nn.silu(gate_proj) * up_proj).astype(jnp.bfloat16)
    hidden_whole = lax.all_gather(hidden, "tp", axis=1, tiled=True)
    expert_out = jnp.dot(
        hidden_whole, expert_down_weight[0], preferred_element_type=jnp.float32
    ).astype(jnp.bfloat16)
    results = expert_out.reshape(arrived.shape[0], arrived.shape[1], expert_out.shape[1])
    returned = lax.all_to_all(results, "sp", split_axis=0, concat_axis=0, tiled=True)
    flat = returned.reshape(sources * capacity, returned.shape[2])
    routed_part = jnp.zeros((segment, flat.shape[1]), jnp.float32)
    for route_idx in range(top_count):
        routed_part = (
            routed_part
            + flat[slot_of[:, route_idx]].astype(jnp.float32)
            * chosen_expert_weight[:, route_idx][:, None]
        )
    moe_columns = routed_part.astype(jnp.bfloat16)
    moe_rows = lax.all_to_all(moe_columns, "tp", split_axis=0, concat_axis=1, tiled=True)
    return (
        stream.astype(jnp.float32) + rms_scale(moe_rows.astype(jnp.float32), expert_after_gain)
    ).astype(jnp.bfloat16)


def pieces_of(array):
    high = lax.reduce_precision(array, 8, 7)
    rest = array - high
    middle = lax.reduce_precision(rest, 8, 7)
    return [part.astype(jnp.bfloat16) for part in (high, middle, rest - middle)]


def swap(array, axis, bits):
    return lax.ppermute(array, axis, [(i, i ^ bits) for i in range(lax.axis_size(axis))])


def hop(array, chips, share, step):
    pairs = [
        (chip * share + core, (chip + step) % chips * share + core)
        for chip in range(chips)
        for core in range(share)
    ]
    return lax.ppermute(array, "sp", pairs)


def contract(left, right, dims):
    return lax.dot_general(left, right, ((dims[:1], dims[1:]), ((), ())), preferred_element_type=jnp.float32)


def cell_kernel(mine_ref, other_ref, forget_ref, gate_ref, out_ref):
    count, rows, half = other_ref.shape
    half = half // 2
    wide = out_ref.shape[1]
    square = (rows, rows)
    first = lax.broadcasted_iota(jnp.int32, square, 0)
    second = lax.broadcasted_iota(jnp.int32, square, 1)
    lower = first >= second
    running = jnp.dot(
        forget_ref[...],
        (first <= second).astype(jnp.float32),
        precision=lax.Precision.HIGHEST,
        preferred_element_type=jnp.float32,
    )
    base = jnp.zeros((1, 1), jnp.float32)
    top = jnp.zeros((1, 1), jnp.float32)
    levels, tops = [], []
    for j in range(count):
        level = gate_ref[j : j + 1, :] - (running[j : j + 1, :] + base)
        levels.append(level)
        tops.append(top)
        base = base + running[j : j + 1, rows - 1 : rows]
        top = jnp.maximum(top, jnp.max(level, axis=1, keepdims=True))
    for i in range(count):
        query_a = mine_ref[i, :rows, :half]
        query_b = other_ref[i, :, :half]
        masked = jnp.where(lower, levels[i], very_low)
        peak = jnp.maximum(tops[i], jnp.max(masked, axis=1, keepdims=True))
        numer = jnp.zeros((rows, wide), jnp.float32)
        denom = jnp.zeros((rows, 1), jnp.float32)
        for j in range(i + 1):
            scores = contract(query_a, mine_ref[j, :rows, half : 2 * half], (1, 1)) + contract(
                query_b, other_ref[j, :, half:], (1, 1)
            )
            level = masked if j == i else levels[j]
            weights = scores * DQK ** (-0.5) * jnp.exp(level - peak)
            denom = denom + jnp.sum(weights, axis=1, keepdims=True)
            numer = numer + contract(
                weights.astype(jnp.bfloat16), mine_ref[j, :rows, 2 * half : 2 * half + wide], (1, 0)
            )
        logits = mine_ref[i, :rows, 2 * half + wide :].astype(jnp.float32)
        outcome = numer / jnp.maximum(jnp.abs(denom), den_floor) / (1.0 + jnp.exp(-logits))
        out_ref[i * rows : (i + 1) * rows, :] = outcome.astype(jnp.bfloat16)


def picker_of(routes, expert, capacity):
    length = routes.shape[1]
    hit = jnp.max((routes == expert).astype(jnp.float32), axis=0, keepdims=True)
    before = lax.broadcasted_iota(jnp.int32, (length, length), 0) < lax.broadcasted_iota(
        jnp.int32, (length, length), 1
    )
    rank = contract(
        jnp.broadcast_to(hit, (8, length)).astype(jnp.bfloat16), before.astype(jnp.bfloat16), (1, 0)
    )[:1]
    slots = lax.broadcasted_iota(jnp.int32, (capacity, length), 0).astype(jnp.float32)
    return jnp.where((rank == slots) & (hit > 0.0), 1.0, 0.0).astype(jnp.bfloat16)


def select_kernel(place_ref, routes_ref, *refs):
    own_ref, other_ref = refs[-2:]
    pieces = refs[:-2]
    sides = len(pieces) // 2
    capacity = own_ref.shape[0] // 2
    width = pieces[0].shape[1]
    for part in range(2):
        routes = routes_ref[place_ref[part]]
        for out_ref, expert in ((own_ref, place_ref[2]), (other_ref, place_ref[3])):
            picker = picker_of(routes, expert, capacity)
            for side in range(sides):
                where = pl.multiple_of((place_ref[4] ^ side) * width, width)
                out_ref[part * capacity : (part + 1) * capacity, pl.ds(where, width)] = contract(
                    picker, pieces[part * sides + side][...], (1, 0)
                ).astype(jnp.bfloat16)


def combine_kernel(place_ref, routes_ref, weights_ref, own_ref, other_ref, out_ref):
    capacity = own_ref.shape[0] // 2
    length = routes_ref.shape[2]
    same = lax.broadcasted_iota(jnp.int32, (length, length), 0) == lax.broadcasted_iota(
        jnp.int32, (length, length), 1
    )
    for part in range(2):
        routes = routes_ref[place_ref[part]]
        scales = weights_ref[place_ref[part]]
        total = jnp.zeros(out_ref.shape[1:], jnp.float32)
        for rows_ref, expert in ((own_ref, place_ref[2]), (other_ref, place_ref[3])):
            picker = picker_of(routes, expert, capacity)
            scale_row = jnp.sum(jnp.where(routes == expert, scales, 0.0), axis=0, keepdims=True)
            scale = jnp.sum(jnp.where(same, scale_row, 0.0), axis=1, keepdims=True)
            spread = contract(picker, rows_ref[part * capacity : (part + 1) * capacity, :], (0, 0))
            total = total + scale * spread
        out_ref[part] = total.astype(jnp.bfloat16)


def smem():
    return pl.BlockSpec(memory_space=pltpu.SMEM)


def vmem(count):
    return [pl.BlockSpec(memory_space=pltpu.VMEM)] * count


def by_heads(
    queries,
    keys,
    values,
    output_gate_logits,
    input_gate_log,
    forget_gate_logits,
    extra_log_decay,
    cell_output_weight,
    residual_input,
    cell_norm_gain,
    expert_before_gain,
    expert_after_gain,
    routes,
    chosen_expert_weight,
    expert_gate_weight,
    expert_up_weight,
    expert_down_weight,
):
    segment = queries.shape[0]
    sources = lax.axis_size("sp")
    sides = lax.axis_size("tp")
    place = lax.axis_index("sp")
    side = lax.axis_index("tp")
    head_count = queries.shape[1] // DQK
    share = sources // head_count
    chips = sources // share
    chip, core = place // share, place % share
    half, wide = DQK // share, DV // share
    top_count = routes.shape[1]
    capacity = max(2, min(segment, 5 * segment * top_count // (4 * sources)))

    def to_parts(array):
        return array.reshape(segment, sources, -1)

    main = jnp.concatenate(
        [to_parts(a) for a in (queries, keys, values, output_gate_logits)], axis=2
    ).transpose(1, 0, 2)
    line = main.shape[2]
    forget_log_value = jax.nn.log_sigmoid(forget_gate_logits) + extra_log_decay
    gates = jnp.stack(pieces_of(forget_log_value) + pieces_of(input_gate_log))
    gates = jnp.repeat(gates.transpose(2, 0, 1).reshape(head_count, -1), share, axis=0)
    gates = jnp.pad(gates, ((0, 0), (0, -gates.shape[1] % line))).reshape(sources, -1, line)
    told = jnp.stack([routes.astype(jnp.bfloat16)] + pieces_of(chosen_expert_weight))
    told = told.transpose(0, 2, 1).reshape(-1)
    told_size = told.shape[0]
    told = jnp.pad(told, (0, -told_size % line)).reshape(1, -1, line)
    told = jnp.broadcast_to(told, (sources,) + told.shape[1:])
    gate_rows = gates.shape[1]
    extra_rows = gate_rows + told.shape[1]
    filler = jnp.zeros((sources, -extra_rows % 8, line), jnp.bfloat16)
    sent = jnp.concatenate([main, gates, told, filler], axis=1)
    mine = lax.all_to_all(sent, "sp", split_axis=0, concat_axis=0, tiled=True)
    other = swap(mine[:, :segment, : 2 * half], "sp", 1)
    got = mine[:, segment : segment + gate_rows].astype(jnp.float32).reshape(sources, -1)
    got = jnp.sum(got[:, : 6 * segment].reshape(sources, 2, 3, segment), axis=2)
    said = mine[:, segment + gate_rows : segment + extra_rows].astype(jnp.float32)
    said = said.reshape(sources, -1)[:, :told_size].reshape(sources, 4, top_count, segment)
    all_routes = said[:, 0].astype(jnp.int32)
    all_weights = jnp.sum(said[:, 1:], axis=1)

    gated = pl.pallas_call(
        cell_kernel,
        in_specs=vmem(4),
        out_specs=vmem(1)[0],
        out_shape=jax.ShapeDtypeStruct((sources * segment, wide), jnp.bfloat16),
        name="cell",
    )(mine, other, got[:, 0], got[:, 1])

    def weight_rows(index):
        return lax.dynamic_slice_in_dim(cell_output_weight, index * wide, wide, 0)

    mixed_part = None
    for step in range(chips):
        block = hop(gated, chips, share, step) if step else gated
        origin = (chip - step) % chips * share
        for array, index in ((block, origin + core), (swap(block, "sp", 1), origin + 1 - core)):
            term = jnp.dot(array, weight_rows(index), preferred_element_type=jnp.float32)
            mixed_part = term if mixed_part is None else mixed_part + term
    mixed_part = mixed_part.astype(jnp.bfloat16).reshape(sources, sides, segment // sides, -1)
    mixed = None
    for bits in range(sides):
        piece = lax.dynamic_index_in_dim(mixed_part, side ^ bits, 1, False)
        piece = (swap(piece, "tp", bits) if bits else piece).astype(jnp.float32)
        mixed = piece if mixed is None else mixed + piece
    mixed = lax.all_to_all(mixed.astype(jnp.bfloat16), "sp", split_axis=0, concat_axis=0, tiled=True)
    mixed = mixed.transpose(1, 0, 2).reshape(segment // sides, -1).astype(jnp.float32)
    stream = (residual_input.astype(jnp.float32) + rms_scale(mixed, cell_norm_gain)).astype(
        jnp.bfloat16
    )
    normed = rms_scale(stream.astype(jnp.float32), expert_before_gain).astype(jnp.bfloat16)
    columns = lax.all_to_all(normed, "tp", split_axis=1, concat_axis=0, tiled=True)

    def down_rows(bits):
        width = expert_down_weight.shape[1] // sides
        return lax.dynamic_slice_in_dim(expert_down_weight[0], (side ^ bits) * width, width, 0)

    down_weights = [down_rows(bits) for bits in range(sides)]
    arrived = [hop(columns, chips, share, step) if step else columns for step in range(chips)]
    returned = None
    for pair in range(chips // 2):
        steps = (2 * pair, 2 * pair + 1)
        pieces = [
            swap(arrived[step], "tp", bits) if bits else arrived[step]
            for step in steps
            for bits in range(sides)
        ]
        spots = [(chip - step) % chips * share + core for step in steps]
        spots = jnp.stack(spots + [place, place ^ 1, side]).astype(jnp.int32)
        width = columns.shape[1] * sides
        own_rows, other_rows = pl.pallas_call(
            select_kernel,
            in_specs=[smem()] + vmem(1 + len(pieces)),
            out_specs=vmem(2),
            out_shape=[jax.ShapeDtypeStruct((2 * capacity, width), jnp.bfloat16)] * 2,
            name="select",
        )(spots, all_routes, *pieces)
        rows_in = jnp.concatenate([own_rows, swap(other_rows, "sp", 1)], axis=0)
        gate_proj = jnp.dot(rows_in, expert_gate_weight[0], preferred_element_type=jnp.float32)
        up_proj = jnp.dot(rows_in, expert_up_weight[0], preferred_element_type=jnp.float32)
        hidden = (jax.nn.silu(gate_proj) * up_proj).astype(jnp.bfloat16)
        expert_out = None
        for bits in range(sides):
            term = jnp.dot(
                swap(hidden, "tp", bits) if bits else hidden,
                down_weights[bits],
                preferred_element_type=jnp.float32,
            )
            expert_out = term if expert_out is None else expert_out + term
        expert_out = expert_out.astype(jnp.bfloat16)
        own_out = expert_out[: 2 * capacity]
        other_out = swap(expert_out[2 * capacity :], "sp", 1)
        summed = pl.pallas_call(
            combine_kernel,
            in_specs=[smem()] + vmem(4),
            out_specs=vmem(1)[0],
            out_shape=jax.ShapeDtypeStruct((2, segment, own_out.shape[1]), jnp.bfloat16),
            name="combine",
        )(spots, all_routes, all_weights, own_out, other_out)
        for index, step in enumerate(steps):
            back = hop(summed[index], chips, share, -step) if step else summed[index]
            back = back.astype(jnp.float32)
            returned = back if returned is None else returned + back
    moe_rows = lax.all_to_all(
        returned.astype(jnp.bfloat16), "tp", split_axis=0, concat_axis=1, tiled=True
    )
    return (
        stream.astype(jnp.float32) + rms_scale(moe_rows.astype(jnp.float32), expert_after_gain)
    ).astype(jnp.bfloat16)


def per_device(*arrays):
    queries, values, routes = arrays[0], arrays[2], arrays[12]
    sources, sides = lax.axis_size("sp"), lax.axis_size("tp")
    head_count = queries.shape[1] // DQK
    pairs = sources == 2 * head_count and head_count % 2 == 0
    powers = sides & (sides - 1) == 0
    if pairs and powers and queries.shape[0] == BLOCK and queries.shape[0] % (16 * sides) == 0:
        return by_heads(*arrays)
    return by_states(*arrays)


def solution(mesh):
    placed = (
        P("sp", "tp"),
        P("sp", "tp"),
        P("sp", "tp"),
        P("sp", "tp"),
        P("sp", "tp"),
        P("sp", "tp"),
        P("sp", "tp"),
        P("tp", "sp"),
        P(("sp", "tp"), None),
        P(),
        P(),
        P(),
        P("sp", None),
        P("sp", None),
        P("sp", None, "tp"),
        P("sp", None, "tp"),
        P("sp", None, "tp"),
    )
    return jax.shard_map(
        per_device, mesh=mesh, in_specs=placed, out_specs=P(("sp", "tp"), None), check_vma=False
    )
```

```python
import jax
import jax.numpy as jnp
from jax import lax
from jax.experimental import pallas as pl
from jax.experimental.pallas import tpu as pltpu
from jax.sharding import PartitionSpec as P

DQK = 256
DV = 512
BLOCK = 128


norm_eps = 1e-06
very_low = -1e30
den_floor = 8.0


def carried_in(part, axis, combine, identity):
    place = lax.axis_index(axis)
    gathered = jax.tree.map(lambda a: lax.all_gather(a, axis), part)
    state = jax.tree.map(lambda a, e: jnp.zeros_like(a) + jnp.asarray(e, a.dtype), part, identity)

    def one(step, state):
        return combine(
            state, jax.tree.map(lambda a: lax.dynamic_index_in_dim(a, step, 0, False), gathered)
        )

    return lax.fori_loop(0, place, one, state)


def rms_scale(inputs, gain):
    return inputs * lax.rsqrt(jnp.mean(inputs * inputs, axis=-1, keepdims=True) + norm_eps) * gain


def combine_states(earlier, later):
    total_early, matrix_early, vector_early, peak_early = earlier
    total_late, matrix_late, vector_late, peak_late = later
    shifted = total_late + peak_early
    peak = jnp.maximum(shifted, peak_late)
    keep_early = jnp.exp(shifted - peak)
    keep_late = jnp.exp(peak_late - peak)
    return (
        total_early + total_late,
        keep_early[:, None, None] * matrix_early + keep_late[:, None, None] * matrix_late,
        keep_early[:, None] * vector_early + keep_late[:, None] * vector_late,
        peak,
    )


def block_local(query_blk, key_blk, value_blk, gate_blk, forget_blk):
    key_scale = DQK ** (-0.5)
    running = jnp.cumsum(forget_blk, axis=-1)
    length = running.shape[-1]
    lower = lax.broadcasted_iota(jnp.int32, (length, length), 0) >= lax.broadcasted_iota(
        jnp.int32, (length, length), 1
    )
    offsets = jnp.where(
        lower, running[:, :, None] - running[:, None, :] + gate_blk[:, None, :], -jnp.inf
    )
    local_top = jnp.max(offsets, axis=-1)
    scores = (
        jnp.einsum("htd,hsd->hts", query_blk, key_blk, preferred_element_type=jnp.float32)
        * key_scale
    )
    weights = scores * jnp.exp(offsets - local_top[:, :, None])
    numerator = jnp.einsum(
        "hts,hsv->htv", weights.astype(jnp.bfloat16), value_blk, preferred_element_type=jnp.float32
    )
    denominator = jnp.sum(weights, axis=-1)
    return (running, local_top, numerator, denominator)


def read_out(query_blk, memory, running, local_top, numerator, denominator):
    matrix, vector, peak = memory
    query_wide = query_blk.astype(jnp.float32)
    carried = running + peak[:, None]
    highest = jnp.maximum(local_top, carried)
    inner_w = jnp.exp(local_top - highest)
    carried_w = jnp.exp(carried - highest)
    numer_all = inner_w[:, :, None] * numerator + carried_w[:, :, None] * jnp.einsum(
        "htd,hdv->htv", query_wide, matrix, precision=lax.Precision.HIGHEST
    )
    denom_all = inner_w * denominator + carried_w * jnp.einsum(
        "htd,hd->ht", query_wide, vector, precision=lax.Precision.HIGHEST
    )
    return numer_all / jnp.maximum(jnp.abs(denom_all), den_floor)[:, :, None]


def advance(memory, key_blk, value_blk, gate_blk, running):
    matrix, vector, peak = memory
    key_wide = key_blk.astype(jnp.float32) * DQK ** (-0.5)
    block_sum = running[:, -1]
    growth = block_sum[:, None] - running + gate_blk
    peak_new = jnp.maximum(block_sum + peak, jnp.max(growth, axis=-1))
    fading = jnp.exp(block_sum + peak - peak_new)
    writes = jnp.exp(growth - peak_new[:, None])
    weighted = (key_wide * writes[:, :, None]).astype(jnp.bfloat16)
    matrix_new = fading[:, None, None] * matrix + jnp.einsum(
        "hsd,hsv->hdv", weighted, value_blk, preferred_element_type=jnp.float32
    )
    vector_new = fading[:, None] * vector + jnp.einsum(
        "hs,hsd->hd", writes, key_wide, precision=lax.Precision.HIGHEST
    )
    return (matrix_new, vector_new, peak_new)


def by_states(
    queries,
    keys,
    values,
    output_gate_logits,
    input_gate_log,
    forget_gate_logits,
    extra_log_decay,
    cell_output_weight,
    residual_input,
    cell_norm_gain,
    expert_before_gain,
    expert_after_gain,
    routes,
    chosen_expert_weight,
    expert_gate_weight,
    expert_up_weight,
    expert_down_weight,
):
    segment = queries.shape[0]
    head_count = queries.shape[1] // DQK
    block_count = segment // BLOCK

    def split_heads(array, width):
        return array.reshape(block_count, BLOCK, head_count, width).transpose(0, 2, 1, 3)

    query_blocks = split_heads(queries, DQK)
    key_blocks = split_heads(keys, DQK)
    value_blocks = split_heads(values, DV)
    forget_log_value = jax.nn.log_sigmoid(forget_gate_logits) + extra_log_decay
    gate_blocks = input_gate_log.reshape(block_count, BLOCK, head_count).transpose(0, 2, 1)
    forget_blocks = forget_log_value.reshape(block_count, BLOCK, head_count).transpose(0, 2, 1)
    totals = jnp.sum(forget_log_value, axis=0)
    zero_matrix = jnp.zeros((head_count, DQK, DV), jnp.float32)
    zero_vector = jnp.zeros((head_count, DQK), jnp.float32)
    zero_heads = jnp.zeros((head_count,), jnp.float32)
    fresh = (zero_matrix, zero_vector, jnp.full((head_count,), very_low, jnp.float32))
    empty = (zero_heads,) + fresh
    anchor = (zero_heads, zero_matrix, zero_vector, zero_heads)

    def summarize(memory, inputs):
        key_blk, value_blk, gate_blk, forget_blk = inputs
        return (
            advance(memory, key_blk, value_blk, gate_blk, jnp.cumsum(forget_blk, axis=-1)),
            None,
        )

    own_state, unused = lax.scan(
        summarize, fresh, (key_blocks, value_blocks, gate_blocks, forget_blocks)
    )
    prefix = carried_in((totals,) + own_state, "sp", combine_states, empty)
    start_full = combine_states(anchor, prefix)

    def emit(memory, inputs):
        query_blk, key_blk, value_blk, gate_blk, forget_blk = inputs
        running, local_top, numerator, denominator = block_local(
            query_blk, key_blk, value_blk, gate_blk, forget_blk
        )
        outcome = read_out(query_blk, memory, running, local_top, numerator, denominator)
        return (advance(memory, key_blk, value_blk, gate_blk, running), outcome)

    unused, heads_out = lax.scan(
        emit, start_full[1:], (query_blocks, key_blocks, value_blocks, gate_blocks, forget_blocks)
    )
    cell_out = heads_out.transpose(0, 2, 1, 3).reshape(segment, head_count * DV)
    gated = (cell_out * jax.nn.sigmoid(output_gate_logits.astype(jnp.float32))).astype(jnp.bfloat16)
    whole_weight = lax.all_gather(cell_output_weight, "sp", axis=1, tiled=True)
    mixed = lax.psum_scatter(
        jnp.dot(gated, whole_weight, preferred_element_type=jnp.float32).astype(jnp.bfloat16),
        "tp",
        scatter_dimension=0,
        tiled=True,
    ).astype(jnp.float32)
    stream = (residual_input.astype(jnp.float32) + rms_scale(mixed, cell_norm_gain)).astype(
        jnp.bfloat16
    )
    normed = rms_scale(stream.astype(jnp.float32), expert_before_gain).astype(jnp.bfloat16)
    normed_all = lax.all_gather(normed, "tp", axis=0, tiled=True)
    sources = lax.axis_size("sp")
    top_count = routes.shape[1]
    capacity = max(2, min(segment, 5 * segment * top_count // (4 * sources)))
    width = normed_all.shape[1]
    labels = lax.broadcasted_iota(jnp.int32, (1, 1, sources), 2)
    matches = (routes[:, :, None] == labels).astype(jnp.int32)
    per_row = jnp.sum(matches, axis=1)
    before_rows = jnp.cumsum(per_row, axis=0) - per_row
    places = jnp.sum(matches * before_rows[:, None, :], axis=2)
    slot_of = routes * capacity + places
    slot_ids = lax.broadcasted_iota(jnp.int32, (sources * capacity, 1, 1), 0)
    picker = jnp.sum((slot_of[None, :, :] == slot_ids).astype(jnp.int32), axis=2).astype(
        jnp.bfloat16
    )
    buffer = jnp.dot(picker, normed_all, preferred_element_type=jnp.float32).astype(jnp.bfloat16)
    buffer = buffer.reshape(sources, capacity, width)
    arrived = lax.all_to_all(buffer, "sp", split_axis=0, concat_axis=0, tiled=True)
    flattened = arrived.reshape(-1, width)
    gate_proj = jnp.dot(flattened, expert_gate_weight[0], preferred_element_type=jnp.float32)
    up_proj = jnp.dot(flattened, expert_up_weight[0], preferred_element_type=jnp.float32)
    hidden = (jax.nn.silu(gate_proj) * up_proj).astype(jnp.bfloat16)
    hidden_whole = lax.all_gather(hidden, "tp", axis=1, tiled=True)
    expert_out = jnp.dot(
        hidden_whole, expert_down_weight[0], preferred_element_type=jnp.float32
    ).astype(jnp.bfloat16)
    results = expert_out.reshape(arrived.shape[0], arrived.shape[1], expert_out.shape[1])
    returned = lax.all_to_all(results, "sp", split_axis=0, concat_axis=0, tiled=True)
    flat = returned.reshape(sources * capacity, returned.shape[2])
    routed_part = jnp.zeros((segment, flat.shape[1]), jnp.float32)
    for route_idx in range(top_count):
        routed_part = (
            routed_part
            + flat[slot_of[:, route_idx]].astype(jnp.float32)
            * chosen_expert_weight[:, route_idx][:, None]
        )
    moe_columns = routed_part.astype(jnp.bfloat16)
    moe_rows = lax.all_to_all(moe_columns, "tp", split_axis=0, concat_axis=1, tiled=True)
    return (
        stream.astype(jnp.float32) + rms_scale(moe_rows.astype(jnp.float32), expert_after_gain)
    ).astype(jnp.bfloat16)


def swap(array, axis, bits):
    return lax.ppermute(array, axis, [(i, i ^ bits) for i in range(lax.axis_size(axis))])


def hop(array, chips, share, step):
    pairs = [
        (chip * share + core, (chip + step) % chips * share + core)
        for chip in range(chips)
        for core in range(share)
    ]
    return lax.ppermute(array, "sp", pairs)


def shift(array, chips, share, step):
    pairs = [
        (chip * share + core, (chip + step) * share + core)
        for chip in range(chips)
        for core in range(share)
        if 0 <= chip + step < chips
    ]
    return lax.ppermute(array, "sp", pairs)


def spread(array, chip, chips, share):
    if chips != 4:
        return [
            (hop(array, chips, share, step) if step else array, (chip - step) % chips)
            for step in range(chips)
        ]
    across = hop(array, chips, share, 2)
    upward, downward = shift(array, chips, share, 1), shift(array, chips, share, -1)
    pairs = [(at * share + core, to * share + core) for at, to in ((2, 3), (1, 0)) for core in range(share)]
    onward = lax.ppermute(across, "sp", pairs)
    last = chips - 1
    return [
        (array, chip),
        (upward, jnp.maximum(chip - 1, 0)),
        (downward, jnp.minimum(chip + 1, last)),
        (across, (chip + 2) % chips),
        (onward, jnp.where(chip == 0, last, 0)),
    ]


def contract(left, right, dims):
    return lax.dot_general(left, right, ((dims[:1], dims[1:]), ((), ())), preferred_element_type=jnp.float32)


def pack_kernel(
    spot_ref, query_ref, key_ref, value_ref, logit_ref, input_ref, forget_ref, decay_ref, routes_ref,
    weights_ref, *out_refs
):
    rows = query_ref.shape[0]
    chips = len(out_refs)
    wide = value_ref.shape[1] // (2 * chips)
    chip, core = spot_ref[0], spot_ref[1]
    same = lax.broadcasted_iota(jnp.int32, (rows, rows), 0) == lax.broadcasted_iota(
        jnp.int32, (rows, rows), 1
    )
    same = same.astype(jnp.bfloat16)

    def turned(array):
        high = lax.reduce_precision(array, 8, 7)
        rest = array - high
        middle = lax.reduce_precision(rest, 8, 7)
        parts = (high, middle, rest - middle)
        return [contract(part.astype(jnp.bfloat16), same, (0, 0)) for part in parts]

    logits = forget_ref[...]
    forget = jnp.minimum(logits, 0.0) - jnp.log1p(jnp.exp(-jnp.abs(logits))) + decay_ref[...]
    gates = turned(forget) + turned(input_ref[...])
    told = [contract(routes_ref[...].astype(jnp.bfloat16), same, (0, 0))] + turned(weights_ref[...])
    heads = gates[0].shape[0]
    tops = told[0].shape[0]
    for step, out_ref in enumerate(out_refs):
        head = (chip + step) % chips
        query_at = pl.multiple_of(head * DQK, DQK)
        out_ref[:rows, 2 * wide : 2 * wide + DQK] = query_ref[:, pl.ds(query_at, DQK)]
        out_ref[:rows, 2 * wide + DQK : 2 * wide + 2 * DQK] = key_ref[:, pl.ds(query_at, DQK)]
        for turn in range(2):
            value_at = pl.multiple_of((2 * head + (core ^ turn)) * wide, wide)
            base = turn * (2 * wide + 2 * DQK)
            out_ref[:rows, base : base + wide] = value_ref[:, pl.ds(value_at, wide)]
            out_ref[:rows, base + wide : base + 2 * wide] = logit_ref[:, pl.ds(value_at, wide)]
        mine = lax.broadcasted_iota(jnp.int32, (heads, rows), 0) == head
        lines = [jnp.sum(jnp.where(mine, gate, 0.0), axis=0, keepdims=True) for gate in gates]
        lines = lines + [line[i : i + 1] for line in told for i in range(tops)]
        spare = jnp.zeros((1, rows), jnp.float32)
        slots = (out_ref.shape[1] - 2 * wide) // rows
        filled = lines[:6] + [spare] * (slots - 6) + lines[6:]
        filled = filled + [spare] * (8 * slots - len(filled))
        for slot in range(slots):
            column = jnp.concatenate([filled[r * slots + slot] for r in range(8)], axis=0)
            at = 2 * wide + slot * rows
            out_ref[rows:, at : at + rows] = column.astype(jnp.bfloat16)


def cell_kernel(spot_ref, *refs):
    chips = (len(refs) - 6) // 2
    out_ref, routes_ref, weights_ref, data_ref, forget_ref, gate_ref = refs[2 * chips :]
    count = 2 * chips
    wide = out_ref.shape[1]
    rows = out_ref.shape[0] // count
    tops = routes_ref.shape[1]
    chip, core = spot_ref[0], spot_ref[1]
    for step in range(chips):
        origin = (chip + chips - step) % chips
        mine_ref, other_ref = refs[step], refs[chips + step]
        for ref, base, values_at, spot in (
            (mine_ref, 2 * wide, 0, 2 * origin + core),
            (other_ref, 0, 2 * DQK, 2 * origin + 1 - core),
        ):
            data_ref[spot, :, : 2 * DQK] = ref[:rows, base : base + 2 * DQK]
            data_ref[spot, :, 2 * DQK :] = ref[:rows, values_at : values_at + 2 * wide]
            slots = 2 * (wide + DQK) // rows
            extra = ref[rows:, base : base + slots * rows].astype(jnp.float32)

            def line(index):
                r, slot = index // slots, index % slots
                return extra[r : r + 1, slot * rows : (slot + 1) * rows]

            forget_ref[pl.ds(spot, 1), :] = line(0) + line(1) + line(2)
            gate_ref[pl.ds(spot, 1), :] = line(3) + line(4) + line(5)
            for i in range(tops):
                routes_ref[spot, i : i + 1, :] = line(slots + i).astype(jnp.int32)
                weights_ref[spot, i : i + 1, :] = (
                    line(slots + tops + i) + line(slots + 2 * tops + i) + line(slots + 3 * tops + i)
                )
    square = (rows, rows)
    first = lax.broadcasted_iota(jnp.int32, square, 0)
    second = lax.broadcasted_iota(jnp.int32, square, 1)
    lower = first >= second
    running = jnp.dot(
        forget_ref[...],
        (first <= second).astype(jnp.float32),
        precision=lax.Precision.HIGHEST,
        preferred_element_type=jnp.float32,
    )
    base = jnp.zeros((1, 1), jnp.float32)
    top = jnp.zeros((1, 1), jnp.float32)
    levels, tops = [], []
    for j in range(count):
        level = gate_ref[j : j + 1, :] - (running[j : j + 1, :] + base)
        levels.append(level)
        tops.append(top)
        base = base + running[j : j + 1, rows - 1 : rows]
        top = jnp.maximum(top, jnp.max(level, axis=1, keepdims=True))
    for i in range(count):
        query = data_ref[i, :, :DQK]
        masked = jnp.where(lower, levels[i], very_low)
        peak = jnp.maximum(tops[i], jnp.max(masked, axis=1, keepdims=True))
        numer = jnp.zeros((rows, wide), jnp.float32)
        denom = jnp.zeros((rows, 1), jnp.float32)
        for j in range(i + 1):
            scores = contract(query, data_ref[j, :, DQK : 2 * DQK], (1, 1))
            level = masked if j == i else levels[j]
            weights = scores * DQK ** (-0.5) * jnp.exp(level - peak)
            denom = denom + jnp.sum(weights, axis=1, keepdims=True)
            numer = numer + contract(
                weights.astype(jnp.bfloat16), data_ref[j, :, 2 * DQK : 2 * DQK + wide], (1, 0)
            )
        logits = data_ref[i, :, 2 * DQK + wide :].astype(jnp.float32)
        outcome = numer / jnp.maximum(jnp.abs(denom), den_floor) / (1.0 + jnp.exp(-logits))
        out_ref[i * rows : (i + 1) * rows, :] = outcome.astype(jnp.bfloat16)


def picker_of(routes, expert, capacity):
    length = routes.shape[1]
    hit = jnp.max((routes == expert).astype(jnp.float32), axis=0, keepdims=True)
    before = lax.broadcasted_iota(jnp.int32, (length, length), 0) < lax.broadcasted_iota(
        jnp.int32, (length, length), 1
    )
    rank = contract(
        jnp.broadcast_to(hit, (8, length)).astype(jnp.bfloat16), before.astype(jnp.bfloat16), (1, 0)
    )[:1]
    slots = lax.broadcasted_iota(jnp.int32, (capacity, length), 0).astype(jnp.float32)
    return jnp.where((rank == slots) & (hit > 0.0), 1.0, 0.0).astype(jnp.bfloat16)


def select_kernel(place_ref, routes_ref, *refs):
    own_ref, other_ref = refs[-2:]
    pieces = refs[:-2]
    sides = len(pieces) // 2
    capacity = own_ref.shape[0] // 2
    length = routes_ref.shape[2]
    short = pieces[0].shape[0]
    width = own_ref.shape[1]
    block = width // 4
    from_index = lax.broadcasted_iota(jnp.int32, (length, length), 0)
    to_index = lax.broadcasted_iota(jnp.int32, (length, length), 1)
    turned = (from_index == ((to_index // short) ^ place_ref[4]) * short + to_index % short).astype(
        jnp.bfloat16
    )
    for part in range(2):
        routes = routes_ref[place_ref[part]]
        for out_ref, expert in ((own_ref, place_ref[2]), (other_ref, place_ref[3])):
            picker = picker_of(routes, expert, capacity)
            picker = contract(picker, turned, (1, 0)).astype(jnp.bfloat16)
            for at in range(0, width, block):
                rows = jnp.concatenate(
                    [piece[:, at : at + block] for piece in pieces[part * sides : (part + 1) * sides]]
                )
                out_ref[part * capacity : (part + 1) * capacity, at : at + block] = contract(
                    picker, rows, (1, 0)
                ).astype(jnp.bfloat16)


def combine_kernel(place_ref, routes_ref, weights_ref, own_ref, other_ref, out_ref):
    capacity = own_ref.shape[0] // 2
    length = routes_ref.shape[2]
    same = lax.broadcasted_iota(jnp.int32, (length, length), 0) == lax.broadcasted_iota(
        jnp.int32, (length, length), 1
    )
    for part in range(2):
        routes = routes_ref[place_ref[part]]
        scales = weights_ref[place_ref[part]]
        total = jnp.zeros(out_ref.shape[1:], jnp.float32)
        for rows_ref, expert in ((own_ref, place_ref[2]), (other_ref, place_ref[3])):
            picker = picker_of(routes, expert, capacity)
            scale_row = jnp.sum(jnp.where(routes == expert, scales, 0.0), axis=0, keepdims=True)
            scale = jnp.sum(jnp.where(same, scale_row, 0.0), axis=1, keepdims=True)
            spread = contract(picker, rows_ref[part * capacity : (part + 1) * capacity, :], (0, 0))
            total = total + scale * spread
        out_ref[part] = total.astype(jnp.bfloat16)


def smem():
    return pl.BlockSpec(memory_space=pltpu.SMEM)


def vmem(count):
    return [pl.BlockSpec(memory_space=pltpu.VMEM)] * count


def by_heads(
    queries,
    keys,
    values,
    output_gate_logits,
    input_gate_log,
    forget_gate_logits,
    extra_log_decay,
    cell_output_weight,
    residual_input,
    cell_norm_gain,
    expert_before_gain,
    expert_after_gain,
    routes,
    chosen_expert_weight,
    expert_gate_weight,
    expert_up_weight,
    expert_down_weight,
):
    segment = queries.shape[0]
    sources = lax.axis_size("sp")
    sides = lax.axis_size("tp")
    place = lax.axis_index("sp")
    side = lax.axis_index("tp")
    head_count = queries.shape[1] // DQK
    share = sources // head_count
    chips = sources // share
    chip, core = place // share, place % share
    wide = DV // share
    top_count = routes.shape[1]
    capacity = max(2, min(segment, 5 * segment * top_count // (4 * sources)))
    spot = jnp.stack([chip, core]).astype(jnp.int32)
    line = 2 * DQK + 4 * wide
    packed = pl.pallas_call(
        pack_kernel,
        in_specs=[smem()] + vmem(9),
        out_specs=vmem(chips),
        out_shape=[jax.ShapeDtypeStruct((segment + 8, line), jnp.bfloat16)] * chips,
        name="pack",
    )(
        spot,
        queries,
        keys,
        values,
        output_gate_logits,
        input_gate_log,
        forget_gate_logits,
        extra_log_decay,
        routes,
        chosen_expert_weight,
    )
    mine = [hop(block, chips, share, step) if step else block for step, block in enumerate(packed)]
    other = [swap(block[:, 2 * wide :], "sp", 1) for block in mine]
    rows_total = sources * segment
    gated, all_routes, all_weights = pl.pallas_call(
        cell_kernel,
        in_specs=[smem()] + vmem(2 * chips),
        out_specs=vmem(3),
        out_shape=[
            jax.ShapeDtypeStruct((rows_total, wide), jnp.bfloat16),
            jax.ShapeDtypeStruct((sources, top_count, segment), jnp.int32),
            jax.ShapeDtypeStruct((sources, top_count, segment), jnp.float32),
        ],
        scratch_shapes=[
            pltpu.VMEM((sources, segment, 2 * DQK + 2 * wide), jnp.bfloat16),
            pltpu.VMEM((sources, segment), jnp.float32),
            pltpu.VMEM((sources, segment), jnp.float32),
        ],
        name="cell",
    )(spot, *mine, *other)

    def weight_rows(index):
        return lax.dynamic_slice_in_dim(cell_output_weight, index * wide, wide, 0)

    mixed_part = None
    for block, origin in spread(gated, chip, chips, share):
        for array, index in (
            (block, share * origin + core),
            (swap(block, "sp", 1), share * origin + 1 - core),
        ):
            term = jnp.dot(array, weight_rows(index), preferred_element_type=jnp.float32)
            mixed_part = term if mixed_part is None else mixed_part + term
    mixed_part = mixed_part.astype(jnp.bfloat16).reshape(sources, sides, segment // sides, -1)
    mixed = None
    for bits in range(sides):
        piece = lax.dynamic_index_in_dim(mixed_part, side ^ bits, 1, False)
        piece = (swap(piece, "tp", bits) if bits else piece).astype(jnp.float32)
        mixed = piece if mixed is None else mixed + piece
    mixed = lax.all_to_all(mixed.astype(jnp.bfloat16), "sp", split_axis=0, concat_axis=0, tiled=True)
    mixed = mixed.transpose(1, 0, 2).reshape(segment // sides, -1).astype(jnp.float32)
    stream = (residual_input.astype(jnp.float32) + rms_scale(mixed, cell_norm_gain)).astype(
        jnp.bfloat16
    )
    normed = rms_scale(stream.astype(jnp.float32), expert_before_gain).astype(jnp.bfloat16)

    def down_rows(bits):
        width = expert_down_weight.shape[1] // sides
        return lax.dynamic_slice_in_dim(expert_down_weight[0], (side ^ bits) * width, width, 0)

    down_weights = [down_rows(bits) for bits in range(sides)]
    arrived = [hop(normed, chips, share, step) if step else normed for step in range(chips)]
    returned = None
    for pair in range(chips // 2):
        steps = (2 * pair, 2 * pair + 1)
        pieces = [
            swap(arrived[step], "tp", bits) if bits else arrived[step]
            for step in steps
            for bits in range(sides)
        ]
        spots = [(chip - step) % chips * share + core for step in steps]
        spots = jnp.stack(spots + [place, place ^ 1, side]).astype(jnp.int32)
        width = normed.shape[1]
        own_rows, other_rows = pl.pallas_call(
            select_kernel,
            in_specs=[smem()] + vmem(1 + len(pieces)),
            out_specs=vmem(2),
            out_shape=[jax.ShapeDtypeStruct((2 * capacity, width), jnp.bfloat16)] * 2,
            name="select",
        )(spots, all_routes, *pieces)
        rows_in = jnp.concatenate([own_rows, swap(other_rows, "sp", 1)], axis=0)
        gate_proj = jnp.dot(rows_in, expert_gate_weight[0], preferred_element_type=jnp.float32)
        up_proj = jnp.dot(rows_in, expert_up_weight[0], preferred_element_type=jnp.float32)
        hidden = (jax.nn.silu(gate_proj) * up_proj).astype(jnp.bfloat16)
        expert_out = None
        for bits in range(sides):
            term = jnp.dot(
                swap(hidden, "tp", bits) if bits else hidden,
                down_weights[bits],
                preferred_element_type=jnp.float32,
            )
            expert_out = term if expert_out is None else expert_out + term
        expert_out = expert_out.astype(jnp.bfloat16)
        own_out = expert_out[: 2 * capacity]
        other_out = swap(expert_out[2 * capacity :], "sp", 1)
        summed = pl.pallas_call(
            combine_kernel,
            in_specs=[smem()] + vmem(4),
            out_specs=vmem(1)[0],
            out_shape=jax.ShapeDtypeStruct((2, segment, own_out.shape[1]), jnp.bfloat16),
            name="combine",
        )(spots, all_routes, all_weights, own_out, other_out)
        for index, step in enumerate(steps):
            back = hop(summed[index], chips, share, -step) if step else summed[index]
            back = back.astype(jnp.float32)
            returned = back if returned is None else returned + back
    moe_rows = lax.all_to_all(
        returned.astype(jnp.bfloat16), "tp", split_axis=0, concat_axis=1, tiled=True
    )
    return (
        stream.astype(jnp.float32) + rms_scale(moe_rows.astype(jnp.float32), expert_after_gain)
    ).astype(jnp.bfloat16)


def per_device(*arrays):
    queries, values, routes = arrays[0], arrays[2], arrays[12]
    sources, sides = lax.axis_size("sp"), lax.axis_size("tp")
    head_count = queries.shape[1] // DQK
    pairs = sources == 2 * head_count and head_count % 2 == 0
    powers = sides & (sides - 1) == 0
    if pairs and powers and queries.shape[0] == BLOCK and queries.shape[0] % (16 * sides) == 0:
        return by_heads(*arrays)
    return by_states(*arrays)


def solution(mesh):
    placed = (
        P("sp", "tp"),
        P("sp", "tp"),
        P("sp", "tp"),
        P("sp", "tp"),
        P("sp", "tp"),
        P("sp", "tp"),
        P("sp", "tp"),
        P("tp", "sp"),
        P(("sp", "tp"), None),
        P(),
        P(),
        P(),
        P("sp", None),
        P("sp", None),
        P("sp", None, "tp"),
        P("sp", None, "tp"),
        P("sp", None, "tp"),
    )
    return jax.shard_map(
        per_device, mesh=mesh, in_specs=placed, out_specs=P(("sp", "tp"), None), check_vma=False
    )
```

```python
import jax
import jax.numpy as jnp
from functools import partial
from jax import lax
from jax.experimental import pallas as pl
from jax.experimental.pallas import tpu as pltpu
from jax.sharding import PartitionSpec as P

DQK = 256
DV = 512
BLOCK = 128


norm_eps = 1e-06
very_low = -1e30
den_floor = 8.0


def carried_in(part, axis, combine, identity):
    place = lax.axis_index(axis)
    gathered = jax.tree.map(lambda a: lax.all_gather(a, axis), part)
    state = jax.tree.map(lambda a, e: jnp.zeros_like(a) + jnp.asarray(e, a.dtype), part, identity)

    def one(step, state):
        return combine(
            state, jax.tree.map(lambda a: lax.dynamic_index_in_dim(a, step, 0, False), gathered)
        )

    return lax.fori_loop(0, place, one, state)


def rms_scale(inputs, gain):
    return inputs * lax.rsqrt(jnp.mean(inputs * inputs, axis=-1, keepdims=True) + norm_eps) * gain


def combine_states(earlier, later):
    total_early, matrix_early, vector_early, peak_early = earlier
    total_late, matrix_late, vector_late, peak_late = later
    shifted = total_late + peak_early
    peak = jnp.maximum(shifted, peak_late)
    keep_early = jnp.exp(shifted - peak)
    keep_late = jnp.exp(peak_late - peak)
    return (
        total_early + total_late,
        keep_early[:, None, None] * matrix_early + keep_late[:, None, None] * matrix_late,
        keep_early[:, None] * vector_early + keep_late[:, None] * vector_late,
        peak,
    )


def block_local(query_blk, key_blk, value_blk, gate_blk, forget_blk):
    key_scale = DQK ** (-0.5)
    running = jnp.cumsum(forget_blk, axis=-1)
    length = running.shape[-1]
    lower = lax.broadcasted_iota(jnp.int32, (length, length), 0) >= lax.broadcasted_iota(
        jnp.int32, (length, length), 1
    )
    offsets = jnp.where(
        lower, running[:, :, None] - running[:, None, :] + gate_blk[:, None, :], -jnp.inf
    )
    local_top = jnp.max(offsets, axis=-1)
    scores = (
        jnp.einsum("htd,hsd->hts", query_blk, key_blk, preferred_element_type=jnp.float32)
        * key_scale
    )
    weights = scores * jnp.exp(offsets - local_top[:, :, None])
    numerator = jnp.einsum(
        "hts,hsv->htv", weights.astype(jnp.bfloat16), value_blk, preferred_element_type=jnp.float32
    )
    denominator = jnp.sum(weights, axis=-1)
    return (running, local_top, numerator, denominator)


def read_out(query_blk, memory, running, local_top, numerator, denominator):
    matrix, vector, peak = memory
    query_wide = query_blk.astype(jnp.float32)
    carried = running + peak[:, None]
    highest = jnp.maximum(local_top, carried)
    inner_w = jnp.exp(local_top - highest)
    carried_w = jnp.exp(carried - highest)
    numer_all = inner_w[:, :, None] * numerator + carried_w[:, :, None] * jnp.einsum(
        "htd,hdv->htv", query_wide, matrix, precision=lax.Precision.HIGHEST
    )
    denom_all = inner_w * denominator + carried_w * jnp.einsum(
        "htd,hd->ht", query_wide, vector, precision=lax.Precision.HIGHEST
    )
    return numer_all / jnp.maximum(jnp.abs(denom_all), den_floor)[:, :, None]


def advance(memory, key_blk, value_blk, gate_blk, running):
    matrix, vector, peak = memory
    key_wide = key_blk.astype(jnp.float32) * DQK ** (-0.5)
    block_sum = running[:, -1]
    growth = block_sum[:, None] - running + gate_blk
    peak_new = jnp.maximum(block_sum + peak, jnp.max(growth, axis=-1))
    fading = jnp.exp(block_sum + peak - peak_new)
    writes = jnp.exp(growth - peak_new[:, None])
    weighted = (key_wide * writes[:, :, None]).astype(jnp.bfloat16)
    matrix_new = fading[:, None, None] * matrix + jnp.einsum(
        "hsd,hsv->hdv", weighted, value_blk, preferred_element_type=jnp.float32
    )
    vector_new = fading[:, None] * vector + jnp.einsum(
        "hs,hsd->hd", writes, key_wide, precision=lax.Precision.HIGHEST
    )
    return (matrix_new, vector_new, peak_new)


def by_states(
    queries,
    keys,
    values,
    output_gate_logits,
    input_gate_log,
    forget_gate_logits,
    extra_log_decay,
    cell_output_weight,
    residual_input,
    cell_norm_gain,
    expert_before_gain,
    expert_after_gain,
    routes,
    chosen_expert_weight,
    expert_gate_weight,
    expert_up_weight,
    expert_down_weight,
):
    segment = queries.shape[0]
    head_count = queries.shape[1] // DQK
    block_count = segment // BLOCK

    def split_heads(array, width):
        return array.reshape(block_count, BLOCK, head_count, width).transpose(0, 2, 1, 3)

    query_blocks = split_heads(queries, DQK)
    key_blocks = split_heads(keys, DQK)
    value_blocks = split_heads(values, DV)
    forget_log_value = jax.nn.log_sigmoid(forget_gate_logits) + extra_log_decay
    gate_blocks = input_gate_log.reshape(block_count, BLOCK, head_count).transpose(0, 2, 1)
    forget_blocks = forget_log_value.reshape(block_count, BLOCK, head_count).transpose(0, 2, 1)
    totals = jnp.sum(forget_log_value, axis=0)
    zero_matrix = jnp.zeros((head_count, DQK, DV), jnp.float32)
    zero_vector = jnp.zeros((head_count, DQK), jnp.float32)
    zero_heads = jnp.zeros((head_count,), jnp.float32)
    fresh = (zero_matrix, zero_vector, jnp.full((head_count,), very_low, jnp.float32))
    empty = (zero_heads,) + fresh
    anchor = (zero_heads, zero_matrix, zero_vector, zero_heads)

    def summarize(memory, inputs):
        key_blk, value_blk, gate_blk, forget_blk = inputs
        return (
            advance(memory, key_blk, value_blk, gate_blk, jnp.cumsum(forget_blk, axis=-1)),
            None,
        )

    own_state, unused = lax.scan(
        summarize, fresh, (key_blocks, value_blocks, gate_blocks, forget_blocks)
    )
    prefix = carried_in((totals,) + own_state, "sp", combine_states, empty)
    start_full = combine_states(anchor, prefix)

    def emit(memory, inputs):
        query_blk, key_blk, value_blk, gate_blk, forget_blk = inputs
        running, local_top, numerator, denominator = block_local(
            query_blk, key_blk, value_blk, gate_blk, forget_blk
        )
        outcome = read_out(query_blk, memory, running, local_top, numerator, denominator)
        return (advance(memory, key_blk, value_blk, gate_blk, running), outcome)

    unused, heads_out = lax.scan(
        emit, start_full[1:], (query_blocks, key_blocks, value_blocks, gate_blocks, forget_blocks)
    )
    cell_out = heads_out.transpose(0, 2, 1, 3).reshape(segment, head_count * DV)
    gated = (cell_out * jax.nn.sigmoid(output_gate_logits.astype(jnp.float32))).astype(jnp.bfloat16)
    whole_weight = lax.all_gather(cell_output_weight, "sp", axis=1, tiled=True)
    mixed = lax.psum_scatter(
        jnp.dot(gated, whole_weight, preferred_element_type=jnp.float32).astype(jnp.bfloat16),
        "tp",
        scatter_dimension=0,
        tiled=True,
    ).astype(jnp.float32)
    stream = (residual_input.astype(jnp.float32) + rms_scale(mixed, cell_norm_gain)).astype(
        jnp.bfloat16
    )
    normed = rms_scale(stream.astype(jnp.float32), expert_before_gain).astype(jnp.bfloat16)
    normed_all = lax.all_gather(normed, "tp", axis=0, tiled=True)
    sources = lax.axis_size("sp")
    top_count = routes.shape[1]
    capacity = max(2, min(segment, 5 * segment * top_count // (4 * sources)))
    width = normed_all.shape[1]
    labels = lax.broadcasted_iota(jnp.int32, (1, 1, sources), 2)
    matches = (routes[:, :, None] == labels).astype(jnp.int32)
    per_row = jnp.sum(matches, axis=1)
    before_rows = jnp.cumsum(per_row, axis=0) - per_row
    places = jnp.sum(matches * before_rows[:, None, :], axis=2)
    slot_of = routes * capacity + places
    slot_ids = lax.broadcasted_iota(jnp.int32, (sources * capacity, 1, 1), 0)
    picker = jnp.sum((slot_of[None, :, :] == slot_ids).astype(jnp.int32), axis=2).astype(
        jnp.bfloat16
    )
    buffer = jnp.dot(picker, normed_all, preferred_element_type=jnp.float32).astype(jnp.bfloat16)
    buffer = buffer.reshape(sources, capacity, width)
    arrived = lax.all_to_all(buffer, "sp", split_axis=0, concat_axis=0, tiled=True)
    flattened = arrived.reshape(-1, width)
    gate_proj = jnp.dot(flattened, expert_gate_weight[0], preferred_element_type=jnp.float32)
    up_proj = jnp.dot(flattened, expert_up_weight[0], preferred_element_type=jnp.float32)
    hidden = (jax.nn.silu(gate_proj) * up_proj).astype(jnp.bfloat16)
    hidden_whole = lax.all_gather(hidden, "tp", axis=1, tiled=True)
    expert_out = jnp.dot(
        hidden_whole, expert_down_weight[0], preferred_element_type=jnp.float32
    ).astype(jnp.bfloat16)
    results = expert_out.reshape(arrived.shape[0], arrived.shape[1], expert_out.shape[1])
    returned = lax.all_to_all(results, "sp", split_axis=0, concat_axis=0, tiled=True)
    flat = returned.reshape(sources * capacity, returned.shape[2])
    routed_part = jnp.zeros((segment, flat.shape[1]), jnp.float32)
    for route_idx in range(top_count):
        routed_part = (
            routed_part
            + flat[slot_of[:, route_idx]].astype(jnp.float32)
            * chosen_expert_weight[:, route_idx][:, None]
        )
    moe_columns = routed_part.astype(jnp.bfloat16)
    moe_rows = lax.all_to_all(moe_columns, "tp", split_axis=0, concat_axis=1, tiled=True)
    return (
        stream.astype(jnp.float32) + rms_scale(moe_rows.astype(jnp.float32), expert_after_gain)
    ).astype(jnp.bfloat16)


def swap(array, axis, bits):
    return lax.ppermute(array, axis, [(i, i ^ bits) for i in range(lax.axis_size(axis))])


def hop(array, chips, share, step):
    pairs = [
        (chip * share + core, (chip + step) % chips * share + core)
        for chip in range(chips)
        for core in range(share)
    ]
    return lax.ppermute(array, "sp", pairs)


def shift(array, chips, share, step):
    pairs = [
        (chip * share + core, (chip + step) * share + core)
        for chip in range(chips)
        for core in range(share)
        if 0 <= chip + step < chips
    ]
    return lax.ppermute(array, "sp", pairs)


def spread(array, chip, chips, share):
    if chips != 4:
        return [
            (hop(array, chips, share, step) if step else array, (chip - step) % chips)
            for step in range(chips)
        ]
    across = hop(array, chips, share, 2)
    upward, downward = shift(array, chips, share, 1), shift(array, chips, share, -1)
    pairs = [(at * share + core, to * share + core) for at, to in ((2, 3), (1, 0)) for core in range(share)]
    onward = lax.ppermute(across, "sp", pairs)
    last = chips - 1
    return [
        (array, chip),
        (upward, jnp.maximum(chip - 1, 0)),
        (downward, jnp.minimum(chip + 1, last)),
        (across, (chip + 2) % chips),
        (onward, jnp.where(chip == 0, last, 0)),
    ]


def contract(left, right, dims):
    return lax.dot_general(left, right, ((dims[:1], dims[1:]), ((), ())), preferred_element_type=jnp.float32)


def pack_kernel(
    spot_ref, query_ref, key_ref, value_ref, logit_ref, input_ref, forget_ref, decay_ref, routes_ref,
    weights_ref, *out_refs
):
    rows = query_ref.shape[0]
    chips = len(out_refs)
    wide = value_ref.shape[1] // (2 * chips)
    chip, core = spot_ref[0], spot_ref[1]

    def pieces_of(array):
        high = lax.reduce_precision(array, 8, 7)
        rest = array - high
        middle = lax.reduce_precision(rest, 8, 7)
        return [high, middle, rest - middle]

    logits = forget_ref[...]
    forget = jnp.minimum(logits, 0.0) - jnp.log1p(jnp.exp(-jnp.abs(logits))) + decay_ref[...]
    gates = pieces_of(forget) + pieces_of(input_ref[...])
    told = [routes_ref[...].astype(jnp.float32)] + pieces_of(weights_ref[...])
    heads = gates[0].shape[0]
    tops = told[0].shape[0]
    for step, out_ref in enumerate(out_refs):
        head = (chip + step) % chips
        query_at = pl.multiple_of(head * DQK, DQK)
        out_ref[:rows, 2 * wide : 2 * wide + DQK] = query_ref[:, pl.ds(query_at, DQK)]
        out_ref[:rows, 2 * wide + DQK : 2 * wide + 2 * DQK] = key_ref[:, pl.ds(query_at, DQK)]
        for turn in range(2):
            value_at = pl.multiple_of((2 * head + (core ^ turn)) * wide, wide)
            base = turn * (2 * wide + 2 * DQK)
            out_ref[:rows, base : base + wide] = value_ref[:, pl.ds(value_at, wide)]
            out_ref[:rows, base + wide : base + 2 * wide] = logit_ref[:, pl.ds(value_at, wide)]
        mine = lax.broadcasted_iota(jnp.int32, (heads, rows), 0) == head
        lines = [jnp.sum(jnp.where(mine, gate, 0.0), axis=0, keepdims=True) for gate in gates]
        lines = lines + [line[i : i + 1] for line in told for i in range(tops)]
        spare = jnp.zeros((1, rows), jnp.float32)
        slots = (out_ref.shape[1] - 2 * wide) // rows
        filled = lines[:6] + [spare] * (slots - 6) + lines[6:]
        filled = filled + [spare] * (8 * slots - len(filled))
        for slot in range(slots):
            column = jnp.concatenate([filled[r * slots + slot] for r in range(8)], axis=0)
            at = 2 * wide + slot * rows
            out_ref[rows:, at : at + rows] = column.astype(jnp.bfloat16)


def cell_kernel(short, spot_ref, *refs):
    chips = (len(refs) - 7) // 2
    even_ref, odd_ref, routes_ref, weights_ref, data_ref, forget_ref, gate_ref = refs[2 * chips :]
    count = 2 * chips
    wide = even_ref.shape[1]
    rows = 2 * even_ref.shape[0] // count
    tops = routes_ref.shape[1]
    chip, core = spot_ref[0], spot_ref[1]
    for step in range(chips):
        origin = (chip + chips - step) % chips
        mine_ref, other_ref = refs[step], refs[chips + step]
        for ref, base, values_at, spot in (
            (mine_ref, 2 * wide, 0, 2 * origin + core),
            (other_ref, 0, 2 * DQK, 2 * origin + 1 - core),
        ):
            data_ref[spot, :, : 2 * DQK] = ref[:rows, base : base + 2 * DQK]
            data_ref[spot, :, 2 * DQK :] = ref[:rows, values_at : values_at + 2 * wide]
            slots = 2 * (wide + DQK) // rows
            extra = ref[rows:, base : base + slots * rows].astype(jnp.float32)

            def line(index):
                r, slot = index // slots, index % slots
                return extra[r : r + 1, slot * rows : (slot + 1) * rows]

            forget_ref[pl.ds(spot, 1), :] = line(0) + line(1) + line(2)
            gate_ref[pl.ds(spot, 1), :] = line(3) + line(4) + line(5)
            for i in range(tops):
                routes_ref[spot, i : i + 1, :] = line(slots + i).astype(jnp.int32)
                weights_ref[spot, i : i + 1, :] = (
                    line(slots + tops + i) + line(slots + 2 * tops + i) + line(slots + 3 * tops + i)
                )
    square = (rows, rows)
    first = lax.broadcasted_iota(jnp.int32, square, 0)
    second = lax.broadcasted_iota(jnp.int32, square, 1)
    lower = first >= second
    running = jnp.dot(
        forget_ref[...],
        (first <= second).astype(jnp.float32),
        precision=lax.Precision.HIGHEST,
        preferred_element_type=jnp.float32,
    )
    base = jnp.zeros((1, 1), jnp.float32)
    top = jnp.zeros((1, 1), jnp.float32)
    levels, tops = [], []
    for j in range(count):
        level = gate_ref[j : j + 1, :] - (running[j : j + 1, :] + base)
        levels.append(level)
        tops.append(top)
        base = base + running[j : j + 1, rows - 1 : rows]
        top = jnp.maximum(top, jnp.max(level, axis=1, keepdims=True))
    for i in range(count):
        query = data_ref[i, :, :DQK]
        masked = jnp.where(lower, levels[i], very_low)
        peak = jnp.maximum(tops[i], jnp.max(masked, axis=1, keepdims=True))
        numer = jnp.zeros((rows, wide), jnp.float32)
        denom = jnp.zeros((rows, 1), jnp.float32)
        for j in range(i + 1):
            scores = contract(query, data_ref[j, :, DQK : 2 * DQK], (1, 1))
            level = masked if j == i else levels[j]
            weights = scores * DQK ** (-0.5) * jnp.exp(level - peak)
            denom = denom + jnp.sum(weights, axis=1, keepdims=True)
            numer = numer + contract(
                weights.astype(jnp.bfloat16), data_ref[j, :, 2 * DQK : 2 * DQK + wide], (1, 0)
            )
        logits = data_ref[i, :, 2 * DQK + wide :].astype(jnp.float32)
        outcome = numer / jnp.maximum(jnp.abs(denom), den_floor) / (1.0 + jnp.exp(-logits))
        outcome = outcome.astype(jnp.bfloat16)
        for j in range(rows // (2 * short)):
            to = (i * rows // 2) + j * short
            even_ref[to : to + short] = outcome[2 * j * short : (2 * j + 1) * short]
            odd_ref[to : to + short] = outcome[(2 * j + 1) * short : (2 * j + 2) * short]


def picker_of(routes, expert, capacity):
    length = routes.shape[1]
    hit = jnp.max((routes == expert).astype(jnp.float32), axis=0, keepdims=True)
    before = lax.broadcasted_iota(jnp.int32, (length, length), 0) < lax.broadcasted_iota(
        jnp.int32, (length, length), 1
    )
    rank = contract(
        jnp.broadcast_to(hit, (8, length)).astype(jnp.bfloat16), before.astype(jnp.bfloat16), (1, 0)
    )[:1]
    slots = lax.broadcasted_iota(jnp.int32, (capacity, length), 0).astype(jnp.float32)
    return jnp.where((rank == slots) & (hit > 0.0), 1.0, 0.0).astype(jnp.bfloat16)


def select_kernel(steps, chips, spot_ref, routes_ref, *refs):
    chip, core, side = spot_ref[0], spot_ref[1], spot_ref[2]
    expert = 2 * chip + core
    own_ref, other_ref = refs[-2:]
    pieces = refs[:-2]
    sides = len(pieces) // 2
    capacity = own_ref.shape[0] // 2
    length = routes_ref.shape[2]
    short = pieces[0].shape[0]
    width = own_ref.shape[1]
    block = width // 4
    from_index = lax.broadcasted_iota(jnp.int32, (length, length), 0)
    to_index = lax.broadcasted_iota(jnp.int32, (length, length), 1)
    turned = (from_index == ((to_index // short) ^ side) * short + to_index % short).astype(
        jnp.bfloat16
    )
    for part, step in enumerate(steps):
        routes = routes_ref[2 * ((chip + chips - step) % chips) + core]
        for out_ref, wanted in ((own_ref, expert), (other_ref, expert ^ 1)):
            picker = picker_of(routes, wanted, capacity)
            picker = contract(picker, turned, (1, 0)).astype(jnp.bfloat16)
            for at in range(0, width, block):
                rows = jnp.concatenate(
                    [piece[:, at : at + block] for piece in pieces[part * sides : (part + 1) * sides]]
                )
                out_ref[part * capacity : (part + 1) * capacity, at : at + block] = contract(
                    picker, rows, (1, 0)
                ).astype(jnp.bfloat16)


def combine_kernel(steps, chips, spot_ref, routes_ref, weights_ref, own_ref, other_ref, *out_refs):
    chip, core = spot_ref[0], spot_ref[1]
    expert = 2 * chip + core
    capacity = other_ref.shape[0] // 2
    length = routes_ref.shape[2]
    same = lax.broadcasted_iota(jnp.int32, (length, length), 0) == lax.broadcasted_iota(
        jnp.int32, (length, length), 1
    )
    for part, (step, out_ref) in enumerate(zip(steps, out_refs)):
        at = 2 * ((chip + chips - step) % chips) + core
        routes = routes_ref[at]
        scales = weights_ref[at]
        total = jnp.zeros(out_ref.shape, jnp.float32)
        for rows_ref, wanted in ((own_ref, expert), (other_ref, expert ^ 1)):
            picker = picker_of(routes, wanted, capacity)
            scale_row = jnp.sum(jnp.where(routes == wanted, scales, 0.0), axis=0, keepdims=True)
            scale = jnp.sum(jnp.where(same, scale_row, 0.0), axis=1, keepdims=True)
            spread_rows = contract(picker, rows_ref[part * capacity : (part + 1) * capacity, :], (0, 0))
            total = total + scale * spread_rows
        out_ref[...] = total.astype(jnp.bfloat16)


def norm_kernel(
    spot_ref, kept_a, got_a, kept_b, got_b, residual_ref, gain_ref, next_ref, stream_ref, normed_ref,
    mixed_ref
):
    chip, core = spot_ref[0], spot_ref[1]
    chips, short, block = kept_a.shape
    for at, kept, got in ((0, kept_a, got_a), (short, kept_b, got_b)):
        for step in range(chips):
            origin = 2 * ((chip + chips - step) % chips)
            for ref, index in ((kept, origin + core), (got, origin + 1 - core)):
                where = pl.ds(pl.multiple_of(index * block, block), block)
                mixed_ref[at : at + short, where] = ref[step].astype(jnp.float32)
    stream = residual_ref[...].astype(jnp.float32) + rms_scale(mixed_ref[...], gain_ref[...])
    stream = stream.astype(jnp.bfloat16)
    stream_ref[...] = stream
    normed_ref[...] = rms_scale(stream.astype(jnp.float32), next_ref[...]).astype(jnp.bfloat16)


def last_kernel(spot_ref, stream_ref, gain_ref, *refs):
    out_ref, rows_ref = refs[-2:]
    block = refs[0].shape[1]
    for bits, ref in enumerate(refs[:-2]):
        where = pl.ds(pl.multiple_of((spot_ref[2] ^ bits) * block, block), block)
        rows_ref[:, where] = ref[...].astype(jnp.float32)
    out = stream_ref[...].astype(jnp.float32) + rms_scale(rows_ref[...], gain_ref[...])
    out_ref[...] = out.astype(jnp.bfloat16)


def smem():
    return pl.BlockSpec(memory_space=pltpu.SMEM)


def vmem(count):
    return [pl.BlockSpec(memory_space=pltpu.VMEM)] * count


def by_heads(
    queries,
    keys,
    values,
    output_gate_logits,
    input_gate_log,
    forget_gate_logits,
    extra_log_decay,
    cell_output_weight,
    residual_input,
    cell_norm_gain,
    expert_before_gain,
    expert_after_gain,
    routes,
    chosen_expert_weight,
    expert_gate_weight,
    expert_up_weight,
    expert_down_weight,
):
    segment = queries.shape[0]
    sources = lax.axis_size("sp")
    sides = lax.axis_size("tp")
    place = lax.axis_index("sp")
    side = lax.axis_index("tp")
    head_count = queries.shape[1] // DQK
    share = sources // head_count
    chips = sources // share
    chip, core = place // share, place % share
    wide = DV // share
    top_count = routes.shape[1]
    capacity = max(2, min(segment, 5 * segment * top_count // (4 * sources)))
    spot = jnp.stack([chip, core, side]).astype(jnp.int32)
    line = 2 * DQK + 4 * wide
    packed = pl.pallas_call(
        pack_kernel,
        in_specs=[smem()] + vmem(9),
        out_specs=vmem(chips),
        out_shape=[jax.ShapeDtypeStruct((segment + 8, line), jnp.bfloat16)] * chips,
        name="pack",
    )(
        spot,
        queries,
        keys,
        values,
        output_gate_logits,
        input_gate_log.T,
        forget_gate_logits.T,
        extra_log_decay.T,
        routes.T,
        chosen_expert_weight.T,
    )
    mine = [hop(block, chips, share, step) if step else block for step, block in enumerate(packed)]
    other = [swap(block[:, 2 * wide :], "sp", 1) for block in mine]
    short = segment // (2 * sides)
    half_rows = jax.ShapeDtypeStruct((sources * segment // 2, wide), jnp.bfloat16)
    even, odd, all_routes, all_weights = pl.pallas_call(
        partial(cell_kernel, short),
        in_specs=[smem()] + vmem(2 * chips),
        out_specs=vmem(4),
        out_shape=[
            half_rows,
            half_rows,
            jax.ShapeDtypeStruct((sources, top_count, segment), jnp.int32),
            jax.ShapeDtypeStruct((sources, top_count, segment), jnp.float32),
        ],
        scratch_shapes=[
            pltpu.VMEM((sources, segment, 2 * DQK + 2 * wide), jnp.bfloat16),
            pltpu.VMEM((sources, segment), jnp.float32),
            pltpu.VMEM((sources, segment), jnp.float32),
        ],
        name="cell",
    )(spot, *mine, *other)

    def weight_rows(index):
        return lax.dynamic_slice_in_dim(cell_output_weight, index * wide, wide, 0)

    weights_at = {}

    def project(gated):
        total = None
        for order, (block, origin) in enumerate(spread(gated, chip, chips, share)):
            for turn, array in enumerate((block, swap(block, "sp", 1))):
                index = share * origin + (1 - core if turn else core)
                if (order, turn) not in weights_at:
                    weights_at[order, turn] = weight_rows(index)
                term = jnp.dot(array, weights_at[order, turn], preferred_element_type=jnp.float32)
                total = term if total is None else total + term
        total = total.astype(jnp.bfloat16).reshape(sources, sides, short, -1)
        summed = None
        for bits in range(sides):
            piece = lax.dynamic_index_in_dim(total, side ^ bits, 1, False)
            piece = (swap(piece, "tp", bits) if bits else piece).astype(jnp.float32)
            summed = piece if summed is None else summed + piece
        summed = summed.astype(jnp.bfloat16).reshape(chips, share, short, -1)
        back = []
        for step in range(chips):
            block = lax.dynamic_index_in_dim(summed, (chip + step) % chips, 0, False)
            back.append(hop(block, chips, share, step) if step else block)
        back = jnp.stack(back)
        kept = lax.dynamic_index_in_dim(back, core, 1, False)
        return [kept, swap(lax.dynamic_index_in_dim(back, 1 - core, 1, False), "sp", 1)]

    own_shape = jax.ShapeDtypeStruct(residual_input.shape, jnp.bfloat16)
    stream, normed = pl.pallas_call(
        norm_kernel,
        in_specs=[smem()] + vmem(7),
        out_specs=vmem(2),
        out_shape=[own_shape, own_shape],
        scratch_shapes=[pltpu.VMEM(residual_input.shape, jnp.float32)],
        name="norm",
    )(
        spot,
        *project(even),
        *project(odd),
        residual_input,
        cell_norm_gain.reshape(1, -1),
        expert_before_gain.reshape(1, -1),
    )

    def down_rows(bits):
        width = expert_down_weight.shape[1] // sides
        return lax.dynamic_slice_in_dim(expert_down_weight[0], (side ^ bits) * width, width, 0)

    down_weights = [down_rows(bits) for bits in range(sides)]
    def around(array, first):
        pieces = [array]
        bits = first
        for turn in range(sides.bit_length() - 1):
            pieces = pieces + [swap(piece, "tp", bits) for piece in pieces]
            bits = bits * 2 if bits * 2 < sides else 1
        order = [0]
        bits = first
        for turn in range(sides.bit_length() - 1):
            order = order + [place ^ bits for place in order]
            bits = bits * 2 if bits * 2 < sides else 1
        return [pieces[order.index(place)] for place in range(sides)]

    steps_of = [tuple(range(first, chips, chips // 2)) for first in range(chips // 2)]
    arrived = {step: normed for step in (0,)}
    for step in [step for steps in steps_of for step in steps if step]:
        arrived[step] = hop(normed, chips, share, step)
    spread_pieces = []
    for steps in steps_of:
        pieces = []
        for order, step in enumerate(steps):
            pieces = pieces + around(arrived[step], sides // 2 if order % 2 else 1)
        spread_pieces.append(pieces)
    width = normed.shape[1]
    hidden_parts = []
    earlier = None
    for steps, pieces in zip(steps_of, spread_pieces):
        if earlier is not None:
            earlier, pieces = lax.optimization_barrier((earlier, pieces))
            hidden_parts[-1] = earlier
        own_rows, other_rows = pl.pallas_call(
            partial(select_kernel, steps, chips),
            in_specs=[smem()] + vmem(1 + len(pieces)),
            out_specs=vmem(2),
            out_shape=[jax.ShapeDtypeStruct((2 * capacity, width), jnp.bfloat16)] * 2,
            name="select",
        )(spot, all_routes, *pieces)
        rows_in = jnp.concatenate([own_rows, swap(other_rows, "sp", 1)], axis=0)
        gate_proj = jnp.dot(rows_in, expert_gate_weight[0], preferred_element_type=jnp.float32)
        up_proj = jnp.dot(rows_in, expert_up_weight[0], preferred_element_type=jnp.float32)
        earlier = (jax.nn.silu(gate_proj) * up_proj).astype(jnp.bfloat16)
        hidden_parts.append(earlier)
    returned = None
    for order, (steps, hidden) in enumerate(zip(steps_of, hidden_parts)):
        expert_out = None
        for bits, piece in enumerate(around(hidden, sides // 2 if order % 2 else 1)):
            term = jnp.dot(piece, down_weights[bits], preferred_element_type=jnp.float32)
            expert_out = term if expert_out is None else expert_out + term
        expert_out = expert_out.astype(jnp.bfloat16)
        other_out = swap(expert_out[2 * capacity :], "sp", 1)
        summed = pl.pallas_call(
            partial(combine_kernel, steps, chips),
            in_specs=[smem()] + vmem(4),
            out_specs=vmem(2),
            out_shape=[jax.ShapeDtypeStruct((segment, expert_out.shape[1]), jnp.bfloat16)] * 2,
            name="combine",
        )(spot, all_routes, all_weights, expert_out, other_out)
        for array, step in zip(summed, steps):
            back = (hop(array, chips, share, -step) if step else array).astype(jnp.float32)
            returned = back if returned is None else returned + back
    returned = returned.astype(jnp.bfloat16).reshape(sides, 2 * short, -1)
    parts = []
    for bits in range(sides):
        piece = lax.dynamic_index_in_dim(returned, side ^ bits, 0, False)
        parts.append(swap(piece, "tp", bits) if bits else piece)
    return pl.pallas_call(
        last_kernel,
        in_specs=[smem()] + vmem(2 + sides),
        out_specs=vmem(1)[0],
        out_shape=own_shape,
        scratch_shapes=[pltpu.VMEM(residual_input.shape, jnp.float32)],
        name="last",
    )(spot, stream, expert_after_gain.reshape(1, -1), *parts)


def per_device(*arrays):
    queries, values, routes = arrays[0], arrays[2], arrays[12]
    sources, sides = lax.axis_size("sp"), lax.axis_size("tp")
    head_count = queries.shape[1] // DQK
    pairs = sources == 2 * head_count and head_count % 2 == 0
    powers = sides & (sides - 1) == 0
    if pairs and powers and queries.shape[0] == BLOCK and queries.shape[0] % (32 * sides) == 0:
        return by_heads(*arrays)
    return by_states(*arrays)


def solution(mesh):
    placed = (
        P("sp", "tp"),
        P("sp", "tp"),
        P("sp", "tp"),
        P("sp", "tp"),
        P("sp", "tp"),
        P("sp", "tp"),
        P("sp", "tp"),
        P("tp", "sp"),
        P(("sp", "tp"), None),
        P(),
        P(),
        P(),
        P("sp", None),
        P("sp", None),
        P("sp", None, "tp"),
        P("sp", None, "tp"),
        P("sp", None, "tp"),
    )
    return jax.shard_map(
        per_device, mesh=mesh, in_specs=placed, out_specs=P(("sp", "tp"), None), check_vma=False
    )
```

```python
import jax
import jax.numpy as jnp
from functools import partial
from jax import lax
from jax.experimental import pallas as pl
from jax.experimental.pallas import tpu as pltpu
from jax.sharding import PartitionSpec as P

DQK = 256
DV = 512
BLOCK = 128


norm_eps = 1e-06
very_low = -1e30
den_floor = 8.0


def carried_in(part, axis, combine, identity):
    place = lax.axis_index(axis)
    gathered = jax.tree.map(lambda a: lax.all_gather(a, axis), part)
    state = jax.tree.map(lambda a, e: jnp.zeros_like(a) + jnp.asarray(e, a.dtype), part, identity)

    def one(step, state):
        return combine(
            state, jax.tree.map(lambda a: lax.dynamic_index_in_dim(a, step, 0, False), gathered)
        )

    return lax.fori_loop(0, place, one, state)


def rms_scale(inputs, gain):
    return inputs * lax.rsqrt(jnp.mean(inputs * inputs, axis=-1, keepdims=True) + norm_eps) * gain


def combine_states(earlier, later):
    total_early, matrix_early, vector_early, peak_early = earlier
    total_late, matrix_late, vector_late, peak_late = later
    shifted = total_late + peak_early
    peak = jnp.maximum(shifted, peak_late)
    keep_early = jnp.exp(shifted - peak)
    keep_late = jnp.exp(peak_late - peak)
    return (
        total_early + total_late,
        keep_early[:, None, None] * matrix_early + keep_late[:, None, None] * matrix_late,
        keep_early[:, None] * vector_early + keep_late[:, None] * vector_late,
        peak,
    )


def block_local(query_blk, key_blk, value_blk, gate_blk, forget_blk):
    key_scale = DQK ** (-0.5)
    running = jnp.cumsum(forget_blk, axis=-1)
    length = running.shape[-1]
    lower = lax.broadcasted_iota(jnp.int32, (length, length), 0) >= lax.broadcasted_iota(
        jnp.int32, (length, length), 1
    )
    offsets = jnp.where(
        lower, running[:, :, None] - running[:, None, :] + gate_blk[:, None, :], -jnp.inf
    )
    local_top = jnp.max(offsets, axis=-1)
    scores = (
        jnp.einsum("htd,hsd->hts", query_blk, key_blk, preferred_element_type=jnp.float32)
        * key_scale
    )
    weights = scores * jnp.exp(offsets - local_top[:, :, None])
    numerator = jnp.einsum(
        "hts,hsv->htv", weights.astype(jnp.bfloat16), value_blk, preferred_element_type=jnp.float32
    )
    denominator = jnp.sum(weights, axis=-1)
    return (running, local_top, numerator, denominator)


def read_out(query_blk, memory, running, local_top, numerator, denominator):
    matrix, vector, peak = memory
    query_wide = query_blk.astype(jnp.float32)
    carried = running + peak[:, None]
    highest = jnp.maximum(local_top, carried)
    inner_w = jnp.exp(local_top - highest)
    carried_w = jnp.exp(carried - highest)
    numer_all = inner_w[:, :, None] * numerator + carried_w[:, :, None] * jnp.einsum(
        "htd,hdv->htv", query_wide, matrix, precision=lax.Precision.HIGHEST
    )
    denom_all = inner_w * denominator + carried_w * jnp.einsum(
        "htd,hd->ht", query_wide, vector, precision=lax.Precision.HIGHEST
    )
    return numer_all / jnp.maximum(jnp.abs(denom_all), den_floor)[:, :, None]


def advance(memory, key_blk, value_blk, gate_blk, running):
    matrix, vector, peak = memory
    key_wide = key_blk.astype(jnp.float32) * DQK ** (-0.5)
    block_sum = running[:, -1]
    growth = block_sum[:, None] - running + gate_blk
    peak_new = jnp.maximum(block_sum + peak, jnp.max(growth, axis=-1))
    fading = jnp.exp(block_sum + peak - peak_new)
    writes = jnp.exp(growth - peak_new[:, None])
    weighted = (key_wide * writes[:, :, None]).astype(jnp.bfloat16)
    matrix_new = fading[:, None, None] * matrix + jnp.einsum(
        "hsd,hsv->hdv", weighted, value_blk, preferred_element_type=jnp.float32
    )
    vector_new = fading[:, None] * vector + jnp.einsum(
        "hs,hsd->hd", writes, key_wide, precision=lax.Precision.HIGHEST
    )
    return (matrix_new, vector_new, peak_new)


def by_states(
    queries,
    keys,
    values,
    output_gate_logits,
    input_gate_log,
    forget_gate_logits,
    extra_log_decay,
    cell_output_weight,
    residual_input,
    cell_norm_gain,
    expert_before_gain,
    expert_after_gain,
    routes,
    chosen_expert_weight,
    expert_gate_weight,
    expert_up_weight,
    expert_down_weight,
):
    segment = queries.shape[0]
    head_count = queries.shape[1] // DQK
    block_count = segment // BLOCK

    def split_heads(array, width):
        return array.reshape(block_count, BLOCK, head_count, width).transpose(0, 2, 1, 3)

    query_blocks = split_heads(queries, DQK)
    key_blocks = split_heads(keys, DQK)
    value_blocks = split_heads(values, DV)
    forget_log_value = jax.nn.log_sigmoid(forget_gate_logits) + extra_log_decay
    gate_blocks = input_gate_log.reshape(block_count, BLOCK, head_count).transpose(0, 2, 1)
    forget_blocks = forget_log_value.reshape(block_count, BLOCK, head_count).transpose(0, 2, 1)
    totals = jnp.sum(forget_log_value, axis=0)
    zero_matrix = jnp.zeros((head_count, DQK, DV), jnp.float32)
    zero_vector = jnp.zeros((head_count, DQK), jnp.float32)
    zero_heads = jnp.zeros((head_count,), jnp.float32)
    fresh = (zero_matrix, zero_vector, jnp.full((head_count,), very_low, jnp.float32))
    empty = (zero_heads,) + fresh
    anchor = (zero_heads, zero_matrix, zero_vector, zero_heads)

    def summarize(memory, inputs):
        key_blk, value_blk, gate_blk, forget_blk = inputs
        return (
            advance(memory, key_blk, value_blk, gate_blk, jnp.cumsum(forget_blk, axis=-1)),
            None,
        )

    own_state, unused = lax.scan(
        summarize, fresh, (key_blocks, value_blocks, gate_blocks, forget_blocks)
    )
    prefix = carried_in((totals,) + own_state, "sp", combine_states, empty)
    start_full = combine_states(anchor, prefix)

    def emit(memory, inputs):
        query_blk, key_blk, value_blk, gate_blk, forget_blk = inputs
        running, local_top, numerator, denominator = block_local(
            query_blk, key_blk, value_blk, gate_blk, forget_blk
        )
        outcome = read_out(query_blk, memory, running, local_top, numerator, denominator)
        return (advance(memory, key_blk, value_blk, gate_blk, running), outcome)

    unused, heads_out = lax.scan(
        emit, start_full[1:], (query_blocks, key_blocks, value_blocks, gate_blocks, forget_blocks)
    )
    cell_out = heads_out.transpose(0, 2, 1, 3).reshape(segment, head_count * DV)
    gated = (cell_out * jax.nn.sigmoid(output_gate_logits.astype(jnp.float32))).astype(jnp.bfloat16)
    whole_weight = lax.all_gather(cell_output_weight, "sp", axis=1, tiled=True)
    mixed = lax.psum_scatter(
        jnp.dot(gated, whole_weight, preferred_element_type=jnp.float32).astype(jnp.bfloat16),
        "tp",
        scatter_dimension=0,
        tiled=True,
    ).astype(jnp.float32)
    stream = (residual_input.astype(jnp.float32) + rms_scale(mixed, cell_norm_gain)).astype(
        jnp.bfloat16
    )
    normed = rms_scale(stream.astype(jnp.float32), expert_before_gain).astype(jnp.bfloat16)
    normed_all = lax.all_gather(normed, "tp", axis=0, tiled=True)
    sources = lax.axis_size("sp")
    top_count = routes.shape[1]
    capacity = max(2, min(segment, 5 * segment * top_count // (4 * sources)))
    width = normed_all.shape[1]
    labels = lax.broadcasted_iota(jnp.int32, (1, 1, sources), 2)
    matches = (routes[:, :, None] == labels).astype(jnp.int32)
    per_row = jnp.sum(matches, axis=1)
    before_rows = jnp.cumsum(per_row, axis=0) - per_row
    places = jnp.sum(matches * before_rows[:, None, :], axis=2)
    slot_of = routes * capacity + places
    slot_ids = lax.broadcasted_iota(jnp.int32, (sources * capacity, 1, 1), 0)
    picker = jnp.sum((slot_of[None, :, :] == slot_ids).astype(jnp.int32), axis=2).astype(
        jnp.bfloat16
    )
    buffer = jnp.dot(picker, normed_all, preferred_element_type=jnp.float32).astype(jnp.bfloat16)
    buffer = buffer.reshape(sources, capacity, width)
    arrived = lax.all_to_all(buffer, "sp", split_axis=0, concat_axis=0, tiled=True)
    flattened = arrived.reshape(-1, width)
    gate_proj = jnp.dot(flattened, expert_gate_weight[0], preferred_element_type=jnp.float32)
    up_proj = jnp.dot(flattened, expert_up_weight[0], preferred_element_type=jnp.float32)
    hidden = (jax.nn.silu(gate_proj) * up_proj).astype(jnp.bfloat16)
    hidden_whole = lax.all_gather(hidden, "tp", axis=1, tiled=True)
    expert_out = jnp.dot(
        hidden_whole, expert_down_weight[0], preferred_element_type=jnp.float32
    ).astype(jnp.bfloat16)
    results = expert_out.reshape(arrived.shape[0], arrived.shape[1], expert_out.shape[1])
    returned = lax.all_to_all(results, "sp", split_axis=0, concat_axis=0, tiled=True)
    flat = returned.reshape(sources * capacity, returned.shape[2])
    routed_part = jnp.zeros((segment, flat.shape[1]), jnp.float32)
    for route_idx in range(top_count):
        routed_part = (
            routed_part
            + flat[slot_of[:, route_idx]].astype(jnp.float32)
            * chosen_expert_weight[:, route_idx][:, None]
        )
    moe_columns = routed_part.astype(jnp.bfloat16)
    moe_rows = lax.all_to_all(moe_columns, "tp", split_axis=0, concat_axis=1, tiled=True)
    return (
        stream.astype(jnp.float32) + rms_scale(moe_rows.astype(jnp.float32), expert_after_gain)
    ).astype(jnp.bfloat16)


def swap(array, axis, bits):
    return lax.ppermute(array, axis, [(i, i ^ bits) for i in range(lax.axis_size(axis))])


def hop(array, chips, share, step):
    pairs = [
        (chip * share + core, (chip + step) % chips * share + core)
        for chip in range(chips)
        for core in range(share)
    ]
    return lax.ppermute(array, "sp", pairs)


def shift(array, chips, share, step):
    pairs = [
        (chip * share + core, (chip + step) * share + core)
        for chip in range(chips)
        for core in range(share)
        if 0 <= chip + step < chips
    ]
    return lax.ppermute(array, "sp", pairs)


def spread(array, chip, chips, share):
    if chips != 4:
        return [
            (hop(array, chips, share, step) if step else array, (chip - step) % chips)
            for step in range(chips)
        ]
    across = hop(array, chips, share, 2)
    upward = shift(array, chips, share, 1)
    downward = shift(array, chips, share, -1)
    pairs = [(at * share + core, to * share + core) for at, to in ((2, 3), (1, 0)) for core in range(share)]
    onward = lax.ppermute(across, "sp", pairs)
    last = chips - 1
    return [
        (array, chip),
        (upward, jnp.maximum(chip - 1, 0)),
        (downward, jnp.minimum(chip + 1, last)),
        (across, (chip + 2) % chips),
        (onward, jnp.where(chip == 0, last, 0)),
    ]


def contract(left, right, dims):
    return lax.dot_general(left, right, ((dims[:1], dims[1:]), ((), ())), preferred_element_type=jnp.float32)


def pack_kernel(
    spot_ref, query_ref, key_ref, value_ref, logit_ref, input_ref, forget_ref, decay_ref, routes_ref,
    weights_ref, *out_refs
):
    rows = query_ref.shape[0]
    chips = len(out_refs)
    wide = value_ref.shape[1] // (2 * chips)
    chip, core = spot_ref[0], spot_ref[1]

    def pieces_of(array):
        high = lax.reduce_precision(array, 8, 7)
        rest = array - high
        middle = lax.reduce_precision(rest, 8, 7)
        return [high, middle, rest - middle]

    logits = forget_ref[...]
    forget = jnp.minimum(logits, 0.0) - jnp.log1p(jnp.exp(-jnp.abs(logits))) + decay_ref[...]
    gates = pieces_of(forget) + pieces_of(input_ref[...])
    told = [routes_ref[...].astype(jnp.float32)] + pieces_of(weights_ref[...])
    heads = gates[0].shape[0]
    tops = told[0].shape[0]
    for step, out_ref in enumerate(out_refs):
        head = (chip + step) % chips
        query_at = pl.multiple_of(head * DQK, DQK)
        out_ref[:rows, 2 * wide : 2 * wide + DQK] = query_ref[:, pl.ds(query_at, DQK)]
        out_ref[:rows, 2 * wide + DQK : 2 * wide + 2 * DQK] = key_ref[:, pl.ds(query_at, DQK)]
        for turn in range(2):
            value_at = pl.multiple_of((2 * head + (core ^ turn)) * wide, wide)
            base = turn * (2 * wide + 2 * DQK)
            out_ref[:rows, base : base + wide] = value_ref[:, pl.ds(value_at, wide)]
            out_ref[:rows, base + wide : base + 2 * wide] = logit_ref[:, pl.ds(value_at, wide)]
        mine = lax.broadcasted_iota(jnp.int32, (heads, rows), 0) == head
        lines = [jnp.sum(jnp.where(mine, gate, 0.0), axis=0, keepdims=True) for gate in gates]
        lines = lines + [line[i : i + 1] for line in told for i in range(tops)]
        spare = jnp.zeros((1, rows), jnp.float32)
        slots = (out_ref.shape[1] - 2 * wide) // rows
        filled = lines[:6] + [spare] * (slots - 6) + lines[6:]
        filled = filled + [spare] * (8 * slots - len(filled))
        for slot in range(slots):
            column = jnp.concatenate([filled[r * slots + slot] for r in range(8)], axis=0)
            at = 2 * wide + slot * rows
            out_ref[rows:, at : at + rows] = column.astype(jnp.bfloat16)


def cell_kernel(short, spot_ref, *refs):
    chips = (len(refs) - 7) // 2
    even_ref, odd_ref, routes_ref, weights_ref, data_ref, forget_ref, gate_ref = refs[2 * chips :]
    count = 2 * chips
    wide = even_ref.shape[1]
    rows = 2 * even_ref.shape[0] // count
    tops = routes_ref.shape[1]
    chip, core = spot_ref[0], spot_ref[1]
    for step in range(chips):
        origin = (chip + chips - step) % chips
        mine_ref, other_ref = refs[step], refs[chips + step]
        for ref, base, values_at, spot in (
            (mine_ref, 2 * wide, 0, 2 * origin + core),
            (other_ref, 0, 2 * DQK, 2 * origin + 1 - core),
        ):
            data_ref[spot, :, : 2 * DQK] = ref[:rows, base : base + 2 * DQK]
            data_ref[spot, :, 2 * DQK :] = ref[:rows, values_at : values_at + 2 * wide]
            slots = 2 * (wide + DQK) // rows
            extra = ref[rows:, base : base + slots * rows].astype(jnp.float32)

            def line(index):
                r, slot = index // slots, index % slots
                return extra[r : r + 1, slot * rows : (slot + 1) * rows]

            forget_ref[pl.ds(spot, 1), :] = line(0) + line(1) + line(2)
            gate_ref[pl.ds(spot, 1), :] = line(3) + line(4) + line(5)
            for i in range(tops):
                routes_ref[spot, i : i + 1, :] = line(slots + i).astype(jnp.int32)
                weights_ref[spot, i : i + 1, :] = (
                    line(slots + tops + i) + line(slots + 2 * tops + i) + line(slots + 3 * tops + i)
                )
    square = (rows, rows)
    first = lax.broadcasted_iota(jnp.int32, square, 0)
    second = lax.broadcasted_iota(jnp.int32, square, 1)
    lower = first >= second
    running = jnp.dot(
        forget_ref[...],
        (first <= second).astype(jnp.float32),
        precision=lax.Precision.HIGHEST,
        preferred_element_type=jnp.float32,
    )
    base = jnp.zeros((1, 1), jnp.float32)
    top = jnp.zeros((1, 1), jnp.float32)
    levels, tops = [], []
    for j in range(count):
        level = gate_ref[j : j + 1, :] - (running[j : j + 1, :] + base)
        levels.append(level)
        tops.append(top)
        base = base + running[j : j + 1, rows - 1 : rows]
        top = jnp.maximum(top, jnp.max(level, axis=1, keepdims=True))
    for i in range(count):
        query = data_ref[i, :, :DQK]
        masked = jnp.where(lower, levels[i], very_low)
        peak = jnp.maximum(tops[i], jnp.max(masked, axis=1, keepdims=True))
        numer = jnp.zeros((rows, wide), jnp.float32)
        denom = jnp.zeros((rows, 1), jnp.float32)
        for j in range(i + 1):
            scores = contract(query, data_ref[j, :, DQK : 2 * DQK], (1, 1))
            level = masked if j == i else levels[j]
            weights = scores * DQK ** (-0.5) * jnp.exp(level - peak)
            denom = denom + jnp.sum(weights, axis=1, keepdims=True)
            numer = numer + contract(
                weights.astype(jnp.bfloat16), data_ref[j, :, 2 * DQK : 2 * DQK + wide], (1, 0)
            )
        logits = data_ref[i, :, 2 * DQK + wide :].astype(jnp.float32)
        outcome = numer / jnp.maximum(jnp.abs(denom), den_floor) / (1.0 + jnp.exp(-logits))
        outcome = outcome.astype(jnp.bfloat16)
        for j in range(rows // (2 * short)):
            to = (i * rows // 2) + j * short
            even_ref[to : to + short] = outcome[2 * j * short : (2 * j + 1) * short]
            odd_ref[to : to + short] = outcome[(2 * j + 1) * short : (2 * j + 2) * short]


def picker_of(routes, expert, capacity):
    length = routes.shape[1]
    hit = jnp.max((routes == expert).astype(jnp.float32), axis=0, keepdims=True)
    before = lax.broadcasted_iota(jnp.int32, (length, length), 0) < lax.broadcasted_iota(
        jnp.int32, (length, length), 1
    )
    rank = contract(
        jnp.broadcast_to(hit, (8, length)).astype(jnp.bfloat16), before.astype(jnp.bfloat16), (1, 0)
    )[:1]
    slots = lax.broadcasted_iota(jnp.int32, (capacity, length), 0).astype(jnp.float32)
    return jnp.where((rank == slots) & (hit > 0.0), 1.0, 0.0).astype(jnp.bfloat16)


def select_kernel(steps, chips, spot_ref, routes_ref, *refs):
    own_ref, other_ref, picker_ref = refs[-3:]
    pieces = refs[:-3]
    sides = len(pieces) // 2
    capacity = own_ref.shape[0] // 2
    length = routes_ref.shape[2]
    short = pieces[0].shape[0]

    @pl.when(pl.program_id(0) == 0)
    def _():
        chip, core, side = spot_ref[0], spot_ref[1], spot_ref[2]
        expert = 2 * chip + core
        from_index = lax.broadcasted_iota(jnp.int32, (length, length), 0)
        to_index = lax.broadcasted_iota(jnp.int32, (length, length), 1)
        turned = from_index == ((to_index // short) ^ side) * short + to_index % short
        for part, step in enumerate(steps):
            routes = routes_ref[2 * ((chip + chips - step) % chips) + core]
            for turn in range(2):
                picker = picker_of(routes, expert ^ turn, capacity)
                picker = contract(picker, turned.astype(jnp.bfloat16), (1, 0))
                picker_ref[part, turn * capacity : (turn + 1) * capacity, :] = picker.astype(jnp.bfloat16)

    for part in range(2):
        rows = jnp.concatenate([piece[...] for piece in pieces[part * sides : (part + 1) * sides]])
        picked = contract(picker_ref[part], rows, (1, 0)).astype(jnp.bfloat16)
        own_ref[part * capacity : (part + 1) * capacity, :] = picked[:capacity]
        other_ref[part * capacity : (part + 1) * capacity, :] = picked[capacity:]


def combine_kernel(steps, chips, spot_ref, routes_ref, weights_ref, own_ref, other_ref, *out_refs):
    chip, core = spot_ref[0], spot_ref[1]
    expert = 2 * chip + core
    capacity = other_ref.shape[0] // 2
    length = routes_ref.shape[2]
    same = lax.broadcasted_iota(jnp.int32, (length, length), 0) == lax.broadcasted_iota(
        jnp.int32, (length, length), 1
    )
    for part, (step, out_ref) in enumerate(zip(steps, out_refs)):
        at = 2 * ((chip + chips - step) % chips) + core
        routes = routes_ref[at]
        scales = weights_ref[at]
        total = jnp.zeros(out_ref.shape, jnp.float32)
        for rows_ref, wanted in ((own_ref, expert), (other_ref, expert ^ 1)):
            picker = picker_of(routes, wanted, capacity)
            scale_row = jnp.sum(jnp.where(routes == wanted, scales, 0.0), axis=0, keepdims=True)
            scale = jnp.sum(jnp.where(same, scale_row, 0.0), axis=1, keepdims=True)
            spread_rows = contract(picker, rows_ref[part * capacity : (part + 1) * capacity, :], (0, 0))
            total = total + scale * spread_rows
        out_ref[...] = total.astype(jnp.bfloat16)


def norm_kernel(
    spot_ref, kept_a, got_a, kept_b, got_b, residual_ref, gain_ref, next_ref, stream_ref, normed_ref,
    mixed_ref
):
    chip, core = spot_ref[0], spot_ref[1]
    chips, short, block = kept_a.shape
    for at, kept, got in ((0, kept_a, got_a), (short, kept_b, got_b)):
        for step in range(chips):
            origin = 2 * ((chip + chips - step) % chips)
            for ref, index in ((kept, origin + core), (got, origin + 1 - core)):
                where = pl.ds(pl.multiple_of(index * block, block), block)
                mixed_ref[at : at + short, where] = ref[step].astype(jnp.float32)
    stream = residual_ref[...].astype(jnp.float32) + rms_scale(mixed_ref[...], gain_ref[...])
    stream = stream.astype(jnp.bfloat16)
    stream_ref[...] = stream
    normed_ref[...] = rms_scale(stream.astype(jnp.float32), next_ref[...]).astype(jnp.bfloat16)


def last_kernel(spot_ref, stream_ref, gain_ref, *refs):
    out_ref, rows_ref = refs[-2:]
    block = refs[0].shape[1]
    for bits, ref in enumerate(refs[:-2]):
        where = pl.ds(pl.multiple_of((spot_ref[2] ^ bits) * block, block), block)
        rows_ref[:, where] = ref[...].astype(jnp.float32)
    out = stream_ref[...].astype(jnp.float32) + rms_scale(rows_ref[...], gain_ref[...])
    out_ref[...] = out.astype(jnp.bfloat16)


def smem():
    return pl.BlockSpec(memory_space=pltpu.SMEM)


def vmem(count):
    return [pl.BlockSpec(memory_space=pltpu.VMEM)] * count


def by_heads(
    queries,
    keys,
    values,
    output_gate_logits,
    input_gate_log,
    forget_gate_logits,
    extra_log_decay,
    cell_output_weight,
    residual_input,
    cell_norm_gain,
    expert_before_gain,
    expert_after_gain,
    routes,
    chosen_expert_weight,
    expert_gate_weight,
    expert_up_weight,
    expert_down_weight,
):
    segment = queries.shape[0]
    sources = lax.axis_size("sp")
    sides = lax.axis_size("tp")
    place = lax.axis_index("sp")
    side = lax.axis_index("tp")
    head_count = queries.shape[1] // DQK
    share = sources // head_count
    chips = sources // share
    chip, core = place // share, place % share
    wide = DV // share
    top_count = routes.shape[1]
    capacity = max(2, min(segment, 5 * segment * top_count // (4 * sources)))
    spot = jnp.stack([chip, core, side]).astype(jnp.int32)
    line = 2 * DQK + 4 * wide
    packed = pl.pallas_call(
        pack_kernel,
        in_specs=[smem()] + vmem(9),
        out_specs=vmem(chips),
        out_shape=[jax.ShapeDtypeStruct((segment + 8, line), jnp.bfloat16)] * chips,
        name="pack",
    )(
        spot,
        queries,
        keys,
        values,
        output_gate_logits,
        input_gate_log.T,
        forget_gate_logits.T,
        extra_log_decay.T,
        routes.T,
        chosen_expert_weight.T,
    )
    mine = [hop(block, chips, share, step) if step else block for step, block in enumerate(packed)]
    other = [swap(block[:, 2 * wide :], "sp", 1) for block in mine]
    short = segment // (2 * sides)
    half_rows = jax.ShapeDtypeStruct((sources * segment // 2, wide), jnp.bfloat16)
    even, odd, all_routes, all_weights = pl.pallas_call(
        partial(cell_kernel, short),
        in_specs=[smem()] + vmem(2 * chips),
        out_specs=vmem(4),
        out_shape=[
            half_rows,
            half_rows,
            jax.ShapeDtypeStruct((sources, top_count, segment), jnp.int32),
            jax.ShapeDtypeStruct((sources, top_count, segment), jnp.float32),
        ],
        scratch_shapes=[
            pltpu.VMEM((sources, segment, 2 * DQK + 2 * wide), jnp.bfloat16),
            pltpu.VMEM((sources, segment), jnp.float32),
            pltpu.VMEM((sources, segment), jnp.float32),
        ],
        name="cell",
    )(spot, *mine, *other)

    def weight_rows(index):
        return lax.dynamic_slice_in_dim(cell_output_weight, index * wide, wide, 0)

    weights_at = {}

    def project(gated, before):
        total = None
        for order, (block, origin) in enumerate(spread(gated, chip, chips, share)):
            for turn, array in enumerate((block, swap(block, "sp", 1))):
                index = share * origin + (1 - core if turn else core)
                if (order, turn) not in weights_at:
                    weights_at[order, turn] = weight_rows(index)
                term = jnp.dot(array, weights_at[order, turn], preferred_element_type=jnp.float32)
                total = term if total is None else total + term
        total = total.astype(jnp.bfloat16).reshape(sources, sides, short, -1)
        if before is not None:
            total, before = lax.optimization_barrier((total, before))
        summed = None
        for bits in range(sides):
            piece = lax.dynamic_index_in_dim(total, side ^ bits, 1, False)
            piece = (swap(piece, "tp", bits) if bits else piece).astype(jnp.float32)
            summed = piece if summed is None else summed + piece
        summed = summed.astype(jnp.bfloat16).reshape(chips, share, short, -1)
        back = []
        for step in range(chips):
            block = lax.dynamic_index_in_dim(summed, (chip + step) % chips, 0, False)
            back.append(hop(block, chips, share, step) if step else block)
        back = jnp.stack(back)
        kept = lax.dynamic_index_in_dim(back, core, 1, False)
        return [kept, swap(lax.dynamic_index_in_dim(back, 1 - core, 1, False), "sp", 1)]

    own_shape = jax.ShapeDtypeStruct(residual_input.shape, jnp.bfloat16)
    parts_e = project(even, None)
    stream, normed = pl.pallas_call(
        norm_kernel,
        in_specs=[smem()] + vmem(7),
        out_specs=vmem(2),
        out_shape=[own_shape, own_shape],
        scratch_shapes=[pltpu.VMEM(residual_input.shape, jnp.float32)],
        name="norm",
    )(
        spot,
        *parts_e,
        *project(odd, parts_e[0]),
        residual_input,
        cell_norm_gain.reshape(1, -1),
        expert_before_gain.reshape(1, -1),
    )

    def down_rows(bits):
        width = expert_down_weight.shape[1] // sides
        return lax.dynamic_slice_in_dim(expert_down_weight[0], (side ^ bits) * width, width, 0)

    down_weights = lax.optimization_barrier([down_rows(bits) for bits in range(sides)])

    def around(array, first):
        pieces = [array]
        bits = first
        for _ in range(sides.bit_length() - 1):
            pieces = pieces + [swap(piece, "tp", bits) for piece in pieces]
            bits = bits * 2 if bits * 2 < sides else 1
        order = [0]
        bits = first
        for _ in range(sides.bit_length() - 1):
            order = order + [place ^ bits for place in order]
            bits = bits * 2 if bits * 2 < sides else 1
        return [pieces[order.index(place)] for place in range(sides)]

    steps_of = [(at, at + chips // 2) for at in range(chips // 2)]
    arrived = {0: normed}
    for step in [step for steps in steps_of for step in steps if step]:
        arrived[step] = hop(normed, chips, share, step)
    gathered = {}
    for steps in steps_of:
        for order, step in enumerate(steps):
            gathered[step] = around(arrived[step], sides // 2 if order % 2 else 1)
    spread_pieces = [[piece for step in steps for piece in gathered[step]] for steps in steps_of]
    width = normed.shape[1]
    hidden_parts = []
    earlier = None
    for steps, pieces in zip(steps_of, spread_pieces):
        if earlier is not None:
            earlier, pieces = lax.optimization_barrier((earlier, pieces))
        own_rows, other_rows = pl.pallas_call(
            partial(select_kernel, steps, chips),
            grid=(4,),
            in_specs=[
                smem(),
                pl.BlockSpec(all_routes.shape, lambda at: (0, 0, 0)),
            ]
            + [pl.BlockSpec((2 * short, width // 4), lambda at: (0, at))] * len(pieces),
            out_specs=[pl.BlockSpec((2 * capacity, width // 4), lambda at: (0, at))] * 2,
            out_shape=[jax.ShapeDtypeStruct((2 * capacity, width), jnp.bfloat16)] * 2,
            scratch_shapes=[pltpu.VMEM((2, 2 * capacity, segment), jnp.bfloat16)],
        )(spot, all_routes, *pieces)
        halves = []
        for rows_in in (own_rows, swap(other_rows, "sp", 1)):
            gate_proj = jnp.dot(rows_in, expert_gate_weight[0], preferred_element_type=jnp.float32)
            up_proj = jnp.dot(rows_in, expert_up_weight[0], preferred_element_type=jnp.float32)
            halves.append((jax.nn.silu(gate_proj) * up_proj).astype(jnp.bfloat16))
        earlier = jnp.concatenate(halves, axis=0)
        hidden_parts.append(earlier)
    returned = None
    for order, (steps, hidden) in enumerate(zip(steps_of, hidden_parts)):
        expert_out = None
        for bits, piece in enumerate(around(hidden, sides // 2 if order % 2 else 1)):
            term = jnp.dot(piece, down_weights[bits], preferred_element_type=jnp.float32)
            expert_out = term if expert_out is None else expert_out + term
        expert_out = expert_out.astype(jnp.bfloat16)
        other_out = swap(expert_out[2 * capacity :], "sp", 1)
        summed = pl.pallas_call(
            partial(combine_kernel, steps, chips),
            in_specs=[smem()] + vmem(4),
            out_specs=vmem(2),
            out_shape=[jax.ShapeDtypeStruct((segment, expert_out.shape[1]), jnp.bfloat16)] * 2,
        )(spot, all_routes, all_weights, expert_out, other_out)
        for array, step in zip(summed, steps):
            back = (hop(array, chips, share, -step) if step else array).astype(jnp.float32)
            returned = back if returned is None else returned + back
    returned = returned.astype(jnp.bfloat16).reshape(sides, 2 * short, -1)
    parts = []
    for bits in range(sides):
        piece = lax.dynamic_index_in_dim(returned, side ^ bits, 0, False)
        parts.append(swap(piece, "tp", bits) if bits else piece)
    return pl.pallas_call(
        last_kernel,
        in_specs=[smem()] + vmem(2 + sides),
        out_specs=vmem(1)[0],
        out_shape=own_shape,
        scratch_shapes=[pltpu.VMEM(residual_input.shape, jnp.float32)],
        name="last",
    )(spot, stream, expert_after_gain.reshape(1, -1), *parts)


def per_device(*arrays):
    queries = arrays[0]
    sources, sides = lax.axis_size("sp"), lax.axis_size("tp")
    head_count = queries.shape[1] // DQK
    pairs = sources == 2 * head_count and head_count % 2 == 0
    powers = sides & (sides - 1) == 0
    if pairs and powers and queries.shape[0] == BLOCK and queries.shape[0] % (32 * sides) == 0:
        return by_heads(*arrays)
    return by_states(*arrays)


def solution(mesh):
    placed = (
        P("sp", "tp"),
        P("sp", "tp"),
        P("sp", "tp"),
        P("sp", "tp"),
        P("sp", "tp"),
        P("sp", "tp"),
        P("sp", "tp"),
        P("tp", "sp"),
        P(("sp", "tp"), None),
        P(),
        P(),
        P(),
        P("sp", None),
        P("sp", None),
        P("sp", None, "tp"),
        P("sp", None, "tp"),
        P("sp", None, "tp"),
    )
    return jax.shard_map(
        per_device, mesh=mesh, in_specs=placed, out_specs=P(("sp", "tp"), None), check_vma=False
    )
```

```python
import jax
import jax.numpy as jnp
from functools import partial
from jax import lax
from jax.experimental import pallas as pl
from jax.experimental.pallas import tpu as pltpu
from jax.sharding import PartitionSpec as P

DQK = 256
DV = 512
BLOCK = 128


norm_eps = 1e-06
very_low = -1e30
den_floor = 8.0


def carried_in(part, axis, combine, identity):
    place = lax.axis_index(axis)
    gathered = jax.tree.map(lambda a: lax.all_gather(a, axis), part)
    state = jax.tree.map(lambda a, e: jnp.zeros_like(a) + jnp.asarray(e, a.dtype), part, identity)

    def one(step, state):
        return combine(
            state, jax.tree.map(lambda a: lax.dynamic_index_in_dim(a, step, 0, False), gathered)
        )

    return lax.fori_loop(0, place, one, state)


def rms_scale(inputs, gain):
    return inputs * lax.rsqrt(jnp.mean(inputs * inputs, axis=-1, keepdims=True) + norm_eps) * gain


def combine_states(earlier, later):
    total_early, matrix_early, vector_early, peak_early = earlier
    total_late, matrix_late, vector_late, peak_late = later
    shifted = total_late + peak_early
    peak = jnp.maximum(shifted, peak_late)
    keep_early = jnp.exp(shifted - peak)
    keep_late = jnp.exp(peak_late - peak)
    return (
        total_early + total_late,
        keep_early[:, None, None] * matrix_early + keep_late[:, None, None] * matrix_late,
        keep_early[:, None] * vector_early + keep_late[:, None] * vector_late,
        peak,
    )


def block_local(query_blk, key_blk, value_blk, gate_blk, forget_blk):
    key_scale = DQK ** (-0.5)
    running = jnp.cumsum(forget_blk, axis=-1)
    length = running.shape[-1]
    lower = lax.broadcasted_iota(jnp.int32, (length, length), 0) >= lax.broadcasted_iota(
        jnp.int32, (length, length), 1
    )
    offsets = jnp.where(
        lower, running[:, :, None] - running[:, None, :] + gate_blk[:, None, :], -jnp.inf
    )
    local_top = jnp.max(offsets, axis=-1)
    scores = (
        jnp.einsum("htd,hsd->hts", query_blk, key_blk, preferred_element_type=jnp.float32)
        * key_scale
    )
    weights = scores * jnp.exp(offsets - local_top[:, :, None])
    numerator = jnp.einsum(
        "hts,hsv->htv", weights.astype(jnp.bfloat16), value_blk, preferred_element_type=jnp.float32
    )
    denominator = jnp.sum(weights, axis=-1)
    return (running, local_top, numerator, denominator)


def read_out(query_blk, memory, running, local_top, numerator, denominator):
    matrix, vector, peak = memory
    query_wide = query_blk.astype(jnp.float32)
    carried = running + peak[:, None]
    highest = jnp.maximum(local_top, carried)
    inner_w = jnp.exp(local_top - highest)
    carried_w = jnp.exp(carried - highest)
    numer_all = inner_w[:, :, None] * numerator + carried_w[:, :, None] * jnp.einsum(
        "htd,hdv->htv", query_wide, matrix, precision=lax.Precision.HIGHEST
    )
    denom_all = inner_w * denominator + carried_w * jnp.einsum(
        "htd,hd->ht", query_wide, vector, precision=lax.Precision.HIGHEST
    )
    return numer_all / jnp.maximum(jnp.abs(denom_all), den_floor)[:, :, None]


def advance(memory, key_blk, value_blk, gate_blk, running):
    matrix, vector, peak = memory
    key_wide = key_blk.astype(jnp.float32) * DQK ** (-0.5)
    block_sum = running[:, -1]
    growth = block_sum[:, None] - running + gate_blk
    peak_new = jnp.maximum(block_sum + peak, jnp.max(growth, axis=-1))
    fading = jnp.exp(block_sum + peak - peak_new)
    writes = jnp.exp(growth - peak_new[:, None])
    weighted = (key_wide * writes[:, :, None]).astype(jnp.bfloat16)
    matrix_new = fading[:, None, None] * matrix + jnp.einsum(
        "hsd,hsv->hdv", weighted, value_blk, preferred_element_type=jnp.float32
    )
    vector_new = fading[:, None] * vector + jnp.einsum(
        "hs,hsd->hd", writes, key_wide, precision=lax.Precision.HIGHEST
    )
    return (matrix_new, vector_new, peak_new)


def by_states(
    queries,
    keys,
    values,
    output_gate_logits,
    input_gate_log,
    forget_gate_logits,
    extra_log_decay,
    cell_output_weight,
    residual_input,
    cell_norm_gain,
    expert_before_gain,
    expert_after_gain,
    routes,
    chosen_expert_weight,
    expert_gate_weight,
    expert_up_weight,
    expert_down_weight,
):
    segment = queries.shape[0]
    head_count = queries.shape[1] // DQK
    block_count = segment // BLOCK

    def split_heads(array, width):
        return array.reshape(block_count, BLOCK, head_count, width).transpose(0, 2, 1, 3)

    query_blocks = split_heads(queries, DQK)
    key_blocks = split_heads(keys, DQK)
    value_blocks = split_heads(values, DV)
    forget_log_value = jax.nn.log_sigmoid(forget_gate_logits) + extra_log_decay
    gate_blocks = input_gate_log.reshape(block_count, BLOCK, head_count).transpose(0, 2, 1)
    forget_blocks = forget_log_value.reshape(block_count, BLOCK, head_count).transpose(0, 2, 1)
    totals = jnp.sum(forget_log_value, axis=0)
    zero_matrix = jnp.zeros((head_count, DQK, DV), jnp.float32)
    zero_vector = jnp.zeros((head_count, DQK), jnp.float32)
    zero_heads = jnp.zeros((head_count,), jnp.float32)
    fresh = (zero_matrix, zero_vector, jnp.full((head_count,), very_low, jnp.float32))
    empty = (zero_heads,) + fresh
    anchor = (zero_heads, zero_matrix, zero_vector, zero_heads)

    def summarize(memory, inputs):
        key_blk, value_blk, gate_blk, forget_blk = inputs
        return (
            advance(memory, key_blk, value_blk, gate_blk, jnp.cumsum(forget_blk, axis=-1)),
            None,
        )

    own_state, unused = lax.scan(
        summarize, fresh, (key_blocks, value_blocks, gate_blocks, forget_blocks)
    )
    prefix = carried_in((totals,) + own_state, "sp", combine_states, empty)
    start_full = combine_states(anchor, prefix)

    def emit(memory, inputs):
        query_blk, key_blk, value_blk, gate_blk, forget_blk = inputs
        running, local_top, numerator, denominator = block_local(
            query_blk, key_blk, value_blk, gate_blk, forget_blk
        )
        outcome = read_out(query_blk, memory, running, local_top, numerator, denominator)
        return (advance(memory, key_blk, value_blk, gate_blk, running), outcome)

    unused, heads_out = lax.scan(
        emit, start_full[1:], (query_blocks, key_blocks, value_blocks, gate_blocks, forget_blocks)
    )
    cell_out = heads_out.transpose(0, 2, 1, 3).reshape(segment, head_count * DV)
    gated = (cell_out * jax.nn.sigmoid(output_gate_logits.astype(jnp.float32))).astype(jnp.bfloat16)
    whole_weight = lax.all_gather(cell_output_weight, "sp", axis=1, tiled=True)
    mixed = lax.psum_scatter(
        jnp.dot(gated, whole_weight, preferred_element_type=jnp.float32).astype(jnp.bfloat16),
        "tp",
        scatter_dimension=0,
        tiled=True,
    ).astype(jnp.float32)
    stream = (residual_input.astype(jnp.float32) + rms_scale(mixed, cell_norm_gain)).astype(
        jnp.bfloat16
    )
    normed = rms_scale(stream.astype(jnp.float32), expert_before_gain).astype(jnp.bfloat16)
    normed_all = lax.all_gather(normed, "tp", axis=0, tiled=True)
    sources = lax.axis_size("sp")
    top_count = routes.shape[1]
    capacity = max(2, min(segment, 5 * segment * top_count // (4 * sources)))
    width = normed_all.shape[1]
    labels = lax.broadcasted_iota(jnp.int32, (1, 1, sources), 2)
    matches = (routes[:, :, None] == labels).astype(jnp.int32)
    per_row = jnp.sum(matches, axis=1)
    before_rows = jnp.cumsum(per_row, axis=0) - per_row
    places = jnp.sum(matches * before_rows[:, None, :], axis=2)
    slot_of = routes * capacity + places
    slot_ids = lax.broadcasted_iota(jnp.int32, (sources * capacity, 1, 1), 0)
    picker = jnp.sum((slot_of[None, :, :] == slot_ids).astype(jnp.int32), axis=2).astype(
        jnp.bfloat16
    )
    buffer = jnp.dot(picker, normed_all, preferred_element_type=jnp.float32).astype(jnp.bfloat16)
    buffer = buffer.reshape(sources, capacity, width)
    arrived = lax.all_to_all(buffer, "sp", split_axis=0, concat_axis=0, tiled=True)
    flattened = arrived.reshape(-1, width)
    gate_proj = jnp.dot(flattened, expert_gate_weight[0], preferred_element_type=jnp.float32)
    up_proj = jnp.dot(flattened, expert_up_weight[0], preferred_element_type=jnp.float32)
    hidden = (jax.nn.silu(gate_proj) * up_proj).astype(jnp.bfloat16)
    hidden_whole = lax.all_gather(hidden, "tp", axis=1, tiled=True)
    expert_out = jnp.dot(
        hidden_whole, expert_down_weight[0], preferred_element_type=jnp.float32
    ).astype(jnp.bfloat16)
    results = expert_out.reshape(arrived.shape[0], arrived.shape[1], expert_out.shape[1])
    returned = lax.all_to_all(results, "sp", split_axis=0, concat_axis=0, tiled=True)
    flat = returned.reshape(sources * capacity, returned.shape[2])
    routed_part = jnp.zeros((segment, flat.shape[1]), jnp.float32)
    for route_idx in range(top_count):
        routed_part = (
            routed_part
            + flat[slot_of[:, route_idx]].astype(jnp.float32)
            * chosen_expert_weight[:, route_idx][:, None]
        )
    moe_columns = routed_part.astype(jnp.bfloat16)
    moe_rows = lax.all_to_all(moe_columns, "tp", split_axis=0, concat_axis=1, tiled=True)
    return (
        stream.astype(jnp.float32) + rms_scale(moe_rows.astype(jnp.float32), expert_after_gain)
    ).astype(jnp.bfloat16)


def swap(array, axis, bits):
    return lax.ppermute(array, axis, [(i, i ^ bits) for i in range(lax.axis_size(axis))])


def hop(array, chips, share, step):
    pairs = [
        (chip * share + core, (chip + step) % chips * share + core)
        for chip in range(chips)
        for core in range(share)
    ]
    return lax.ppermute(array, "sp", pairs)


def shift(array, chips, share, step):
    pairs = [
        (chip * share + core, (chip + step) * share + core)
        for chip in range(chips)
        for core in range(share)
        if 0 <= chip + step < chips
    ]
    return lax.ppermute(array, "sp", pairs)


def spread(array, chip, chips, share):
    if chips != 4:
        return [
            (hop(array, chips, share, step) if step else array, (chip - step) % chips)
            for step in range(chips)
        ]
    across = hop(array, chips, share, 2)
    upward = shift(array, chips, share, 1)
    downward = shift(array, chips, share, -1)
    pairs = [(at * share + core, to * share + core) for at, to in ((2, 3), (1, 0)) for core in range(share)]
    onward = lax.ppermute(across, "sp", pairs)
    last = chips - 1
    return [
        (array, chip),
        (upward, jnp.maximum(chip - 1, 0)),
        (downward, jnp.minimum(chip + 1, last)),
        (across, (chip + 2) % chips),
        (onward, jnp.where(chip == 0, last, 0)),
    ]


def contract(left, right, dims):
    return lax.dot_general(left, right, ((dims[:1], dims[1:]), ((), ())), preferred_element_type=jnp.float32)


def pack_kernel(
    spot_ref, query_ref, key_ref, value_ref, logit_ref, input_ref, forget_ref, decay_ref, routes_ref,
    weights_ref, *out_refs
):
    rows = query_ref.shape[0]
    chips = len(out_refs)
    wide = value_ref.shape[1] // (2 * chips)
    chip, core = spot_ref[0], spot_ref[1]

    def pieces_of(array):
        high = lax.reduce_precision(array, 8, 7)
        rest = array - high
        middle = lax.reduce_precision(rest, 8, 7)
        return [high, middle, rest - middle]

    logits = forget_ref[...]
    forget = jnp.minimum(logits, 0.0) - jnp.log1p(jnp.exp(-jnp.abs(logits))) + decay_ref[...]
    gates = pieces_of(forget) + pieces_of(input_ref[...])
    told = [routes_ref[...].astype(jnp.float32)] + pieces_of(weights_ref[...])
    heads = gates[0].shape[0]
    tops = told[0].shape[0]
    for step, out_ref in enumerate(out_refs):
        head = (chip + step) % chips
        query_at = pl.multiple_of(head * DQK, DQK)
        out_ref[:rows, 2 * wide : 2 * wide + DQK] = query_ref[:, pl.ds(query_at, DQK)]
        out_ref[:rows, 2 * wide + DQK : 2 * wide + 2 * DQK] = key_ref[:, pl.ds(query_at, DQK)]
        for turn in range(2):
            value_at = pl.multiple_of((2 * head + (core ^ turn)) * wide, wide)
            base = turn * (2 * wide + 2 * DQK)
            out_ref[:rows, base : base + wide] = value_ref[:, pl.ds(value_at, wide)]
            out_ref[:rows, base + wide : base + 2 * wide] = logit_ref[:, pl.ds(value_at, wide)]
        mine = lax.broadcasted_iota(jnp.int32, (heads, rows), 0) == head
        lines = [jnp.sum(jnp.where(mine, gate, 0.0), axis=0, keepdims=True) for gate in gates]
        lines = lines + [line[i : i + 1] for line in told for i in range(tops)]
        spare = jnp.zeros((1, rows), jnp.float32)
        slots = (out_ref.shape[1] - 2 * wide) // rows
        filled = lines[:6] + [spare] * (slots - 6) + lines[6:]
        filled = filled + [spare] * (8 * slots - len(filled))
        for slot in range(slots):
            column = jnp.concatenate([filled[r * slots + slot] for r in range(8)], axis=0)
            at = 2 * wide + slot * rows
            out_ref[rows:, at : at + rows] = column.astype(jnp.bfloat16)


def cell_kernel(short, spot_ref, *refs):
    chips = (len(refs) - 7) // 2
    even_ref, odd_ref, routes_ref, weights_ref, data_ref, forget_ref, gate_ref = refs[2 * chips :]
    count = 2 * chips
    wide = even_ref.shape[1]
    rows = 2 * even_ref.shape[0] // count
    tops = routes_ref.shape[1]
    chip, core = spot_ref[0], spot_ref[1]
    for step in range(chips):
        origin = (chip + chips - step) % chips
        mine_ref, other_ref = refs[step], refs[chips + step]
        for ref, base, values_at, spot in (
            (mine_ref, 2 * wide, 0, 2 * origin + core),
            (other_ref, 0, 2 * DQK, 2 * origin + 1 - core),
        ):
            data_ref[spot, :, : 2 * DQK] = ref[:rows, base : base + 2 * DQK]
            data_ref[spot, :, 2 * DQK :] = ref[:rows, values_at : values_at + 2 * wide]
            slots = 2 * (wide + DQK) // rows
            extra = ref[rows:, base : base + slots * rows].astype(jnp.float32)

            def line(index):
                r, slot = index // slots, index % slots
                return extra[r : r + 1, slot * rows : (slot + 1) * rows]

            forget_ref[pl.ds(spot, 1), :] = line(0) + line(1) + line(2)
            gate_ref[pl.ds(spot, 1), :] = line(3) + line(4) + line(5)
            for i in range(tops):
                routes_ref[spot, i : i + 1, :] = line(slots + i).astype(jnp.int32)
                weights_ref[spot, i : i + 1, :] = (
                    line(slots + tops + i) + line(slots + 2 * tops + i) + line(slots + 3 * tops + i)
                )
    square = (rows, rows)
    first = lax.broadcasted_iota(jnp.int32, square, 0)
    second = lax.broadcasted_iota(jnp.int32, square, 1)
    lower = first >= second
    running = jnp.dot(
        forget_ref[...],
        (first <= second).astype(jnp.float32),
        precision=lax.Precision.HIGHEST,
        preferred_element_type=jnp.float32,
    )
    base = jnp.zeros((1, 1), jnp.float32)
    top = jnp.zeros((1, 1), jnp.float32)
    levels, tops = [], []
    for j in range(count):
        level = gate_ref[j : j + 1, :] - (running[j : j + 1, :] + base)
        levels.append(level)
        tops.append(top)
        base = base + running[j : j + 1, rows - 1 : rows]
        top = jnp.maximum(top, jnp.max(level, axis=1, keepdims=True))
    for i in range(count):
        query = data_ref[i, :, :DQK]
        masked = jnp.where(lower, levels[i], very_low)
        peak = jnp.maximum(tops[i], jnp.max(masked, axis=1, keepdims=True))
        numer = jnp.zeros((rows, wide), jnp.float32)
        denom = jnp.zeros((rows, 1), jnp.float32)
        for j in range(i + 1):
            scores = contract(query, data_ref[j, :, DQK : 2 * DQK], (1, 1))
            level = masked if j == i else levels[j]
            weights = scores * DQK ** (-0.5) * jnp.exp(level - peak)
            denom = denom + jnp.sum(weights, axis=1, keepdims=True)
            numer = numer + contract(
                weights.astype(jnp.bfloat16), data_ref[j, :, 2 * DQK : 2 * DQK + wide], (1, 0)
            )
        logits = data_ref[i, :, 2 * DQK + wide :].astype(jnp.float32)
        outcome = numer / jnp.maximum(jnp.abs(denom), den_floor) / (1.0 + jnp.exp(-logits))
        outcome = outcome.astype(jnp.bfloat16)
        for j in range(rows // (2 * short)):
            to = (i * rows // 2) + j * short
            even_ref[to : to + short] = outcome[2 * j * short : (2 * j + 1) * short]
            odd_ref[to : to + short] = outcome[(2 * j + 1) * short : (2 * j + 2) * short]


def picker_of(routes, expert, capacity):
    length = routes.shape[1]
    hit = jnp.max((routes == expert).astype(jnp.float32), axis=0, keepdims=True)
    before = lax.broadcasted_iota(jnp.int32, (length, length), 0) < lax.broadcasted_iota(
        jnp.int32, (length, length), 1
    )
    rank = contract(
        jnp.broadcast_to(hit, (8, length)).astype(jnp.bfloat16), before.astype(jnp.bfloat16), (1, 0)
    )[:1]
    slots = lax.broadcasted_iota(jnp.int32, (capacity, length), 0).astype(jnp.float32)
    return jnp.where((rank == slots) & (hit > 0.0), 1.0, 0.0).astype(jnp.bfloat16)


def select_kernel(steps, chips, spot_ref, routes_ref, *refs):
    own_ref, other_ref = refs[-2:]
    pieces = refs[:-2]
    sides = len(pieces) // 2
    capacity = own_ref.shape[0] // 2
    length = routes_ref.shape[2]
    short, width = pieces[0].shape
    block = width // 8
    chip, core, side = spot_ref[0], spot_ref[1], spot_ref[2]
    expert = 2 * chip + core
    from_index = lax.broadcasted_iota(jnp.int32, (length, length), 0)
    to_index = lax.broadcasted_iota(jnp.int32, (length, length), 1)
    turned = from_index == ((to_index // short) ^ side) * short + to_index % short
    for part, step in enumerate(steps):
        routes = routes_ref[2 * ((chip + chips - step) % chips) + core]
        picker = jnp.concatenate(
            [picker_of(routes, expert ^ turn, capacity) for turn in range(2)], axis=0
        )
        picker = contract(picker, turned.astype(jnp.bfloat16), (1, 0)).astype(jnp.bfloat16)
        rows = slice(part * capacity, (part + 1) * capacity)
        for at in range(0, width, block):
            columns = slice(at, at + block)
            here = jnp.concatenate(
                [piece[:, columns] for piece in pieces[part * sides : (part + 1) * sides]]
            )
            picked = contract(picker, here, (1, 0)).astype(jnp.bfloat16)
            own_ref[rows, columns] = picked[:capacity]
            other_ref[rows, columns] = picked[capacity:]


def combine_kernel(steps, chips, spot_ref, routes_ref, weights_ref, own_ref, other_ref, *out_refs):
    chip, core = spot_ref[0], spot_ref[1]
    expert = 2 * chip + core
    capacity = other_ref.shape[0] // 2
    length = routes_ref.shape[2]
    first = lax.broadcasted_iota(jnp.int32, (length, length), 0)
    second = lax.broadcasted_iota(jnp.int32, (length, length), 1)
    same, before = first == second, second < first
    slots = lax.broadcasted_iota(jnp.int32, (length, capacity), 1).astype(jnp.float32)
    for part, (step, out_ref) in enumerate(zip(steps, out_refs)):
        at = 2 * ((chip + chips - step) % chips) + core
        routes = routes_ref[at]
        scales = weights_ref[at]
        total = jnp.zeros(out_ref.shape, jnp.float32)
        for rows_ref, wanted in ((own_ref, expert), (other_ref, expert ^ 1)):
            hit = jnp.max((routes == wanted).astype(jnp.float32), axis=0, keepdims=True)
            rank = jnp.sum(jnp.where(before, hit, 0.0), axis=1, keepdims=True)
            hit = jnp.sum(jnp.where(same, hit, 0.0), axis=1, keepdims=True)
            picker = jnp.where((rank == slots) & (hit > 0.0), 1.0, 0.0).astype(jnp.bfloat16)
            scale_row = jnp.sum(jnp.where(routes == wanted, scales, 0.0), axis=0, keepdims=True)
            scale = jnp.sum(jnp.where(same, scale_row, 0.0), axis=1, keepdims=True)
            spread_rows = contract(picker, rows_ref[part * capacity : (part + 1) * capacity, :], (1, 0))
            total = total + scale * spread_rows
        out_ref[...] = total.astype(jnp.bfloat16)


def norm_kernel(
    spot_ref, kept_a, got_a, kept_b, got_b, residual_ref, gain_ref, next_ref, stream_ref, normed_ref,
    mixed_ref
):
    chip, core = spot_ref[0], spot_ref[1]
    chips, short, block = kept_a.shape
    for at, kept, got in ((0, kept_a, got_a), (short, kept_b, got_b)):
        for step in range(chips):
            origin = 2 * ((chip + chips - step) % chips)
            for ref, index in ((kept, origin + core), (got, origin + 1 - core)):
                where = pl.ds(pl.multiple_of(index * block, block), block)
                mixed_ref[at : at + short, where] = ref[step].astype(jnp.float32)
    stream = residual_ref[...].astype(jnp.float32) + rms_scale(mixed_ref[...], gain_ref[...])
    stream = stream.astype(jnp.bfloat16)
    stream_ref[...] = stream
    normed_ref[...] = rms_scale(stream.astype(jnp.float32), next_ref[...]).astype(jnp.bfloat16)


def last_kernel(spot_ref, stream_ref, gain_ref, *refs):
    out_ref, rows_ref = refs[-2:]
    block = refs[0].shape[1]
    for bits, ref in enumerate(refs[:-2]):
        where = pl.ds(pl.multiple_of((spot_ref[2] ^ bits) * block, block), block)
        rows_ref[:, where] = ref[...].astype(jnp.float32)
    out = stream_ref[...].astype(jnp.float32) + rms_scale(rows_ref[...], gain_ref[...])
    out_ref[...] = out.astype(jnp.bfloat16)


def smem():
    return pl.BlockSpec(memory_space=pltpu.SMEM)


def vmem(count):
    return [pl.BlockSpec(memory_space=pltpu.VMEM)] * count


def by_heads(
    queries,
    keys,
    values,
    output_gate_logits,
    input_gate_log,
    forget_gate_logits,
    extra_log_decay,
    cell_output_weight,
    residual_input,
    cell_norm_gain,
    expert_before_gain,
    expert_after_gain,
    routes,
    chosen_expert_weight,
    expert_gate_weight,
    expert_up_weight,
    expert_down_weight,
):
    segment = queries.shape[0]
    sources = lax.axis_size("sp")
    sides = lax.axis_size("tp")
    place = lax.axis_index("sp")
    side = lax.axis_index("tp")
    head_count = queries.shape[1] // DQK
    share = sources // head_count
    chips = sources // share
    chip, core = place // share, place % share
    wide = DV // share
    top_count = routes.shape[1]
    capacity = max(2, min(segment, 5 * segment * top_count // (4 * sources)))
    spot = jnp.stack([chip, core, side]).astype(jnp.int32)
    line = 2 * DQK + 4 * wide
    packed = pl.pallas_call(
        pack_kernel,
        in_specs=[smem()] + vmem(9),
        out_specs=vmem(chips),
        out_shape=[jax.ShapeDtypeStruct((segment + 8, line), jnp.bfloat16)] * chips,
        name="pack",
    )(
        spot,
        queries,
        keys,
        values,
        output_gate_logits,
        input_gate_log.T,
        forget_gate_logits.T,
        extra_log_decay.T,
        routes.T,
        chosen_expert_weight.T,
    )
    mine = [hop(block, chips, share, step) if step else block for step, block in enumerate(packed)]
    other = [swap(block[:, 2 * wide :], "sp", 1) for block in mine]
    short = segment // (2 * sides)
    half_rows = jax.ShapeDtypeStruct((sources * segment // 2, wide), jnp.bfloat16)
    even, odd, all_routes, all_weights = pl.pallas_call(
        partial(cell_kernel, short),
        in_specs=[smem()] + vmem(2 * chips),
        out_specs=vmem(4),
        out_shape=[
            half_rows,
            half_rows,
            jax.ShapeDtypeStruct((sources, top_count, segment), jnp.int32),
            jax.ShapeDtypeStruct((sources, top_count, segment), jnp.float32),
        ],
        scratch_shapes=[
            pltpu.VMEM((sources, segment, 2 * DQK + 2 * wide), jnp.bfloat16),
            pltpu.VMEM((sources, segment), jnp.float32),
            pltpu.VMEM((sources, segment), jnp.float32),
        ],
        name="cell",
    )(spot, *mine, *other)

    def weight_rows(index):
        return lax.dynamic_slice_in_dim(cell_output_weight, index * wide, wide, 0)

    weights_at = {}

    def project(gated, before):
        total = None
        for order, (block, origin) in enumerate(spread(gated, chip, chips, share)):
            for turn, array in enumerate((block, swap(block, "sp", 1))):
                index = share * origin + (1 - core if turn else core)
                if (order, turn) not in weights_at:
                    weights_at[order, turn] = weight_rows(index)
                term = jnp.dot(array, weights_at[order, turn], preferred_element_type=jnp.float32)
                total = term if total is None else total + term
        total = total.astype(jnp.bfloat16).reshape(sources, sides, short, -1)
        if before is not None:
            total, before = lax.optimization_barrier((total, before))
        summed = None
        for bits in range(sides):
            piece = lax.dynamic_index_in_dim(total, side ^ bits, 1, False)
            piece = (swap(piece, "tp", bits) if bits else piece).astype(jnp.float32)
            summed = piece if summed is None else summed + piece
        summed = summed.astype(jnp.bfloat16).reshape(chips, share, short, -1)
        back = []
        for step in range(chips):
            block = lax.dynamic_index_in_dim(summed, (chip + step) % chips, 0, False)
            back.append(hop(block, chips, share, step) if step else block)
        back = jnp.stack(back)
        kept = lax.dynamic_index_in_dim(back, core, 1, False)
        return [kept, swap(lax.dynamic_index_in_dim(back, 1 - core, 1, False), "sp", 1)]

    own_shape = jax.ShapeDtypeStruct(residual_input.shape, jnp.bfloat16)
    parts_e = project(even, None)
    stream, normed = pl.pallas_call(
        norm_kernel,
        in_specs=[smem()] + vmem(7),
        out_specs=vmem(2),
        out_shape=[own_shape, own_shape],
        scratch_shapes=[pltpu.VMEM(residual_input.shape, jnp.float32)],
        name="norm",
    )(
        spot,
        *parts_e,
        *project(odd, parts_e[0]),
        residual_input,
        cell_norm_gain.reshape(1, -1),
        expert_before_gain.reshape(1, -1),
    )

    def down_rows(bits):
        width = expert_down_weight.shape[1] // sides
        return lax.dynamic_slice_in_dim(expert_down_weight[0], (side ^ bits) * width, width, 0)

    down_weights = lax.optimization_barrier([down_rows(bits) for bits in range(sides)])

    def around(array, first):
        pieces = [array]
        bits = first
        for _ in range(sides.bit_length() - 1):
            pieces = pieces + [swap(piece, "tp", bits) for piece in pieces]
            bits = bits * 2 if bits * 2 < sides else 1
        order = [0]
        bits = first
        for _ in range(sides.bit_length() - 1):
            order = order + [place ^ bits for place in order]
            bits = bits * 2 if bits * 2 < sides else 1
        return [pieces[order.index(place)] for place in range(sides)]

    sequence = [0, 1] + list(range(chips - 1, 1, -1))
    steps_of = [tuple(sequence[at : at + 2]) for at in range(0, chips, 2)]
    arrived = {0: normed}
    for step in [step for steps in steps_of for step in steps if step]:
        arrived[step] = hop(normed, chips, share, step)
    gathered = {}
    for steps in steps_of:
        for order, step in enumerate(steps):
            gathered[step] = around(arrived[step], sides // 2 if order % 2 else 1)
    spread_pieces = [[piece for step in steps for piece in gathered[step]] for steps in steps_of]
    width = normed.shape[1]
    hidden_parts = []
    earlier = None
    for steps, pieces in zip(steps_of, spread_pieces):
        if earlier is not None:
            earlier, pieces = lax.optimization_barrier((earlier, pieces))
        own_rows, other_rows = pl.pallas_call(
            partial(select_kernel, steps, chips),
            in_specs=[smem()] + vmem(1 + len(pieces)),
            out_specs=vmem(2),
            out_shape=[jax.ShapeDtypeStruct((2 * capacity, width), jnp.bfloat16)] * 2,
        )(spot, all_routes, *pieces)
        picked = swap(other_rows, "sp", 1)
        rows_in = jnp.concatenate([own_rows, picked], axis=0)
        gate_proj = jnp.dot(rows_in, expert_gate_weight[0], preferred_element_type=jnp.float32)
        up_proj = jnp.dot(rows_in, expert_up_weight[0], preferred_element_type=jnp.float32)
        earlier = (jax.nn.silu(gate_proj) * up_proj).astype(jnp.bfloat16)
        hidden_parts.append(earlier)
    returned = None
    for order, (steps, hidden) in enumerate(zip(steps_of, hidden_parts)):
        expert_out = None
        if order + 1 == len(steps_of) and sides == 4:
            far = swap(hidden, "tp", 3)
            spread_hidden = [hidden, swap(hidden, "tp", 1), swap(hidden, "tp", 2), far]
        else:
            spread_hidden = around(hidden, sides // 2 if order % 2 else 1)
        for bits, piece in enumerate(spread_hidden):
            term = jnp.dot(piece, down_weights[bits], preferred_element_type=jnp.float32)
            expert_out = term if expert_out is None else expert_out + term
        expert_out = expert_out.astype(jnp.bfloat16)
        other_out = swap(expert_out[2 * capacity :], "sp", 1)
        summed = pl.pallas_call(
            partial(combine_kernel, steps, chips),
            in_specs=[smem()] + vmem(4),
            out_specs=vmem(2),
            out_shape=[jax.ShapeDtypeStruct((segment, expert_out.shape[1]), jnp.bfloat16)] * 2,
        )(spot, all_routes, all_weights, expert_out, other_out)
        for array, step in zip(summed, steps):
            back = (hop(array, chips, share, -step) if step else array).astype(jnp.float32)
            returned = back if returned is None else returned + back
    returned = returned.astype(jnp.bfloat16).reshape(sides, 2 * short, -1)
    parts = []
    for bits in range(sides):
        piece = lax.dynamic_index_in_dim(returned, side ^ bits, 0, False)
        parts.append(swap(piece, "tp", bits) if bits else piece)
    return pl.pallas_call(
        last_kernel,
        in_specs=[smem()] + vmem(2 + sides),
        out_specs=vmem(1)[0],
        out_shape=own_shape,
        scratch_shapes=[pltpu.VMEM(residual_input.shape, jnp.float32)],
        name="last",
    )(spot, stream, expert_after_gain.reshape(1, -1), *parts)


def per_device(*arrays):
    queries = arrays[0]
    sources, sides = lax.axis_size("sp"), lax.axis_size("tp")
    head_count = queries.shape[1] // DQK
    pairs = sources == 2 * head_count and head_count % 2 == 0
    powers = sides & (sides - 1) == 0
    if pairs and powers and queries.shape[0] == BLOCK and queries.shape[0] % (32 * sides) == 0:
        return by_heads(*arrays)
    return by_states(*arrays)


def solution(mesh):
    placed = (
        P("sp", "tp"),
        P("sp", "tp"),
        P("sp", "tp"),
        P("sp", "tp"),
        P("sp", "tp"),
        P("sp", "tp"),
        P("sp", "tp"),
        P("tp", "sp"),
        P(("sp", "tp"), None),
        P(),
        P(),
        P(),
        P("sp", None),
        P("sp", None),
        P("sp", None, "tp"),
        P("sp", None, "tp"),
        P("sp", None, "tp"),
    )
    return jax.shard_map(
        per_device, mesh=mesh, in_specs=placed, out_specs=P(("sp", "tp"), None), check_vma=False
    )
```

```python
import jax
import jax.numpy as jnp
from functools import partial
from jax import lax
from jax.experimental import pallas as pl
from jax.experimental.pallas import tpu as pltpu
from jax.sharding import PartitionSpec as P

DQK = 256
DV = 512
BLOCK = 128


norm_eps = 1e-06
very_low = -1e30
den_floor = 8.0


def carried_in(part, axis, combine, identity):
    place = lax.axis_index(axis)
    gathered = jax.tree.map(lambda a: lax.all_gather(a, axis), part)
    state = jax.tree.map(lambda a, e: jnp.zeros_like(a) + jnp.asarray(e, a.dtype), part, identity)

    def one(step, state):
        return combine(
            state, jax.tree.map(lambda a: lax.dynamic_index_in_dim(a, step, 0, False), gathered)
        )

    return lax.fori_loop(0, place, one, state)


def rms_scale(inputs, gain):
    return inputs * lax.rsqrt(jnp.mean(inputs * inputs, axis=-1, keepdims=True) + norm_eps) * gain


def combine_states(earlier, later):
    total_early, matrix_early, vector_early, peak_early = earlier
    total_late, matrix_late, vector_late, peak_late = later
    shifted = total_late + peak_early
    peak = jnp.maximum(shifted, peak_late)
    keep_early = jnp.exp(shifted - peak)
    keep_late = jnp.exp(peak_late - peak)
    return (
        total_early + total_late,
        keep_early[:, None, None] * matrix_early + keep_late[:, None, None] * matrix_late,
        keep_early[:, None] * vector_early + keep_late[:, None] * vector_late,
        peak,
    )


def block_local(query_blk, key_blk, value_blk, gate_blk, forget_blk):
    key_scale = DQK ** (-0.5)
    running = jnp.cumsum(forget_blk, axis=-1)
    length = running.shape[-1]
    lower = lax.broadcasted_iota(jnp.int32, (length, length), 0) >= lax.broadcasted_iota(
        jnp.int32, (length, length), 1
    )
    offsets = jnp.where(
        lower, running[:, :, None] - running[:, None, :] + gate_blk[:, None, :], -jnp.inf
    )
    local_top = jnp.max(offsets, axis=-1)
    scores = (
        jnp.einsum("htd,hsd->hts", query_blk, key_blk, preferred_element_type=jnp.float32)
        * key_scale
    )
    weights = scores * jnp.exp(offsets - local_top[:, :, None])
    numerator = jnp.einsum(
        "hts,hsv->htv", weights.astype(jnp.bfloat16), value_blk, preferred_element_type=jnp.float32
    )
    denominator = jnp.sum(weights, axis=-1)
    return (running, local_top, numerator, denominator)


def read_out(query_blk, memory, running, local_top, numerator, denominator):
    matrix, vector, peak = memory
    query_wide = query_blk.astype(jnp.float32)
    carried = running + peak[:, None]
    highest = jnp.maximum(local_top, carried)
    inner_w = jnp.exp(local_top - highest)
    carried_w = jnp.exp(carried - highest)
    numer_all = inner_w[:, :, None] * numerator + carried_w[:, :, None] * jnp.einsum(
        "htd,hdv->htv", query_wide, matrix, precision=lax.Precision.HIGHEST
    )
    denom_all = inner_w * denominator + carried_w * jnp.einsum(
        "htd,hd->ht", query_wide, vector, precision=lax.Precision.HIGHEST
    )
    return numer_all / jnp.maximum(jnp.abs(denom_all), den_floor)[:, :, None]


def advance(memory, key_blk, value_blk, gate_blk, running):
    matrix, vector, peak = memory
    key_wide = key_blk.astype(jnp.float32) * DQK ** (-0.5)
    block_sum = running[:, -1]
    growth = block_sum[:, None] - running + gate_blk
    peak_new = jnp.maximum(block_sum + peak, jnp.max(growth, axis=-1))
    fading = jnp.exp(block_sum + peak - peak_new)
    writes = jnp.exp(growth - peak_new[:, None])
    weighted = (key_wide * writes[:, :, None]).astype(jnp.bfloat16)
    matrix_new = fading[:, None, None] * matrix + jnp.einsum(
        "hsd,hsv->hdv", weighted, value_blk, preferred_element_type=jnp.float32
    )
    vector_new = fading[:, None] * vector + jnp.einsum(
        "hs,hsd->hd", writes, key_wide, precision=lax.Precision.HIGHEST
    )
    return (matrix_new, vector_new, peak_new)


def by_states(
    queries,
    keys,
    values,
    output_gate_logits,
    input_gate_log,
    forget_gate_logits,
    extra_log_decay,
    cell_output_weight,
    residual_input,
    cell_norm_gain,
    expert_before_gain,
    expert_after_gain,
    routes,
    chosen_expert_weight,
    expert_gate_weight,
    expert_up_weight,
    expert_down_weight,
):
    segment = queries.shape[0]
    head_count = queries.shape[1] // DQK
    block_count = segment // BLOCK

    def split_heads(array, width):
        return array.reshape(block_count, BLOCK, head_count, width).transpose(0, 2, 1, 3)

    query_blocks = split_heads(queries, DQK)
    key_blocks = split_heads(keys, DQK)
    value_blocks = split_heads(values, DV)
    forget_log_value = jax.nn.log_sigmoid(forget_gate_logits) + extra_log_decay
    gate_blocks = input_gate_log.reshape(block_count, BLOCK, head_count).transpose(0, 2, 1)
    forget_blocks = forget_log_value.reshape(block_count, BLOCK, head_count).transpose(0, 2, 1)
    totals = jnp.sum(forget_log_value, axis=0)
    zero_matrix = jnp.zeros((head_count, DQK, DV), jnp.float32)
    zero_vector = jnp.zeros((head_count, DQK), jnp.float32)
    zero_heads = jnp.zeros((head_count,), jnp.float32)
    fresh = (zero_matrix, zero_vector, jnp.full((head_count,), very_low, jnp.float32))
    empty = (zero_heads,) + fresh
    anchor = (zero_heads, zero_matrix, zero_vector, zero_heads)

    def summarize(memory, inputs):
        key_blk, value_blk, gate_blk, forget_blk = inputs
        return (
            advance(memory, key_blk, value_blk, gate_blk, jnp.cumsum(forget_blk, axis=-1)),
            None,
        )

    own_state, unused = lax.scan(
        summarize, fresh, (key_blocks, value_blocks, gate_blocks, forget_blocks)
    )
    prefix = carried_in((totals,) + own_state, "sp", combine_states, empty)
    start_full = combine_states(anchor, prefix)

    def emit(memory, inputs):
        query_blk, key_blk, value_blk, gate_blk, forget_blk = inputs
        running, local_top, numerator, denominator = block_local(
            query_blk, key_blk, value_blk, gate_blk, forget_blk
        )
        outcome = read_out(query_blk, memory, running, local_top, numerator, denominator)
        return (advance(memory, key_blk, value_blk, gate_blk, running), outcome)

    unused, heads_out = lax.scan(
        emit, start_full[1:], (query_blocks, key_blocks, value_blocks, gate_blocks, forget_blocks)
    )
    cell_out = heads_out.transpose(0, 2, 1, 3).reshape(segment, head_count * DV)
    gated = (cell_out * jax.nn.sigmoid(output_gate_logits.astype(jnp.float32))).astype(jnp.bfloat16)
    whole_weight = lax.all_gather(cell_output_weight, "sp", axis=1, tiled=True)
    mixed = lax.psum_scatter(
        jnp.dot(gated, whole_weight, preferred_element_type=jnp.float32).astype(jnp.bfloat16),
        "tp",
        scatter_dimension=0,
        tiled=True,
    ).astype(jnp.float32)
    stream = (residual_input.astype(jnp.float32) + rms_scale(mixed, cell_norm_gain)).astype(
        jnp.bfloat16
    )
    normed = rms_scale(stream.astype(jnp.float32), expert_before_gain).astype(jnp.bfloat16)
    normed_all = lax.all_gather(normed, "tp", axis=0, tiled=True)
    sources = lax.axis_size("sp")
    top_count = routes.shape[1]
    capacity = max(2, min(segment, 5 * segment * top_count // (4 * sources)))
    width = normed_all.shape[1]
    labels = lax.broadcasted_iota(jnp.int32, (1, 1, sources), 2)
    matches = (routes[:, :, None] == labels).astype(jnp.int32)
    per_row = jnp.sum(matches, axis=1)
    before_rows = jnp.cumsum(per_row, axis=0) - per_row
    places = jnp.sum(matches * before_rows[:, None, :], axis=2)
    slot_of = routes * capacity + places
    slot_ids = lax.broadcasted_iota(jnp.int32, (sources * capacity, 1, 1), 0)
    picker = jnp.sum((slot_of[None, :, :] == slot_ids).astype(jnp.int32), axis=2).astype(
        jnp.bfloat16
    )
    buffer = jnp.dot(picker, normed_all, preferred_element_type=jnp.float32).astype(jnp.bfloat16)
    buffer = buffer.reshape(sources, capacity, width)
    arrived = lax.all_to_all(buffer, "sp", split_axis=0, concat_axis=0, tiled=True)
    flattened = arrived.reshape(-1, width)
    gate_proj = jnp.dot(flattened, expert_gate_weight[0], preferred_element_type=jnp.float32)
    up_proj = jnp.dot(flattened, expert_up_weight[0], preferred_element_type=jnp.float32)
    hidden = (jax.nn.silu(gate_proj) * up_proj).astype(jnp.bfloat16)
    hidden_whole = lax.all_gather(hidden, "tp", axis=1, tiled=True)
    expert_out = jnp.dot(
        hidden_whole, expert_down_weight[0], preferred_element_type=jnp.float32
    ).astype(jnp.bfloat16)
    results = expert_out.reshape(arrived.shape[0], arrived.shape[1], expert_out.shape[1])
    returned = lax.all_to_all(results, "sp", split_axis=0, concat_axis=0, tiled=True)
    flat = returned.reshape(sources * capacity, returned.shape[2])
    routed_part = jnp.zeros((segment, flat.shape[1]), jnp.float32)
    for route_idx in range(top_count):
        routed_part = (
            routed_part
            + flat[slot_of[:, route_idx]].astype(jnp.float32)
            * chosen_expert_weight[:, route_idx][:, None]
        )
    moe_columns = routed_part.astype(jnp.bfloat16)
    moe_rows = lax.all_to_all(moe_columns, "tp", split_axis=0, concat_axis=1, tiled=True)
    return (
        stream.astype(jnp.float32) + rms_scale(moe_rows.astype(jnp.float32), expert_after_gain)
    ).astype(jnp.bfloat16)


def swap(array, axis, bits):
    return lax.ppermute(array, axis, [(i, i ^ bits) for i in range(lax.axis_size(axis))])


def hop(array, chips, share, step):
    pairs = [
        (chip * share + core, (chip + step) % chips * share + core)
        for chip in range(chips)
        for core in range(share)
    ]
    return lax.ppermute(array, "sp", pairs)


def shift(array, chips, share, step):
    pairs = [
        (chip * share + core, (chip + step) * share + core)
        for chip in range(chips)
        for core in range(share)
        if 0 <= chip + step < chips
    ]
    return lax.ppermute(array, "sp", pairs)


def spread(array, chip, chips, share):
    if chips != 4:
        return [
            (hop(array, chips, share, step) if step else array, (chip - step) % chips)
            for step in range(chips)
        ]
    across = hop(array, chips, share, 2)
    upward = shift(array, chips, share, 1)
    downward = shift(array, chips, share, -1)
    pairs = [(at * share + core, to * share + core) for at, to in ((2, 3), (1, 0)) for core in range(share)]
    onward = lax.ppermute(across, "sp", pairs)
    last = chips - 1
    return [
        (array, chip),
        (upward, jnp.maximum(chip - 1, 0)),
        (downward, jnp.minimum(chip + 1, last)),
        (across, (chip + 2) % chips),
        (onward, jnp.where(chip == 0, last, 0)),
    ]


def contract(left, right, dims):
    return lax.dot_general(left, right, ((dims[:1], dims[1:]), ((), ())), preferred_element_type=jnp.float32)


def pack_kernel(
    spot_ref, query_ref, key_ref, value_ref, logit_ref, input_ref, forget_ref, decay_ref, routes_ref,
    weights_ref, *out_refs
):
    rows = query_ref.shape[0]
    chips = len(out_refs)
    wide = value_ref.shape[1] // (2 * chips)
    chip, core = spot_ref[0], spot_ref[1]

    def pieces_of(array):
        high = lax.reduce_precision(array, 8, 7)
        rest = array - high
        middle = lax.reduce_precision(rest, 8, 7)
        return [high, middle, rest - middle]

    logits = forget_ref[...]
    forget = jnp.minimum(logits, 0.0) - jnp.log1p(jnp.exp(-jnp.abs(logits))) + decay_ref[...]
    gates = pieces_of(forget) + pieces_of(input_ref[...])
    told = [routes_ref[...].astype(jnp.float32)] + pieces_of(weights_ref[...])
    heads = gates[0].shape[0]
    tops = told[0].shape[0]
    for step, out_ref in enumerate(out_refs):
        head = (chip + step) % chips
        query_at = pl.multiple_of(head * DQK, DQK)
        out_ref[:rows, 2 * wide : 2 * wide + DQK] = query_ref[:, pl.ds(query_at, DQK)]
        out_ref[:rows, 2 * wide + DQK : 2 * wide + 2 * DQK] = key_ref[:, pl.ds(query_at, DQK)]
        for turn in range(2):
            value_at = pl.multiple_of((2 * head + (core ^ turn)) * wide, wide)
            base = turn * (2 * wide + 2 * DQK)
            out_ref[:rows, base : base + wide] = value_ref[:, pl.ds(value_at, wide)]
            out_ref[:rows, base + wide : base + 2 * wide] = logit_ref[:, pl.ds(value_at, wide)]
        mine = lax.broadcasted_iota(jnp.int32, (heads, rows), 0) == head
        lines = [jnp.sum(jnp.where(mine, gate, 0.0), axis=0, keepdims=True) for gate in gates]
        lines = lines + [line[i : i + 1] for line in told for i in range(tops)]
        spare = jnp.zeros((1, rows), jnp.float32)
        slots = (out_ref.shape[1] - 2 * wide) // rows
        filled = lines[:6] + [spare] * (slots - 6) + lines[6:]
        filled = filled + [spare] * (8 * slots - len(filled))
        for slot in range(slots):
            column = jnp.concatenate([filled[r * slots + slot] for r in range(8)], axis=0)
            at = 2 * wide + slot * rows
            out_ref[rows:, at : at + rows] = column.astype(jnp.bfloat16)


def cell_kernel(short, spot_ref, *refs):
    chips = (len(refs) - 7) // 2
    even_ref, odd_ref, routes_ref, weights_ref, data_ref, forget_ref, gate_ref = refs[2 * chips :]
    count = 2 * chips
    wide = even_ref.shape[1]
    rows = 2 * even_ref.shape[0] // count
    tops = routes_ref.shape[1]
    chip, core = spot_ref[0], spot_ref[1]
    for step in range(chips):
        origin = (chip + chips - step) % chips
        mine_ref, other_ref = refs[step], refs[chips + step]
        for ref, base, values_at, spot in (
            (mine_ref, 2 * wide, 0, 2 * origin + core),
            (other_ref, 0, 2 * DQK, 2 * origin + 1 - core),
        ):
            data_ref[spot, :, : 2 * DQK] = ref[:rows, base : base + 2 * DQK]
            data_ref[spot, :, 2 * DQK :] = ref[:rows, values_at : values_at + 2 * wide]
            slots = 2 * (wide + DQK) // rows
            extra = ref[rows:, base : base + slots * rows].astype(jnp.float32)

            def line(index):
                r, slot = index // slots, index % slots
                return extra[r : r + 1, slot * rows : (slot + 1) * rows]

            forget_ref[pl.ds(spot, 1), :] = line(0) + line(1) + line(2)
            gate_ref[pl.ds(spot, 1), :] = line(3) + line(4) + line(5)
            for i in range(tops):
                routes_ref[spot, i : i + 1, :] = line(slots + i).astype(jnp.int32)
                weights_ref[spot, i : i + 1, :] = (
                    line(slots + tops + i) + line(slots + 2 * tops + i) + line(slots + 3 * tops + i)
                )
    square = (rows, rows)
    first = lax.broadcasted_iota(jnp.int32, square, 0)
    second = lax.broadcasted_iota(jnp.int32, square, 1)
    lower = first >= second
    running = jnp.dot(
        forget_ref[...],
        (first <= second).astype(jnp.float32),
        precision=lax.Precision.HIGHEST,
        preferred_element_type=jnp.float32,
    )
    base = jnp.zeros((1, 1), jnp.float32)
    top = jnp.zeros((1, 1), jnp.float32)
    levels, tops = [], []
    for j in range(count):
        level = gate_ref[j : j + 1, :] - (running[j : j + 1, :] + base)
        levels.append(level)
        tops.append(top)
        base = base + running[j : j + 1, rows - 1 : rows]
        top = jnp.maximum(top, jnp.max(level, axis=1, keepdims=True))
    for i in range(count):
        query = data_ref[i, :, :DQK]
        masked = jnp.where(lower, levels[i], very_low)
        peak = jnp.maximum(tops[i], jnp.max(masked, axis=1, keepdims=True))
        numer = jnp.zeros((rows, wide), jnp.float32)
        denom = jnp.zeros((rows, 1), jnp.float32)
        for j in range(i + 1):
            scores = contract(query, data_ref[j, :, DQK : 2 * DQK], (1, 1))
            level = masked if j == i else levels[j]
            weights = scores * DQK ** (-0.5) * jnp.exp(level - peak)
            denom = denom + jnp.sum(weights, axis=1, keepdims=True)
            numer = numer + contract(
                weights.astype(jnp.bfloat16), data_ref[j, :, 2 * DQK : 2 * DQK + wide], (1, 0)
            )
        logits = data_ref[i, :, 2 * DQK + wide :].astype(jnp.float32)
        outcome = numer / jnp.maximum(jnp.abs(denom), den_floor) / (1.0 + jnp.exp(-logits))
        outcome = outcome.astype(jnp.bfloat16)
        for j in range(rows // (2 * short)):
            to = (i * rows // 2) + j * short
            even_ref[to : to + short] = outcome[2 * j * short : (2 * j + 1) * short]
            odd_ref[to : to + short] = outcome[(2 * j + 1) * short : (2 * j + 2) * short]


def picker_of(routes, expert, capacity):
    length = routes.shape[1]
    hit = jnp.max((routes == expert).astype(jnp.float32), axis=0, keepdims=True)
    before = lax.broadcasted_iota(jnp.int32, (length, length), 0) < lax.broadcasted_iota(
        jnp.int32, (length, length), 1
    )
    rank = contract(
        jnp.broadcast_to(hit, (8, length)).astype(jnp.bfloat16), before.astype(jnp.bfloat16), (1, 0)
    )[:1]
    slots = lax.broadcasted_iota(jnp.int32, (capacity, length), 0).astype(jnp.float32)
    return jnp.where((rank == slots) & (hit > 0.0), 1.0, 0.0).astype(jnp.bfloat16)


def select_kernel(steps, chips, spot_ref, routes_ref, *refs):
    own_ref, other_ref = refs[-2:]
    pieces = refs[:-2]
    sides = len(pieces) // len(steps)
    capacity = own_ref.shape[0] // len(steps)
    length = routes_ref.shape[2]
    short, width = pieces[0].shape
    block = width // 8
    chip, core, side = spot_ref[0], spot_ref[1], spot_ref[2]
    expert = 2 * chip + core
    from_index = lax.broadcasted_iota(jnp.int32, (length, length), 0)
    to_index = lax.broadcasted_iota(jnp.int32, (length, length), 1)
    turned = from_index == ((to_index // short) ^ side) * short + to_index % short
    for part, step in enumerate(steps):
        routes = routes_ref[2 * ((chip + chips - step) % chips) + core]
        picker = jnp.concatenate(
            [picker_of(routes, expert ^ turn, capacity) for turn in range(2)], axis=0
        )
        picker = contract(picker, turned.astype(jnp.bfloat16), (1, 0)).astype(jnp.bfloat16)
        rows = slice(part * capacity, (part + 1) * capacity)
        for at in range(0, width, block):
            columns = slice(at, at + block)
            here = jnp.concatenate(
                [piece[:, columns] for piece in pieces[part * sides : (part + 1) * sides]]
            )
            picked = contract(picker, here, (1, 0)).astype(jnp.bfloat16)
            own_ref[rows, columns] = picked[:capacity]
            other_ref[rows, columns] = picked[capacity:]


def combine_kernel(steps, chips, spot_ref, routes_ref, weights_ref, own_ref, other_ref, *out_refs):
    chip, core = spot_ref[0], spot_ref[1]
    expert = 2 * chip + core
    capacity = other_ref.shape[0] // len(steps)
    length = routes_ref.shape[2]
    first = lax.broadcasted_iota(jnp.int32, (length, length), 0)
    second = lax.broadcasted_iota(jnp.int32, (length, length), 1)
    same, before = first == second, second < first
    slots = lax.broadcasted_iota(jnp.int32, (length, capacity), 1).astype(jnp.float32)
    for part, (step, out_ref) in enumerate(zip(steps, out_refs)):
        at = 2 * ((chip + chips - step) % chips) + core
        routes = routes_ref[at]
        scales = weights_ref[at]
        total = jnp.zeros(out_ref.shape, jnp.float32)
        for rows_ref, wanted in ((own_ref, expert), (other_ref, expert ^ 1)):
            hit = jnp.max((routes == wanted).astype(jnp.float32), axis=0, keepdims=True)
            rank = jnp.sum(jnp.where(before, hit, 0.0), axis=1, keepdims=True)
            hit = jnp.sum(jnp.where(same, hit, 0.0), axis=1, keepdims=True)
            picker = jnp.where((rank == slots) & (hit > 0.0), 1.0, 0.0).astype(jnp.bfloat16)
            scale_row = jnp.sum(jnp.where(routes == wanted, scales, 0.0), axis=0, keepdims=True)
            scale = jnp.sum(jnp.where(same, scale_row, 0.0), axis=1, keepdims=True)
            spread_rows = contract(picker, rows_ref[part * capacity : (part + 1) * capacity, :], (1, 0))
            total = total + scale * spread_rows
        out_ref[...] = total.astype(jnp.bfloat16)


def norm_kernel(
    spot_ref, kept_a, got_a, kept_b, got_b, residual_ref, gain_ref, next_ref, stream_ref, normed_ref,
    mixed_ref
):
    chip, core = spot_ref[0], spot_ref[1]
    chips, short, block = kept_a.shape
    for at, kept, got in ((0, kept_a, got_a), (short, kept_b, got_b)):
        for step in range(chips):
            origin = 2 * ((chip + chips - step) % chips)
            for ref, index in ((kept, origin + core), (got, origin + 1 - core)):
                where = pl.ds(pl.multiple_of(index * block, block), block)
                mixed_ref[at : at + short, where] = ref[step].astype(jnp.float32)
    stream = residual_ref[...].astype(jnp.float32) + rms_scale(mixed_ref[...], gain_ref[...])
    stream = stream.astype(jnp.bfloat16)
    stream_ref[...] = stream
    normed_ref[...] = rms_scale(stream.astype(jnp.float32), next_ref[...]).astype(jnp.bfloat16)


def last_kernel(spot_ref, stream_ref, gain_ref, *refs):
    out_ref, rows_ref = refs[-2:]
    block = refs[0].shape[1]
    for bits, ref in enumerate(refs[:-2]):
        where = pl.ds(pl.multiple_of((spot_ref[2] ^ bits) * block, block), block)
        rows_ref[:, where] = ref[...].astype(jnp.float32)
    out = stream_ref[...].astype(jnp.float32) + rms_scale(rows_ref[...], gain_ref[...])
    out_ref[...] = out.astype(jnp.bfloat16)


def smem():
    return pl.BlockSpec(memory_space=pltpu.SMEM)


def vmem(count):
    return [pl.BlockSpec(memory_space=pltpu.VMEM)] * count


def by_heads(
    queries,
    keys,
    values,
    output_gate_logits,
    input_gate_log,
    forget_gate_logits,
    extra_log_decay,
    cell_output_weight,
    residual_input,
    cell_norm_gain,
    expert_before_gain,
    expert_after_gain,
    routes,
    chosen_expert_weight,
    expert_gate_weight,
    expert_up_weight,
    expert_down_weight,
):
    segment = queries.shape[0]
    sources = lax.axis_size("sp")
    sides = lax.axis_size("tp")
    place = lax.axis_index("sp")
    side = lax.axis_index("tp")
    head_count = queries.shape[1] // DQK
    share = sources // head_count
    chips = sources // share
    chip, core = place // share, place % share
    wide = DV // share
    top_count = routes.shape[1]
    capacity = max(2, min(segment, 5 * segment * top_count // (4 * sources)))
    spot = jnp.stack([chip, core, side]).astype(jnp.int32)
    line = 2 * DQK + 4 * wide
    packed = pl.pallas_call(
        pack_kernel,
        in_specs=[smem()] + vmem(9),
        out_specs=vmem(chips),
        out_shape=[jax.ShapeDtypeStruct((segment + 8, line), jnp.bfloat16)] * chips,
        name="pack",
    )(
        spot,
        queries,
        keys,
        values,
        output_gate_logits,
        input_gate_log.T,
        forget_gate_logits.T,
        extra_log_decay.T,
        routes.T,
        chosen_expert_weight.T,
    )
    mine = [hop(block, chips, share, step) if step else block for step, block in enumerate(packed)]
    other = [swap(block[:, 2 * wide :], "sp", 1) for block in mine]
    short = segment // (2 * sides)
    half_rows = jax.ShapeDtypeStruct((sources * segment // 2, wide), jnp.bfloat16)
    even, odd, all_routes, all_weights = pl.pallas_call(
        partial(cell_kernel, short),
        in_specs=[smem()] + vmem(2 * chips),
        out_specs=vmem(4),
        out_shape=[
            half_rows,
            half_rows,
            jax.ShapeDtypeStruct((sources, top_count, segment), jnp.int32),
            jax.ShapeDtypeStruct((sources, top_count, segment), jnp.float32),
        ],
        scratch_shapes=[
            pltpu.VMEM((sources, segment, 2 * DQK + 2 * wide), jnp.bfloat16),
            pltpu.VMEM((sources, segment), jnp.float32),
            pltpu.VMEM((sources, segment), jnp.float32),
        ],
        name="cell",
    )(spot, *mine, *other)

    def weight_rows(index):
        return lax.dynamic_slice_in_dim(cell_output_weight, index * wide, wide, 0)

    weights_at = {}

    def project(gated, before):
        total = None
        for order, (block, origin) in enumerate(spread(gated, chip, chips, share)):
            for turn, array in enumerate((block, swap(block, "sp", 1))):
                index = share * origin + (1 - core if turn else core)
                if (order, turn) not in weights_at:
                    weights_at[order, turn] = weight_rows(index)
                term = jnp.dot(array, weights_at[order, turn], preferred_element_type=jnp.float32)
                total = term if total is None else total + term
        total = total.astype(jnp.bfloat16).reshape(sources, sides, short, -1)
        if before is not None:
            total, before = lax.optimization_barrier((total, before))
        summed = None
        for bits in range(sides):
            piece = lax.dynamic_index_in_dim(total, side ^ bits, 1, False)
            piece = (swap(piece, "tp", bits) if bits else piece).astype(jnp.float32)
            summed = piece if summed is None else summed + piece
        summed = summed.astype(jnp.bfloat16).reshape(chips, share, short, -1)
        back = []
        for step in range(chips):
            block = lax.dynamic_index_in_dim(summed, (chip + step) % chips, 0, False)
            back.append(hop(block, chips, share, step) if step else block)
        back = jnp.stack(back)
        kept = lax.dynamic_index_in_dim(back, core, 1, False)
        return [kept, swap(lax.dynamic_index_in_dim(back, 1 - core, 1, False), "sp", 1)]

    own_shape = jax.ShapeDtypeStruct(residual_input.shape, jnp.bfloat16)
    parts_e = project(even, None)
    stream, normed = pl.pallas_call(
        norm_kernel,
        in_specs=[smem()] + vmem(7),
        out_specs=vmem(2),
        out_shape=[own_shape, own_shape],
        scratch_shapes=[pltpu.VMEM(residual_input.shape, jnp.float32)],
        name="norm",
    )(
        spot,
        *parts_e,
        *project(odd, parts_e[0]),
        residual_input,
        cell_norm_gain.reshape(1, -1),
        expert_before_gain.reshape(1, -1),
    )

    def down_rows(bits):
        width = expert_down_weight.shape[1] // sides
        return lax.dynamic_slice_in_dim(expert_down_weight[0], (side ^ bits) * width, width, 0)

    down_weights = lax.optimization_barrier([down_rows(bits) for bits in range(sides)])

    def around(array, first):
        pieces = [array]
        bits = first
        for _ in range(sides.bit_length() - 1):
            pieces = pieces + [swap(piece, "tp", bits) for piece in pieces]
            bits = bits * 2 if bits * 2 < sides else 1
        order = [0]
        bits = first
        for _ in range(sides.bit_length() - 1):
            order = order + [place ^ bits for place in order]
            bits = bits * 2 if bits * 2 < sides else 1
        return [pieces[order.index(place)] for place in range(sides)]

    middle = chips // 2
    steps_of = [tuple(step for step in range(chips) if step != middle), (middle,)]
    arrived = {0: normed}
    gathered = {}
    for order, step in enumerate([step for steps in steps_of for step in steps]):
        if step:
            arrived[step] = hop(normed, chips, share, step)
        gathered[step] = around(arrived[step], sides // 2 if order % 2 else 1)
    spread_pieces = [[piece for step in steps for piece in gathered[step]] for steps in steps_of]
    width = normed.shape[1]
    hidden_parts = []
    earlier = None
    for steps, pieces in zip(steps_of, spread_pieces):
        if earlier is not None:
            earlier, pieces = lax.optimization_barrier((earlier, pieces))
        own_rows, other_rows = pl.pallas_call(
            partial(select_kernel, steps, chips),
            in_specs=[smem()] + vmem(1 + len(pieces)),
            out_specs=vmem(2),
            out_shape=[jax.ShapeDtypeStruct((len(steps) * capacity, width), jnp.bfloat16)] * 2,
        )(spot, all_routes, *pieces)
        picked = swap(other_rows, "sp", 1)
        rows_in = jnp.concatenate([own_rows, picked], axis=0)
        gate_proj = jnp.dot(rows_in, expert_gate_weight[0], preferred_element_type=jnp.float32)
        up_proj = jnp.dot(rows_in, expert_up_weight[0], preferred_element_type=jnp.float32)
        earlier = (jax.nn.silu(gate_proj) * up_proj).astype(jnp.bfloat16)
        hidden_parts.append(earlier)
    returned = None
    for order, (steps, hidden) in enumerate(zip(steps_of, hidden_parts)):
        expert_out = None
        if order + 1 == len(steps_of) and sides == 4:
            far = swap(hidden, "tp", 3)
            spread_hidden = [hidden, swap(hidden, "tp", 1), swap(hidden, "tp", 2), far]
        else:
            spread_hidden = around(hidden, sides // 2 if order % 2 else 1)
        for bits, piece in enumerate(spread_hidden):
            term = jnp.dot(piece, down_weights[bits], preferred_element_type=jnp.float32)
            expert_out = term if expert_out is None else expert_out + term
        expert_out = expert_out.astype(jnp.bfloat16)
        other_out = swap(expert_out[len(steps) * capacity :], "sp", 1)
        summed = pl.pallas_call(
            partial(combine_kernel, steps, chips),
            in_specs=[smem()] + vmem(4),
            out_specs=vmem(len(steps)),
            out_shape=[jax.ShapeDtypeStruct((segment, expert_out.shape[1]), jnp.bfloat16)] * len(steps),
        )(spot, all_routes, all_weights, expert_out, other_out)
        for array, step in zip(summed, steps):
            back = (hop(array, chips, share, -step) if step else array).astype(jnp.float32)
            returned = back if returned is None else returned + back
    returned = returned.astype(jnp.bfloat16).reshape(sides, 2 * short, -1)
    parts = []
    for bits in range(sides):
        piece = lax.dynamic_index_in_dim(returned, side ^ bits, 0, False)
        parts.append(swap(piece, "tp", bits) if bits else piece)
    return pl.pallas_call(
        last_kernel,
        in_specs=[smem()] + vmem(2 + sides),
        out_specs=vmem(1)[0],
        out_shape=own_shape,
        scratch_shapes=[pltpu.VMEM(residual_input.shape, jnp.float32)],
        name="last",
    )(spot, stream, expert_after_gain.reshape(1, -1), *parts)


def per_device(*arrays):
    queries = arrays[0]
    sources, sides = lax.axis_size("sp"), lax.axis_size("tp")
    head_count = queries.shape[1] // DQK
    pairs = sources == 2 * head_count and head_count % 2 == 0
    powers = sides & (sides - 1) == 0
    if pairs and powers and queries.shape[0] == BLOCK and queries.shape[0] % (32 * sides) == 0:
        return by_heads(*arrays)
    return by_states(*arrays)


def solution(mesh):
    placed = (
        P("sp", "tp"),
        P("sp", "tp"),
        P("sp", "tp"),
        P("sp", "tp"),
        P("sp", "tp"),
        P("sp", "tp"),
        P("sp", "tp"),
        P("tp", "sp"),
        P(("sp", "tp"), None),
        P(),
        P(),
        P(),
        P("sp", None),
        P("sp", None),
        P("sp", None, "tp"),
        P("sp", None, "tp"),
        P("sp", None, "tp"),
    )
    return jax.shard_map(
        per_device, mesh=mesh, in_specs=placed, out_specs=P(("sp", "tp"), None), check_vma=False
    )
```

```python
import jax
import jax.numpy as jnp
from functools import partial
from jax import lax
from jax.experimental import pallas as pl
from jax.experimental.pallas import tpu as pltpu
from jax.sharding import PartitionSpec as P

DQK = 256
DV = 512
BLOCK = 128


norm_eps = 1e-06
very_low = -1e30
den_floor = 8.0


def carried_in(part, axis, combine, identity):
    place = lax.axis_index(axis)
    gathered = jax.tree.map(lambda a: lax.all_gather(a, axis), part)
    state = jax.tree.map(lambda a, e: jnp.zeros_like(a) + jnp.asarray(e, a.dtype), part, identity)

    def one(step, state):
        return combine(
            state, jax.tree.map(lambda a: lax.dynamic_index_in_dim(a, step, 0, False), gathered)
        )

    return lax.fori_loop(0, place, one, state)


def rms_scale(inputs, gain):
    return inputs * lax.rsqrt(jnp.mean(inputs * inputs, axis=-1, keepdims=True) + norm_eps) * gain


def combine_states(earlier, later):
    total_early, matrix_early, vector_early, peak_early = earlier
    total_late, matrix_late, vector_late, peak_late = later
    shifted = total_late + peak_early
    peak = jnp.maximum(shifted, peak_late)
    keep_early = jnp.exp(shifted - peak)
    keep_late = jnp.exp(peak_late - peak)
    return (
        total_early + total_late,
        keep_early[:, None, None] * matrix_early + keep_late[:, None, None] * matrix_late,
        keep_early[:, None] * vector_early + keep_late[:, None] * vector_late,
        peak,
    )


def block_local(query_blk, key_blk, value_blk, gate_blk, forget_blk):
    key_scale = DQK ** (-0.5)
    running = jnp.cumsum(forget_blk, axis=-1)
    length = running.shape[-1]
    lower = lax.broadcasted_iota(jnp.int32, (length, length), 0) >= lax.broadcasted_iota(
        jnp.int32, (length, length), 1
    )
    offsets = jnp.where(
        lower, running[:, :, None] - running[:, None, :] + gate_blk[:, None, :], -jnp.inf
    )
    local_top = jnp.max(offsets, axis=-1)
    scores = (
        jnp.einsum("htd,hsd->hts", query_blk, key_blk, preferred_element_type=jnp.float32)
        * key_scale
    )
    weights = scores * jnp.exp(offsets - local_top[:, :, None])
    numerator = jnp.einsum(
        "hts,hsv->htv", weights.astype(jnp.bfloat16), value_blk, preferred_element_type=jnp.float32
    )
    denominator = jnp.sum(weights, axis=-1)
    return (running, local_top, numerator, denominator)


def read_out(query_blk, memory, running, local_top, numerator, denominator):
    matrix, vector, peak = memory
    query_wide = query_blk.astype(jnp.float32)
    carried = running + peak[:, None]
    highest = jnp.maximum(local_top, carried)
    inner_w = jnp.exp(local_top - highest)
    carried_w = jnp.exp(carried - highest)
    numer_all = inner_w[:, :, None] * numerator + carried_w[:, :, None] * jnp.einsum(
        "htd,hdv->htv", query_wide, matrix, precision=lax.Precision.HIGHEST
    )
    denom_all = inner_w * denominator + carried_w * jnp.einsum(
        "htd,hd->ht", query_wide, vector, precision=lax.Precision.HIGHEST
    )
    return numer_all / jnp.maximum(jnp.abs(denom_all), den_floor)[:, :, None]


def advance(memory, key_blk, value_blk, gate_blk, running):
    matrix, vector, peak = memory
    key_wide = key_blk.astype(jnp.float32) * DQK ** (-0.5)
    block_sum = running[:, -1]
    growth = block_sum[:, None] - running + gate_blk
    peak_new = jnp.maximum(block_sum + peak, jnp.max(growth, axis=-1))
    fading = jnp.exp(block_sum + peak - peak_new)
    writes = jnp.exp(growth - peak_new[:, None])
    weighted = (key_wide * writes[:, :, None]).astype(jnp.bfloat16)
    matrix_new = fading[:, None, None] * matrix + jnp.einsum(
        "hsd,hsv->hdv", weighted, value_blk, preferred_element_type=jnp.float32
    )
    vector_new = fading[:, None] * vector + jnp.einsum(
        "hs,hsd->hd", writes, key_wide, precision=lax.Precision.HIGHEST
    )
    return (matrix_new, vector_new, peak_new)


def by_states(
    queries,
    keys,
    values,
    output_gate_logits,
    input_gate_log,
    forget_gate_logits,
    extra_log_decay,
    cell_output_weight,
    residual_input,
    cell_norm_gain,
    expert_before_gain,
    expert_after_gain,
    routes,
    chosen_expert_weight,
    expert_gate_weight,
    expert_up_weight,
    expert_down_weight,
):
    segment = queries.shape[0]
    head_count = queries.shape[1] // DQK
    block_count = segment // BLOCK

    def split_heads(array, width):
        return array.reshape(block_count, BLOCK, head_count, width).transpose(0, 2, 1, 3)

    query_blocks = split_heads(queries, DQK)
    key_blocks = split_heads(keys, DQK)
    value_blocks = split_heads(values, DV)
    forget_log_value = jax.nn.log_sigmoid(forget_gate_logits) + extra_log_decay
    gate_blocks = input_gate_log.reshape(block_count, BLOCK, head_count).transpose(0, 2, 1)
    forget_blocks = forget_log_value.reshape(block_count, BLOCK, head_count).transpose(0, 2, 1)
    totals = jnp.sum(forget_log_value, axis=0)
    zero_matrix = jnp.zeros((head_count, DQK, DV), jnp.float32)
    zero_vector = jnp.zeros((head_count, DQK), jnp.float32)
    zero_heads = jnp.zeros((head_count,), jnp.float32)
    fresh = (zero_matrix, zero_vector, jnp.full((head_count,), very_low, jnp.float32))
    empty = (zero_heads,) + fresh
    anchor = (zero_heads, zero_matrix, zero_vector, zero_heads)

    def summarize(memory, inputs):
        key_blk, value_blk, gate_blk, forget_blk = inputs
        return (
            advance(memory, key_blk, value_blk, gate_blk, jnp.cumsum(forget_blk, axis=-1)),
            None,
        )

    own_state, unused = lax.scan(
        summarize, fresh, (key_blocks, value_blocks, gate_blocks, forget_blocks)
    )
    prefix = carried_in((totals,) + own_state, "sp", combine_states, empty)
    start_full = combine_states(anchor, prefix)

    def emit(memory, inputs):
        query_blk, key_blk, value_blk, gate_blk, forget_blk = inputs
        running, local_top, numerator, denominator = block_local(
            query_blk, key_blk, value_blk, gate_blk, forget_blk
        )
        outcome = read_out(query_blk, memory, running, local_top, numerator, denominator)
        return (advance(memory, key_blk, value_blk, gate_blk, running), outcome)

    unused, heads_out = lax.scan(
        emit, start_full[1:], (query_blocks, key_blocks, value_blocks, gate_blocks, forget_blocks)
    )
    cell_out = heads_out.transpose(0, 2, 1, 3).reshape(segment, head_count * DV)
    gated = (cell_out * jax.nn.sigmoid(output_gate_logits.astype(jnp.float32))).astype(jnp.bfloat16)
    whole_weight = lax.all_gather(cell_output_weight, "sp", axis=1, tiled=True)
    mixed = lax.psum_scatter(
        jnp.dot(gated, whole_weight, preferred_element_type=jnp.float32).astype(jnp.bfloat16),
        "tp",
        scatter_dimension=0,
        tiled=True,
    ).astype(jnp.float32)
    stream = (residual_input.astype(jnp.float32) + rms_scale(mixed, cell_norm_gain)).astype(
        jnp.bfloat16
    )
    normed = rms_scale(stream.astype(jnp.float32), expert_before_gain).astype(jnp.bfloat16)
    normed_all = lax.all_gather(normed, "tp", axis=0, tiled=True)
    sources = lax.axis_size("sp")
    top_count = routes.shape[1]
    capacity = max(2, min(segment, 5 * segment * top_count // (4 * sources)))
    width = normed_all.shape[1]
    labels = lax.broadcasted_iota(jnp.int32, (1, 1, sources), 2)
    matches = (routes[:, :, None] == labels).astype(jnp.int32)
    per_row = jnp.sum(matches, axis=1)
    before_rows = jnp.cumsum(per_row, axis=0) - per_row
    places = jnp.sum(matches * before_rows[:, None, :], axis=2)
    slot_of = routes * capacity + places
    slot_ids = lax.broadcasted_iota(jnp.int32, (sources * capacity, 1, 1), 0)
    picker = jnp.sum((slot_of[None, :, :] == slot_ids).astype(jnp.int32), axis=2).astype(
        jnp.bfloat16
    )
    buffer = jnp.dot(picker, normed_all, preferred_element_type=jnp.float32).astype(jnp.bfloat16)
    buffer = buffer.reshape(sources, capacity, width)
    arrived = lax.all_to_all(buffer, "sp", split_axis=0, concat_axis=0, tiled=True)
    flattened = arrived.reshape(-1, width)
    gate_proj = jnp.dot(flattened, expert_gate_weight[0], preferred_element_type=jnp.float32)
    up_proj = jnp.dot(flattened, expert_up_weight[0], preferred_element_type=jnp.float32)
    hidden = (jax.nn.silu(gate_proj) * up_proj).astype(jnp.bfloat16)
    hidden_whole = lax.all_gather(hidden, "tp", axis=1, tiled=True)
    expert_out = jnp.dot(
        hidden_whole, expert_down_weight[0], preferred_element_type=jnp.float32
    ).astype(jnp.bfloat16)
    results = expert_out.reshape(arrived.shape[0], arrived.shape[1], expert_out.shape[1])
    returned = lax.all_to_all(results, "sp", split_axis=0, concat_axis=0, tiled=True)
    flat = returned.reshape(sources * capacity, returned.shape[2])
    routed_part = jnp.zeros((segment, flat.shape[1]), jnp.float32)
    for route_idx in range(top_count):
        routed_part = (
            routed_part
            + flat[slot_of[:, route_idx]].astype(jnp.float32)
            * chosen_expert_weight[:, route_idx][:, None]
        )
    moe_columns = routed_part.astype(jnp.bfloat16)
    moe_rows = lax.all_to_all(moe_columns, "tp", split_axis=0, concat_axis=1, tiled=True)
    return (
        stream.astype(jnp.float32) + rms_scale(moe_rows.astype(jnp.float32), expert_after_gain)
    ).astype(jnp.bfloat16)


def swap(array, axis, bits):
    return lax.ppermute(array, axis, [(i, i ^ bits) for i in range(lax.axis_size(axis))])


def hop(array, chips, share, step):
    pairs = [
        (chip * share + core, (chip + step) % chips * share + core)
        for chip in range(chips)
        for core in range(share)
    ]
    return lax.ppermute(array, "sp", pairs)


def shift(array, chips, share, step):
    pairs = [
        (chip * share + core, (chip + step) * share + core)
        for chip in range(chips)
        for core in range(share)
        if 0 <= chip + step < chips
    ]
    return lax.ppermute(array, "sp", pairs)


def spread(array, chip, chips, share):
    if chips != 4:
        return [
            (hop(array, chips, share, step) if step else array, (chip - step) % chips)
            for step in range(chips)
        ]
    across = hop(array, chips, share, 2)
    upward = shift(array, chips, share, 1)
    downward = shift(array, chips, share, -1)
    pairs = [(at * share + core, to * share + core) for at, to in ((2, 3), (1, 0)) for core in range(share)]
    onward = lax.ppermute(across, "sp", pairs)
    last = chips - 1
    return [
        (array, chip),
        (upward, jnp.maximum(chip - 1, 0)),
        (downward, jnp.minimum(chip + 1, last)),
        (across, (chip + 2) % chips),
        (onward, jnp.where(chip == 0, last, 0)),
    ]


def contract(left, right, dims):
    return lax.dot_general(left, right, ((dims[:1], dims[1:]), ((), ())), preferred_element_type=jnp.float32)


def pack_kernel(
    spot_ref, query_ref, key_ref, value_ref, logit_ref, input_ref, forget_ref, decay_ref, routes_ref,
    weights_ref, *out_refs
):
    rows = query_ref.shape[0]
    chips = len(out_refs)
    wide = value_ref.shape[1] // (2 * chips)
    chip, core = spot_ref[0], spot_ref[1]

    def pieces_of(array):
        high = lax.reduce_precision(array, 8, 7)
        rest = array - high
        middle = lax.reduce_precision(rest, 8, 7)
        return [high, middle, rest - middle]

    logits = forget_ref[...]
    forget = jnp.minimum(logits, 0.0) - jnp.log1p(jnp.exp(-jnp.abs(logits))) + decay_ref[...]
    gates = pieces_of(forget) + pieces_of(input_ref[...])
    told = [routes_ref[...].astype(jnp.float32)] + pieces_of(weights_ref[...])
    heads = gates[0].shape[0]
    tops = told[0].shape[0]
    for step, out_ref in enumerate(out_refs):
        head = (chip + step) % chips
        query_at = pl.multiple_of(head * DQK, DQK)
        out_ref[:rows, 2 * wide : 2 * wide + DQK] = query_ref[:, pl.ds(query_at, DQK)]
        out_ref[:rows, 2 * wide + DQK : 2 * wide + 2 * DQK] = key_ref[:, pl.ds(query_at, DQK)]
        for turn in range(2):
            value_at = pl.multiple_of((2 * head + (core ^ turn)) * wide, wide)
            base = turn * (2 * wide + 2 * DQK)
            out_ref[:rows, base : base + wide] = value_ref[:, pl.ds(value_at, wide)]
            out_ref[:rows, base + wide : base + 2 * wide] = logit_ref[:, pl.ds(value_at, wide)]
        mine = lax.broadcasted_iota(jnp.int32, (heads, rows), 0) == head
        lines = [jnp.sum(jnp.where(mine, gate, 0.0), axis=0, keepdims=True) for gate in gates]
        lines = lines + [line[i : i + 1] for line in told for i in range(tops)]
        spare = jnp.zeros((1, rows), jnp.float32)
        slots = (out_ref.shape[1] - 2 * wide) // rows
        filled = lines[:6] + [spare] * (slots - 6) + lines[6:]
        filled = filled + [spare] * (8 * slots - len(filled))
        for slot in range(slots):
            column = jnp.concatenate([filled[r * slots + slot] for r in range(8)], axis=0)
            at = 2 * wide + slot * rows
            out_ref[rows:, at : at + rows] = column.astype(jnp.bfloat16)


def cell_kernel(short, spot_ref, *refs):
    chips = (len(refs) - 7) // 2
    even_ref, odd_ref, routes_ref, weights_ref, data_ref, forget_ref, gate_ref = refs[2 * chips :]
    count = 2 * chips
    wide = even_ref.shape[1]
    rows = 2 * even_ref.shape[0] // count
    tops = routes_ref.shape[1]
    chip, core = spot_ref[0], spot_ref[1]
    for step in range(chips):
        origin = (chip + chips - step) % chips
        mine_ref, other_ref = refs[step], refs[chips + step]
        for ref, base, values_at, spot in (
            (mine_ref, 2 * wide, 0, 2 * origin + core),
            (other_ref, 0, 2 * DQK, 2 * origin + 1 - core),
        ):
            data_ref[spot, :, : 2 * DQK] = ref[:rows, base : base + 2 * DQK]
            data_ref[spot, :, 2 * DQK :] = ref[:rows, values_at : values_at + 2 * wide]
            slots = 2 * (wide + DQK) // rows
            extra = ref[rows:, base : base + slots * rows].astype(jnp.float32)

            def line(index):
                r, slot = index // slots, index % slots
                return extra[r : r + 1, slot * rows : (slot + 1) * rows]

            forget_ref[pl.ds(spot, 1), :] = line(0) + line(1) + line(2)
            gate_ref[pl.ds(spot, 1), :] = line(3) + line(4) + line(5)
            for i in range(tops):
                routes_ref[spot, i : i + 1, :] = line(slots + i).astype(jnp.int32)
                weights_ref[spot, i : i + 1, :] = (
                    line(slots + tops + i) + line(slots + 2 * tops + i) + line(slots + 3 * tops + i)
                )
    square = (rows, rows)
    first = lax.broadcasted_iota(jnp.int32, square, 0)
    second = lax.broadcasted_iota(jnp.int32, square, 1)
    lower = first >= second
    running = jnp.dot(
        forget_ref[...],
        (first <= second).astype(jnp.float32),
        precision=lax.Precision.HIGHEST,
        preferred_element_type=jnp.float32,
    )
    base = jnp.zeros((1, 1), jnp.float32)
    top = jnp.zeros((1, 1), jnp.float32)
    levels, tops = [], []
    for j in range(count):
        level = gate_ref[j : j + 1, :] - (running[j : j + 1, :] + base)
        levels.append(level)
        tops.append(top)
        base = base + running[j : j + 1, rows - 1 : rows]
        top = jnp.maximum(top, jnp.max(level, axis=1, keepdims=True))
    for i in range(count):
        query = data_ref[i, :, :DQK]
        masked = jnp.where(lower, levels[i], very_low)
        peak = jnp.maximum(tops[i], jnp.max(masked, axis=1, keepdims=True))
        numer = jnp.zeros((rows, wide), jnp.float32)
        denom = jnp.zeros((rows, 1), jnp.float32)
        for j in range(i + 1):
            scores = contract(query, data_ref[j, :, DQK : 2 * DQK], (1, 1))
            level = masked if j == i else levels[j]
            weights = scores * DQK ** (-0.5) * jnp.exp(level - peak)
            denom = denom + jnp.sum(weights, axis=1, keepdims=True)
            numer = numer + contract(
                weights.astype(jnp.bfloat16), data_ref[j, :, 2 * DQK : 2 * DQK + wide], (1, 0)
            )
        logits = data_ref[i, :, 2 * DQK + wide :].astype(jnp.float32)
        outcome = numer / jnp.maximum(jnp.abs(denom), den_floor) / (1.0 + jnp.exp(-logits))
        outcome = outcome.astype(jnp.bfloat16)
        for j in range(rows // (2 * short)):
            to = (i * rows // 2) + j * short
            even_ref[to : to + short] = outcome[2 * j * short : (2 * j + 1) * short]
            odd_ref[to : to + short] = outcome[(2 * j + 1) * short : (2 * j + 2) * short]


def picker_of(routes, expert, capacity):
    length = routes.shape[1]
    hit = jnp.max((routes == expert).astype(jnp.float32), axis=0, keepdims=True)
    before = lax.broadcasted_iota(jnp.int32, (length, length), 0) < lax.broadcasted_iota(
        jnp.int32, (length, length), 1
    )
    rank = contract(
        jnp.broadcast_to(hit, (8, length)).astype(jnp.bfloat16), before.astype(jnp.bfloat16), (1, 0)
    )[:1]
    slots = lax.broadcasted_iota(jnp.int32, (capacity, length), 0).astype(jnp.float32)
    return jnp.where((rank == slots) & (hit > 0.0), 1.0, 0.0).astype(jnp.bfloat16)


def select_kernel(steps, chips, spot_ref, routes_ref, *refs):
    own_ref, other_ref = refs[-2:]
    pieces = refs[:-2]
    sides = len(pieces) // 2
    capacity = own_ref.shape[0] // 2
    length = routes_ref.shape[2]
    short, width = pieces[0].shape
    block = width // 8
    chip, core, side = spot_ref[0], spot_ref[1], spot_ref[2]
    expert = 2 * chip + core
    from_index = lax.broadcasted_iota(jnp.int32, (length, length), 0)
    to_index = lax.broadcasted_iota(jnp.int32, (length, length), 1)
    turned = from_index == ((to_index // short) ^ side) * short + to_index % short
    for part, step in enumerate(steps):
        routes = routes_ref[2 * ((chip + chips - step) % chips) + core]
        picker = jnp.concatenate(
            [picker_of(routes, expert ^ turn, capacity) for turn in range(2)], axis=0
        )
        picker = contract(picker, turned.astype(jnp.bfloat16), (1, 0)).astype(jnp.bfloat16)
        rows = slice(part * capacity, (part + 1) * capacity)
        for at in range(0, width, block):
            columns = slice(at, at + block)
            here = jnp.concatenate(
                [piece[:, columns] for piece in pieces[part * sides : (part + 1) * sides]]
            )
            picked = contract(picker, here, (1, 0)).astype(jnp.bfloat16)
            own_ref[rows, columns] = picked[:capacity]
            other_ref[rows, columns] = picked[capacity:]


def combine_kernel(steps, chips, spot_ref, routes_ref, weights_ref, own_ref, other_ref, *out_refs):
    chip, core = spot_ref[0], spot_ref[1]
    expert = 2 * chip + core
    capacity = other_ref.shape[0] // 2
    length = routes_ref.shape[2]
    first = lax.broadcasted_iota(jnp.int32, (length, length), 0)
    second = lax.broadcasted_iota(jnp.int32, (length, length), 1)
    same, before = first == second, second < first
    slots = lax.broadcasted_iota(jnp.int32, (length, capacity), 1).astype(jnp.float32)
    for part, (step, out_ref) in enumerate(zip(steps, out_refs)):
        at = 2 * ((chip + chips - step) % chips) + core
        routes = routes_ref[at]
        scales = weights_ref[at]
        total = jnp.zeros(out_ref.shape, jnp.float32)
        for rows_ref, wanted in ((own_ref, expert), (other_ref, expert ^ 1)):
            hit = jnp.max((routes == wanted).astype(jnp.float32), axis=0, keepdims=True)
            rank = jnp.sum(jnp.where(before, hit, 0.0), axis=1, keepdims=True)
            hit = jnp.sum(jnp.where(same, hit, 0.0), axis=1, keepdims=True)
            picker = jnp.where((rank == slots) & (hit > 0.0), 1.0, 0.0).astype(jnp.bfloat16)
            scale_row = jnp.sum(jnp.where(routes == wanted, scales, 0.0), axis=0, keepdims=True)
            scale = jnp.sum(jnp.where(same, scale_row, 0.0), axis=1, keepdims=True)
            spread_rows = contract(picker, rows_ref[part * capacity : (part + 1) * capacity, :], (1, 0))
            total = total + scale * spread_rows
        out_ref[...] = total.astype(jnp.bfloat16)


def norm_kernel(
    spot_ref, kept_a, got_a, kept_b, got_b, residual_ref, gain_ref, next_ref, stream_ref, normed_ref,
    mixed_ref
):
    chip, core = spot_ref[0], spot_ref[1]
    chips, short, block = kept_a.shape
    for at, kept, got in ((0, kept_a, got_a), (short, kept_b, got_b)):
        for step in range(chips):
            origin = 2 * ((chip + chips - step) % chips)
            for ref, index in ((kept, origin + core), (got, origin + 1 - core)):
                where = pl.ds(pl.multiple_of(index * block, block), block)
                mixed_ref[at : at + short, where] = ref[step].astype(jnp.float32)
    stream = residual_ref[...].astype(jnp.float32) + rms_scale(mixed_ref[...], gain_ref[...])
    stream = stream.astype(jnp.bfloat16)
    stream_ref[...] = stream
    normed_ref[...] = rms_scale(stream.astype(jnp.float32), next_ref[...]).astype(jnp.bfloat16)


def last_kernel(spot_ref, stream_ref, gain_ref, *refs):
    out_ref, rows_ref = refs[-2:]
    block = refs[0].shape[1]
    for bits, ref in enumerate(refs[:-2]):
        where = pl.ds(pl.multiple_of((spot_ref[2] ^ bits) * block, block), block)
        rows_ref[:, where] = ref[...].astype(jnp.float32)
    out = stream_ref[...].astype(jnp.float32) + rms_scale(rows_ref[...], gain_ref[...])
    out_ref[...] = out.astype(jnp.bfloat16)


def smem():
    return pl.BlockSpec(memory_space=pltpu.SMEM)


def vmem(count):
    return [pl.BlockSpec(memory_space=pltpu.VMEM)] * count


def by_heads(
    queries,
    keys,
    values,
    output_gate_logits,
    input_gate_log,
    forget_gate_logits,
    extra_log_decay,
    cell_output_weight,
    residual_input,
    cell_norm_gain,
    expert_before_gain,
    expert_after_gain,
    routes,
    chosen_expert_weight,
    expert_gate_weight,
    expert_up_weight,
    expert_down_weight,
):
    segment = queries.shape[0]
    sources = lax.axis_size("sp")
    sides = lax.axis_size("tp")
    place = lax.axis_index("sp")
    side = lax.axis_index("tp")
    head_count = queries.shape[1] // DQK
    share = sources // head_count
    chips = sources // share
    chip, core = place // share, place % share
    wide = DV // share
    top_count = routes.shape[1]
    capacity = max(2, min(segment, 5 * segment * top_count // (4 * sources)))
    spot = jnp.stack([chip, core, side]).astype(jnp.int32)
    line = 2 * DQK + 4 * wide
    packed = pl.pallas_call(
        pack_kernel,
        in_specs=[smem()] + vmem(9),
        out_specs=vmem(chips),
        out_shape=[jax.ShapeDtypeStruct((segment + 8, line), jnp.bfloat16)] * chips,
        name="pack",
    )(
        spot,
        queries,
        keys,
        values,
        output_gate_logits,
        input_gate_log.T,
        forget_gate_logits.T,
        extra_log_decay.T,
        routes.T,
        chosen_expert_weight.T,
    )
    mine = [hop(block, chips, share, step) if step else block for step, block in enumerate(packed)]
    other = [swap(block[:, 2 * wide :], "sp", 1) for block in mine]
    short = segment // (2 * sides)
    half_rows = jax.ShapeDtypeStruct((sources * segment // 2, wide), jnp.bfloat16)
    even, odd, all_routes, all_weights = pl.pallas_call(
        partial(cell_kernel, short),
        in_specs=[smem()] + vmem(2 * chips),
        out_specs=vmem(4),
        out_shape=[
            half_rows,
            half_rows,
            jax.ShapeDtypeStruct((sources, top_count, segment), jnp.int32),
            jax.ShapeDtypeStruct((sources, top_count, segment), jnp.float32),
        ],
        scratch_shapes=[
            pltpu.VMEM((sources, segment, 2 * DQK + 2 * wide), jnp.bfloat16),
            pltpu.VMEM((sources, segment), jnp.float32),
            pltpu.VMEM((sources, segment), jnp.float32),
        ],
        name="cell",
    )(spot, *mine, *other)

    def weight_rows(index):
        return lax.dynamic_slice_in_dim(cell_output_weight, index * wide, wide, 0)

    weights_at = {}

    def project(gated, before):
        total = None
        for order, (block, origin) in enumerate(spread(gated, chip, chips, share)):
            for turn, array in enumerate((block, swap(block, "sp", 1))):
                index = share * origin + (1 - core if turn else core)
                if (order, turn) not in weights_at:
                    weights_at[order, turn] = weight_rows(index)
                term = jnp.dot(array, weights_at[order, turn], preferred_element_type=jnp.float32)
                total = term if total is None else total + term
        total = total.astype(jnp.bfloat16).reshape(sources, sides, short, -1)
        if before is not None:
            total, before = lax.optimization_barrier((total, before))
        summed = None
        for bits in range(sides):
            piece = lax.dynamic_index_in_dim(total, side ^ bits, 1, False)
            piece = (swap(piece, "tp", bits) if bits else piece).astype(jnp.float32)
            summed = piece if summed is None else summed + piece
        summed = summed.astype(jnp.bfloat16).reshape(chips, share, short, -1)
        back = []
        for step in range(chips):
            block = lax.dynamic_index_in_dim(summed, (chip + step) % chips, 0, False)
            back.append(hop(block, chips, share, step) if step else block)
        back = jnp.stack(back)
        kept = lax.dynamic_index_in_dim(back, core, 1, False)
        return [kept, swap(lax.dynamic_index_in_dim(back, 1 - core, 1, False), "sp", 1)]

    own_shape = jax.ShapeDtypeStruct(residual_input.shape, jnp.bfloat16)
    parts_e = project(even, None)
    stream, normed = pl.pallas_call(
        norm_kernel,
        in_specs=[smem()] + vmem(7),
        out_specs=vmem(2),
        out_shape=[own_shape, own_shape],
        scratch_shapes=[pltpu.VMEM(residual_input.shape, jnp.float32)],
        name="norm",
    )(
        spot,
        *parts_e,
        *project(odd, parts_e[0]),
        residual_input,
        cell_norm_gain.reshape(1, -1),
        expert_before_gain.reshape(1, -1),
    )

    def down_rows(bits):
        width = expert_down_weight.shape[1] // sides
        return lax.dynamic_slice_in_dim(expert_down_weight[0], (side ^ bits) * width, width, 0)

    down_weights = lax.optimization_barrier([down_rows(bits) for bits in range(sides)])

    def around(array, first):
        pieces = [array]
        bits = first
        for _ in range(sides.bit_length() - 1):
            pieces = pieces + [swap(piece, "tp", bits) for piece in pieces]
            bits = bits * 2 if bits * 2 < sides else 1
        order = [0]
        bits = first
        for _ in range(sides.bit_length() - 1):
            order = order + [place ^ bits for place in order]
            bits = bits * 2 if bits * 2 < sides else 1
        return [pieces[order.index(place)] for place in range(sides)]

    sequence = list(range(1, chips, 2)) + list(range(0, chips, 2))
    steps_of = [tuple(sequence[at : at + 2]) for at in range(0, chips, 2)]
    arrived = {0: normed}
    gathered = {}
    for order, step in enumerate([0] + [step for step in sequence if step]):
        if step:
            arrived[step] = hop(normed, chips, share, step)
        gathered[step] = around(arrived[step], sides // 2 if order % 2 else 1)
    spread_pieces = [[piece for step in steps for piece in gathered[step]] for steps in steps_of]
    width = normed.shape[1]
    hidden_parts = []
    earlier = None
    for steps, pieces in zip(steps_of, spread_pieces):
        if earlier is not None:
            earlier, pieces = lax.optimization_barrier((earlier, pieces))
        own_rows, other_rows = pl.pallas_call(
            partial(select_kernel, steps, chips),
            in_specs=[smem()] + vmem(1 + len(pieces)),
            out_specs=vmem(2),
            out_shape=[jax.ShapeDtypeStruct((2 * capacity, width), jnp.bfloat16)] * 2,
        )(spot, all_routes, *pieces)
        picked = swap(other_rows, "sp", 1)
        rows_in = jnp.concatenate([own_rows, picked], axis=0)
        gate_proj = jnp.dot(rows_in, expert_gate_weight[0], preferred_element_type=jnp.float32)
        up_proj = jnp.dot(rows_in, expert_up_weight[0], preferred_element_type=jnp.float32)
        earlier = (jax.nn.silu(gate_proj) * up_proj).astype(jnp.bfloat16)
        hidden_parts.append(earlier)
    returned = None
    for order, (steps, hidden) in enumerate(zip(steps_of, hidden_parts)):
        expert_out = None
        if order + 1 == len(steps_of) and sides == 4:
            far = swap(hidden, "tp", 3)
            spread_hidden = [hidden, swap(hidden, "tp", 1), swap(hidden, "tp", 2), far]
        else:
            spread_hidden = around(hidden, sides // 2 if order % 2 else 1)
        for bits, piece in enumerate(spread_hidden):
            term = jnp.dot(piece, down_weights[bits], preferred_element_type=jnp.float32)
            expert_out = term if expert_out is None else expert_out + term
        expert_out = expert_out.astype(jnp.bfloat16)
        other_out = swap(expert_out[2 * capacity :], "sp", 1)
        summed = pl.pallas_call(
            partial(combine_kernel, steps, chips),
            in_specs=[smem()] + vmem(4),
            out_specs=vmem(2),
            out_shape=[jax.ShapeDtypeStruct((segment, expert_out.shape[1]), jnp.bfloat16)] * 2,
        )(spot, all_routes, all_weights, expert_out, other_out)
        for array, step in zip(summed, steps):
            back = (hop(array, chips, share, -step) if step else array).astype(jnp.float32)
            returned = back if returned is None else returned + back
    returned = returned.astype(jnp.bfloat16).reshape(sides, 2 * short, -1)
    parts = []
    for bits in range(sides):
        piece = lax.dynamic_index_in_dim(returned, side ^ bits, 0, False)
        parts.append(swap(piece, "tp", bits) if bits else piece)
    return pl.pallas_call(
        last_kernel,
        in_specs=[smem()] + vmem(2 + sides),
        out_specs=vmem(1)[0],
        out_shape=own_shape,
        scratch_shapes=[pltpu.VMEM(residual_input.shape, jnp.float32)],
        name="last",
    )(spot, stream, expert_after_gain.reshape(1, -1), *parts)


def per_device(*arrays):
    queries = arrays[0]
    sources, sides = lax.axis_size("sp"), lax.axis_size("tp")
    head_count = queries.shape[1] // DQK
    pairs = sources == 2 * head_count and head_count % 2 == 0
    powers = sides & (sides - 1) == 0
    if pairs and powers and queries.shape[0] == BLOCK and queries.shape[0] % (32 * sides) == 0:
        return by_heads(*arrays)
    return by_states(*arrays)


def solution(mesh):
    placed = (
        P("sp", "tp"),
        P("sp", "tp"),
        P("sp", "tp"),
        P("sp", "tp"),
        P("sp", "tp"),
        P("sp", "tp"),
        P("sp", "tp"),
        P("tp", "sp"),
        P(("sp", "tp"), None),
        P(),
        P(),
        P(),
        P("sp", None),
        P("sp", None),
        P("sp", None, "tp"),
        P("sp", None, "tp"),
        P("sp", None, "tp"),
    )
    return jax.shard_map(
        per_device, mesh=mesh, in_specs=placed, out_specs=P(("sp", "tp"), None), check_vma=False
    )
```

```python
import jax
import jax.numpy as jnp
from functools import partial
from jax import lax
from jax.experimental import pallas as pl
from jax.experimental.pallas import tpu as pltpu
from jax.sharding import PartitionSpec as P

DQK = 256
DV = 512
BLOCK = 128


norm_eps = 1e-06
very_low = -1e30
den_floor = 8.0


def carried_in(part, axis, combine, identity):
    place = lax.axis_index(axis)
    gathered = jax.tree.map(lambda a: lax.all_gather(a, axis), part)
    state = jax.tree.map(lambda a, e: jnp.zeros_like(a) + jnp.asarray(e, a.dtype), part, identity)

    def one(step, state):
        return combine(
            state, jax.tree.map(lambda a: lax.dynamic_index_in_dim(a, step, 0, False), gathered)
        )

    return lax.fori_loop(0, place, one, state)


def rms_scale(inputs, gain):
    return inputs * lax.rsqrt(jnp.mean(inputs * inputs, axis=-1, keepdims=True) + norm_eps) * gain


def combine_states(earlier, later):
    total_early, matrix_early, vector_early, peak_early = earlier
    total_late, matrix_late, vector_late, peak_late = later
    shifted = total_late + peak_early
    peak = jnp.maximum(shifted, peak_late)
    keep_early = jnp.exp(shifted - peak)
    keep_late = jnp.exp(peak_late - peak)
    return (
        total_early + total_late,
        keep_early[:, None, None] * matrix_early + keep_late[:, None, None] * matrix_late,
        keep_early[:, None] * vector_early + keep_late[:, None] * vector_late,
        peak,
    )


def block_local(query_blk, key_blk, value_blk, gate_blk, forget_blk):
    key_scale = DQK ** (-0.5)
    running = jnp.cumsum(forget_blk, axis=-1)
    length = running.shape[-1]
    lower = lax.broadcasted_iota(jnp.int32, (length, length), 0) >= lax.broadcasted_iota(
        jnp.int32, (length, length), 1
    )
    offsets = jnp.where(
        lower, running[:, :, None] - running[:, None, :] + gate_blk[:, None, :], -jnp.inf
    )
    local_top = jnp.max(offsets, axis=-1)
    scores = (
        jnp.einsum("htd,hsd->hts", query_blk, key_blk, preferred_element_type=jnp.float32)
        * key_scale
    )
    weights = scores * jnp.exp(offsets - local_top[:, :, None])
    numerator = jnp.einsum(
        "hts,hsv->htv", weights.astype(jnp.bfloat16), value_blk, preferred_element_type=jnp.float32
    )
    denominator = jnp.sum(weights, axis=-1)
    return (running, local_top, numerator, denominator)


def read_out(query_blk, memory, running, local_top, numerator, denominator):
    matrix, vector, peak = memory
    query_wide = query_blk.astype(jnp.float32)
    carried = running + peak[:, None]
    highest = jnp.maximum(local_top, carried)
    inner_w = jnp.exp(local_top - highest)
    carried_w = jnp.exp(carried - highest)
    numer_all = inner_w[:, :, None] * numerator + carried_w[:, :, None] * jnp.einsum(
        "htd,hdv->htv", query_wide, matrix, precision=lax.Precision.HIGHEST
    )
    denom_all = inner_w * denominator + carried_w * jnp.einsum(
        "htd,hd->ht", query_wide, vector, precision=lax.Precision.HIGHEST
    )
    return numer_all / jnp.maximum(jnp.abs(denom_all), den_floor)[:, :, None]


def advance(memory, key_blk, value_blk, gate_blk, running):
    matrix, vector, peak = memory
    key_wide = key_blk.astype(jnp.float32) * DQK ** (-0.5)
    block_sum = running[:, -1]
    growth = block_sum[:, None] - running + gate_blk
    peak_new = jnp.maximum(block_sum + peak, jnp.max(growth, axis=-1))
    fading = jnp.exp(block_sum + peak - peak_new)
    writes = jnp.exp(growth - peak_new[:, None])
    weighted = (key_wide * writes[:, :, None]).astype(jnp.bfloat16)
    matrix_new = fading[:, None, None] * matrix + jnp.einsum(
        "hsd,hsv->hdv", weighted, value_blk, preferred_element_type=jnp.float32
    )
    vector_new = fading[:, None] * vector + jnp.einsum(
        "hs,hsd->hd", writes, key_wide, precision=lax.Precision.HIGHEST
    )
    return (matrix_new, vector_new, peak_new)


def by_states(
    queries,
    keys,
    values,
    output_gate_logits,
    input_gate_log,
    forget_gate_logits,
    extra_log_decay,
    cell_output_weight,
    residual_input,
    cell_norm_gain,
    expert_before_gain,
    expert_after_gain,
    routes,
    chosen_expert_weight,
    expert_gate_weight,
    expert_up_weight,
    expert_down_weight,
):
    segment = queries.shape[0]
    head_count = queries.shape[1] // DQK
    block_count = segment // BLOCK

    def split_heads(array, width):
        return array.reshape(block_count, BLOCK, head_count, width).transpose(0, 2, 1, 3)

    query_blocks = split_heads(queries, DQK)
    key_blocks = split_heads(keys, DQK)
    value_blocks = split_heads(values, DV)
    forget_log_value = jax.nn.log_sigmoid(forget_gate_logits) + extra_log_decay
    gate_blocks = input_gate_log.reshape(block_count, BLOCK, head_count).transpose(0, 2, 1)
    forget_blocks = forget_log_value.reshape(block_count, BLOCK, head_count).transpose(0, 2, 1)
    totals = jnp.sum(forget_log_value, axis=0)
    zero_matrix = jnp.zeros((head_count, DQK, DV), jnp.float32)
    zero_vector = jnp.zeros((head_count, DQK), jnp.float32)
    zero_heads = jnp.zeros((head_count,), jnp.float32)
    fresh = (zero_matrix, zero_vector, jnp.full((head_count,), very_low, jnp.float32))
    empty = (zero_heads,) + fresh
    anchor = (zero_heads, zero_matrix, zero_vector, zero_heads)

    def summarize(memory, inputs):
        key_blk, value_blk, gate_blk, forget_blk = inputs
        return (
            advance(memory, key_blk, value_blk, gate_blk, jnp.cumsum(forget_blk, axis=-1)),
            None,
        )

    own_state, unused = lax.scan(
        summarize, fresh, (key_blocks, value_blocks, gate_blocks, forget_blocks)
    )
    prefix = carried_in((totals,) + own_state, "sp", combine_states, empty)
    start_full = combine_states(anchor, prefix)

    def emit(memory, inputs):
        query_blk, key_blk, value_blk, gate_blk, forget_blk = inputs
        running, local_top, numerator, denominator = block_local(
            query_blk, key_blk, value_blk, gate_blk, forget_blk
        )
        outcome = read_out(query_blk, memory, running, local_top, numerator, denominator)
        return (advance(memory, key_blk, value_blk, gate_blk, running), outcome)

    unused, heads_out = lax.scan(
        emit, start_full[1:], (query_blocks, key_blocks, value_blocks, gate_blocks, forget_blocks)
    )
    cell_out = heads_out.transpose(0, 2, 1, 3).reshape(segment, head_count * DV)
    gated = (cell_out * jax.nn.sigmoid(output_gate_logits.astype(jnp.float32))).astype(jnp.bfloat16)
    whole_weight = lax.all_gather(cell_output_weight, "sp", axis=1, tiled=True)
    mixed = lax.psum_scatter(
        jnp.dot(gated, whole_weight, preferred_element_type=jnp.float32).astype(jnp.bfloat16),
        "tp",
        scatter_dimension=0,
        tiled=True,
    ).astype(jnp.float32)
    stream = (residual_input.astype(jnp.float32) + rms_scale(mixed, cell_norm_gain)).astype(
        jnp.bfloat16
    )
    normed = rms_scale(stream.astype(jnp.float32), expert_before_gain).astype(jnp.bfloat16)
    normed_all = lax.all_gather(normed, "tp", axis=0, tiled=True)
    sources = lax.axis_size("sp")
    top_count = routes.shape[1]
    capacity = max(2, min(segment, 5 * segment * top_count // (4 * sources)))
    width = normed_all.shape[1]
    labels = lax.broadcasted_iota(jnp.int32, (1, 1, sources), 2)
    matches = (routes[:, :, None] == labels).astype(jnp.int32)
    per_row = jnp.sum(matches, axis=1)
    before_rows = jnp.cumsum(per_row, axis=0) - per_row
    places = jnp.sum(matches * before_rows[:, None, :], axis=2)
    slot_of = routes * capacity + places
    slot_ids = lax.broadcasted_iota(jnp.int32, (sources * capacity, 1, 1), 0)
    picker = jnp.sum((slot_of[None, :, :] == slot_ids).astype(jnp.int32), axis=2).astype(
        jnp.bfloat16
    )
    buffer = jnp.dot(picker, normed_all, preferred_element_type=jnp.float32).astype(jnp.bfloat16)
    buffer = buffer.reshape(sources, capacity, width)
    arrived = lax.all_to_all(buffer, "sp", split_axis=0, concat_axis=0, tiled=True)
    flattened = arrived.reshape(-1, width)
    gate_proj = jnp.dot(flattened, expert_gate_weight[0], preferred_element_type=jnp.float32)
    up_proj = jnp.dot(flattened, expert_up_weight[0], preferred_element_type=jnp.float32)
    hidden = (jax.nn.silu(gate_proj) * up_proj).astype(jnp.bfloat16)
    hidden_whole = lax.all_gather(hidden, "tp", axis=1, tiled=True)
    expert_out = jnp.dot(
        hidden_whole, expert_down_weight[0], preferred_element_type=jnp.float32
    ).astype(jnp.bfloat16)
    results = expert_out.reshape(arrived.shape[0], arrived.shape[1], expert_out.shape[1])
    returned = lax.all_to_all(results, "sp", split_axis=0, concat_axis=0, tiled=True)
    flat = returned.reshape(sources * capacity, returned.shape[2])
    routed_part = jnp.zeros((segment, flat.shape[1]), jnp.float32)
    for route_idx in range(top_count):
        routed_part = (
            routed_part
            + flat[slot_of[:, route_idx]].astype(jnp.float32)
            * chosen_expert_weight[:, route_idx][:, None]
        )
    moe_columns = routed_part.astype(jnp.bfloat16)
    moe_rows = lax.all_to_all(moe_columns, "tp", split_axis=0, concat_axis=1, tiled=True)
    return (
        stream.astype(jnp.float32) + rms_scale(moe_rows.astype(jnp.float32), expert_after_gain)
    ).astype(jnp.bfloat16)


def swap(array, axis, bits):
    return lax.ppermute(array, axis, [(i, i ^ bits) for i in range(lax.axis_size(axis))])


def hop(array, chips, share, step):
    pairs = [
        (chip * share + core, (chip + step) % chips * share + core)
        for chip in range(chips)
        for core in range(share)
    ]
    return lax.ppermute(array, "sp", pairs)


def shift(array, chips, share, step):
    pairs = [
        (chip * share + core, (chip + step) * share + core)
        for chip in range(chips)
        for core in range(share)
        if 0 <= chip + step < chips
    ]
    return lax.ppermute(array, "sp", pairs)


def spread(array, chip, chips, share):
    if chips != 4:
        return [
            (hop(array, chips, share, step) if step else array, (chip - step) % chips)
            for step in range(chips)
        ]
    across = hop(array, chips, share, 2)
    upward = shift(array, chips, share, 1)
    downward = shift(array, chips, share, -1)
    pairs = [(at * share + core, to * share + core) for at, to in ((2, 3), (1, 0)) for core in range(share)]
    onward = lax.ppermute(across, "sp", pairs)
    last = chips - 1
    return [
        (array, chip),
        (upward, jnp.maximum(chip - 1, 0)),
        (downward, jnp.minimum(chip + 1, last)),
        (across, (chip + 2) % chips),
        (onward, jnp.where(chip == 0, last, 0)),
    ]


def contract(left, right, dims):
    return lax.dot_general(left, right, ((dims[:1], dims[1:]), ((), ())), preferred_element_type=jnp.float32)


def pack_kernel(
    spot_ref, query_ref, key_ref, value_ref, logit_ref, input_ref, forget_ref, decay_ref, routes_ref,
    weights_ref, *out_refs
):
    rows = query_ref.shape[0]
    chips = len(out_refs)
    wide = value_ref.shape[1] // (2 * chips)
    chip, core = spot_ref[0], spot_ref[1]

    def pieces_of(array):
        high = lax.reduce_precision(array, 8, 7)
        rest = array - high
        middle = lax.reduce_precision(rest, 8, 7)
        return [high, middle, rest - middle]

    logits = forget_ref[...]
    forget = jnp.minimum(logits, 0.0) - jnp.log1p(jnp.exp(-jnp.abs(logits))) + decay_ref[...]
    gates = pieces_of(forget) + pieces_of(input_ref[...])
    told = [routes_ref[...].astype(jnp.float32)] + pieces_of(weights_ref[...])
    heads = gates[0].shape[0]
    tops = told[0].shape[0]
    for step, out_ref in enumerate(out_refs):
        head = (chip + step) % chips
        query_at = pl.multiple_of(head * DQK, DQK)
        out_ref[:rows, 2 * wide : 2 * wide + DQK] = query_ref[:, pl.ds(query_at, DQK)]
        out_ref[:rows, 2 * wide + DQK : 2 * wide + 2 * DQK] = key_ref[:, pl.ds(query_at, DQK)]
        for turn in range(2):
            value_at = pl.multiple_of((2 * head + (core ^ turn)) * wide, wide)
            base = turn * (2 * wide + 2 * DQK)
            out_ref[:rows, base : base + wide] = value_ref[:, pl.ds(value_at, wide)]
            out_ref[:rows, base + wide : base + 2 * wide] = logit_ref[:, pl.ds(value_at, wide)]
        mine = lax.broadcasted_iota(jnp.int32, (heads, rows), 0) == head
        lines = [jnp.sum(jnp.where(mine, gate, 0.0), axis=0, keepdims=True) for gate in gates]
        lines = lines + [line[i : i + 1] for line in told for i in range(tops)]
        spare = jnp.zeros((1, rows), jnp.float32)
        slots = (out_ref.shape[1] - 2 * wide) // rows
        filled = lines[:6] + [spare] * (slots - 6) + lines[6:]
        filled = filled + [spare] * (8 * slots - len(filled))
        for slot in range(slots):
            column = jnp.concatenate([filled[r * slots + slot] for r in range(8)], axis=0)
            at = 2 * wide + slot * rows
            out_ref[rows:, at : at + rows] = column.astype(jnp.bfloat16)


def cell_kernel(short, spot_ref, *refs):
    chips = (len(refs) - 7) // 2
    even_ref, odd_ref, routes_ref, weights_ref, data_ref, forget_ref, gate_ref = refs[2 * chips :]
    count = 2 * chips
    wide = even_ref.shape[1]
    rows = 2 * even_ref.shape[0] // count
    tops = routes_ref.shape[1]
    chip, core = spot_ref[0], spot_ref[1]
    for step in range(chips):
        origin = (chip + chips - step) % chips
        mine_ref, other_ref = refs[step], refs[chips + step]
        for ref, base, values_at, spot in (
            (mine_ref, 2 * wide, 0, 2 * origin + core),
            (other_ref, 0, 2 * DQK, 2 * origin + 1 - core),
        ):
            data_ref[spot, :, : 2 * DQK] = ref[:rows, base : base + 2 * DQK]
            data_ref[spot, :, 2 * DQK :] = ref[:rows, values_at : values_at + 2 * wide]
            slots = 2 * (wide + DQK) // rows
            extra = ref[rows:, base : base + slots * rows].astype(jnp.float32)

            def line(index):
                r, slot = index // slots, index % slots
                return extra[r : r + 1, slot * rows : (slot + 1) * rows]

            forget_ref[pl.ds(spot, 1), :] = line(0) + line(1) + line(2)
            gate_ref[pl.ds(spot, 1), :] = line(3) + line(4) + line(5)
            for i in range(tops):
                routes_ref[spot, i : i + 1, :] = line(slots + i).astype(jnp.int32)
                weights_ref[spot, i : i + 1, :] = (
                    line(slots + tops + i) + line(slots + 2 * tops + i) + line(slots + 3 * tops + i)
                )
    square = (rows, rows)
    first = lax.broadcasted_iota(jnp.int32, square, 0)
    second = lax.broadcasted_iota(jnp.int32, square, 1)
    lower = first >= second
    running = jnp.dot(
        forget_ref[...],
        (first <= second).astype(jnp.float32),
        precision=lax.Precision.HIGHEST,
        preferred_element_type=jnp.float32,
    )
    base = jnp.zeros((1, 1), jnp.float32)
    top = jnp.zeros((1, 1), jnp.float32)
    levels, tops = [], []
    for j in range(count):
        level = gate_ref[j : j + 1, :] - (running[j : j + 1, :] + base)
        levels.append(level)
        tops.append(top)
        base = base + running[j : j + 1, rows - 1 : rows]
        top = jnp.maximum(top, jnp.max(level, axis=1, keepdims=True))
    for i in range(count):
        query = data_ref[i, :, :DQK]
        masked = jnp.where(lower, levels[i], very_low)
        peak = jnp.maximum(tops[i], jnp.max(masked, axis=1, keepdims=True))
        numer = jnp.zeros((rows, wide), jnp.float32)
        denom = jnp.zeros((rows, 1), jnp.float32)
        for j in range(i + 1):
            scores = contract(query, data_ref[j, :, DQK : 2 * DQK], (1, 1))
            level = masked if j == i else levels[j]
            weights = scores * DQK ** (-0.5) * jnp.exp(level - peak)
            denom = denom + jnp.sum(weights, axis=1, keepdims=True)
            numer = numer + contract(
                weights.astype(jnp.bfloat16), data_ref[j, :, 2 * DQK : 2 * DQK + wide], (1, 0)
            )
        logits = data_ref[i, :, 2 * DQK + wide :].astype(jnp.float32)
        outcome = numer / jnp.maximum(jnp.abs(denom), den_floor) / (1.0 + jnp.exp(-logits))
        outcome = outcome.astype(jnp.bfloat16)
        for j in range(rows // (2 * short)):
            to = (i * rows // 2) + j * short
            even_ref[to : to + short] = outcome[2 * j * short : (2 * j + 1) * short]
            odd_ref[to : to + short] = outcome[(2 * j + 1) * short : (2 * j + 2) * short]


def picker_of(routes, expert, capacity):
    length = routes.shape[1]
    hit = jnp.max((routes == expert).astype(jnp.float32), axis=0, keepdims=True)
    before = lax.broadcasted_iota(jnp.int32, (length, length), 0) < lax.broadcasted_iota(
        jnp.int32, (length, length), 1
    )
    rank = contract(
        jnp.broadcast_to(hit, (8, length)).astype(jnp.bfloat16), before.astype(jnp.bfloat16), (1, 0)
    )[:1]
    slots = lax.broadcasted_iota(jnp.int32, (capacity, length), 0).astype(jnp.float32)
    return jnp.where((rank == slots) & (hit > 0.0), 1.0, 0.0).astype(jnp.bfloat16)


def select_kernel(steps, chips, spot_ref, routes_ref, *refs):
    own_ref, other_ref = refs[-2:]
    pieces = refs[:-2]
    sides = len(pieces) // 2
    capacity = own_ref.shape[0] // 2
    length = routes_ref.shape[2]
    short, width = pieces[0].shape
    block = width // 8
    chip, core, side = spot_ref[0], spot_ref[1], spot_ref[2]
    expert = 2 * chip + core
    from_index = lax.broadcasted_iota(jnp.int32, (length, length), 0)
    to_index = lax.broadcasted_iota(jnp.int32, (length, length), 1)
    turned = from_index == ((to_index // short) ^ side) * short + to_index % short
    for part, step in enumerate(steps):
        routes = routes_ref[2 * ((chip + chips - step) % chips) + core]
        picker = jnp.concatenate(
            [picker_of(routes, expert ^ turn, capacity) for turn in range(2)], axis=0
        )
        picker = contract(picker, turned.astype(jnp.bfloat16), (1, 0)).astype(jnp.bfloat16)
        rows = slice(part * capacity, (part + 1) * capacity)
        for at in range(0, width, block):
            columns = slice(at, at + block)
            here = jnp.concatenate(
                [piece[:, columns] for piece in pieces[part * sides : (part + 1) * sides]]
            )
            picked = contract(picker, here, (1, 0)).astype(jnp.bfloat16)
            own_ref[rows, columns] = picked[:capacity]
            other_ref[rows, columns] = picked[capacity:]


def combine_kernel(steps, chips, spot_ref, routes_ref, weights_ref, own_ref, other_ref, *out_refs):
    chip, core = spot_ref[0], spot_ref[1]
    expert = 2 * chip + core
    capacity = other_ref.shape[0] // 2
    length = routes_ref.shape[2]
    first = lax.broadcasted_iota(jnp.int32, (length, length), 0)
    second = lax.broadcasted_iota(jnp.int32, (length, length), 1)
    same, before = first == second, second < first
    slots = lax.broadcasted_iota(jnp.int32, (length, capacity), 1).astype(jnp.float32)
    for part, (step, out_ref) in enumerate(zip(steps, out_refs)):
        at = 2 * ((chip + chips - step) % chips) + core
        routes = routes_ref[at]
        scales = weights_ref[at]
        total = jnp.zeros(out_ref.shape, jnp.float32)
        for rows_ref, wanted in ((own_ref, expert), (other_ref, expert ^ 1)):
            hit = jnp.max((routes == wanted).astype(jnp.float32), axis=0, keepdims=True)
            rank = jnp.sum(jnp.where(before, hit, 0.0), axis=1, keepdims=True)
            hit = jnp.sum(jnp.where(same, hit, 0.0), axis=1, keepdims=True)
            picker = jnp.where((rank == slots) & (hit > 0.0), 1.0, 0.0).astype(jnp.bfloat16)
            scale_row = jnp.sum(jnp.where(routes == wanted, scales, 0.0), axis=0, keepdims=True)
            scale = jnp.sum(jnp.where(same, scale_row, 0.0), axis=1, keepdims=True)
            spread_rows = contract(picker, rows_ref[part * capacity : (part + 1) * capacity, :], (1, 0))
            total = total + scale * spread_rows
        out_ref[...] = total.astype(jnp.bfloat16)


def norm_kernel(
    spot_ref, kept_a, got_a, kept_b, got_b, residual_ref, gain_ref, next_ref, stream_ref, normed_ref,
    mixed_ref
):
    chip, core = spot_ref[0], spot_ref[1]
    chips, short, block = kept_a.shape
    for at, kept, got in ((0, kept_a, got_a), (short, kept_b, got_b)):
        for step in range(chips):
            origin = 2 * ((chip + chips - step) % chips)
            for ref, index in ((kept, origin + core), (got, origin + 1 - core)):
                where = pl.ds(pl.multiple_of(index * block, block), block)
                mixed_ref[at : at + short, where] = ref[step].astype(jnp.float32)
    stream = residual_ref[...].astype(jnp.float32) + rms_scale(mixed_ref[...], gain_ref[...])
    stream = stream.astype(jnp.bfloat16)
    stream_ref[...] = stream
    normed_ref[...] = rms_scale(stream.astype(jnp.float32), next_ref[...]).astype(jnp.bfloat16)


def last_kernel(spot_ref, stream_ref, gain_ref, *refs):
    out_ref, rows_ref = refs[-2:]
    block = refs[0].shape[1]
    for bits, ref in enumerate(refs[:-2]):
        where = pl.ds(pl.multiple_of((spot_ref[2] ^ bits) * block, block), block)
        rows_ref[:, where] = ref[...].astype(jnp.float32)
    out = stream_ref[...].astype(jnp.float32) + rms_scale(rows_ref[...], gain_ref[...])
    out_ref[...] = out.astype(jnp.bfloat16)


def smem():
    return pl.BlockSpec(memory_space=pltpu.SMEM)


def vmem(count):
    return [pl.BlockSpec(memory_space=pltpu.VMEM)] * count


def by_heads(
    queries,
    keys,
    values,
    output_gate_logits,
    input_gate_log,
    forget_gate_logits,
    extra_log_decay,
    cell_output_weight,
    residual_input,
    cell_norm_gain,
    expert_before_gain,
    expert_after_gain,
    routes,
    chosen_expert_weight,
    expert_gate_weight,
    expert_up_weight,
    expert_down_weight,
):
    segment = queries.shape[0]
    sources = lax.axis_size("sp")
    sides = lax.axis_size("tp")
    place = lax.axis_index("sp")
    side = lax.axis_index("tp")
    head_count = queries.shape[1] // DQK
    share = sources // head_count
    chips = sources // share
    chip, core = place // share, place % share
    wide = DV // share
    top_count = routes.shape[1]
    capacity = max(2, min(segment, 5 * segment * top_count // (4 * sources)))
    spot = jnp.stack([chip, core, side]).astype(jnp.int32)
    line = 2 * DQK + 4 * wide
    packed = pl.pallas_call(
        pack_kernel,
        in_specs=[smem()] + vmem(9),
        out_specs=vmem(chips),
        out_shape=[jax.ShapeDtypeStruct((segment + 8, line), jnp.bfloat16)] * chips,
        name="pack",
    )(
        spot,
        queries,
        keys,
        values,
        output_gate_logits,
        input_gate_log.T,
        forget_gate_logits.T,
        extra_log_decay.T,
        routes.T,
        chosen_expert_weight.T,
    )
    mine = [hop(block, chips, share, step) if step else block for step, block in enumerate(packed)]
    other = [swap(block[:, 2 * wide :], "sp", 1) for block in mine]
    short = segment // (2 * sides)
    half_rows = jax.ShapeDtypeStruct((sources * segment // 2, wide), jnp.bfloat16)
    even, odd, all_routes, all_weights = pl.pallas_call(
        partial(cell_kernel, short),
        in_specs=[smem()] + vmem(2 * chips),
        out_specs=vmem(4),
        out_shape=[
            half_rows,
            half_rows,
            jax.ShapeDtypeStruct((sources, top_count, segment), jnp.int32),
            jax.ShapeDtypeStruct((sources, top_count, segment), jnp.float32),
        ],
        scratch_shapes=[
            pltpu.VMEM((sources, segment, 2 * DQK + 2 * wide), jnp.bfloat16),
            pltpu.VMEM((sources, segment), jnp.float32),
            pltpu.VMEM((sources, segment), jnp.float32),
        ],
        name="cell",
    )(spot, *mine, *other)

    def weight_rows(index):
        return lax.dynamic_slice_in_dim(cell_output_weight, index * wide, wide, 0)

    weights_at = {}

    def project(gated, before):
        total = None
        for order, (block, origin) in enumerate(spread(gated, chip, chips, share)):
            for turn, array in enumerate((block, swap(block, "sp", 1))):
                index = share * origin + (1 - core if turn else core)
                if (order, turn) not in weights_at:
                    weights_at[order, turn] = weight_rows(index)
                term = jnp.dot(array, weights_at[order, turn], preferred_element_type=jnp.float32)
                total = term if total is None else total + term
        total = total.astype(jnp.bfloat16).reshape(sources, sides, short, -1)
        if before is not None:
            total, before = lax.optimization_barrier((total, before))
        summed = None
        for bits in range(sides):
            piece = lax.dynamic_index_in_dim(total, side ^ bits, 1, False)
            piece = (swap(piece, "tp", bits) if bits else piece).astype(jnp.float32)
            summed = piece if summed is None else summed + piece
        summed = summed.astype(jnp.bfloat16).reshape(chips, share, short, -1)
        back = []
        for step in range(chips):
            block = lax.dynamic_index_in_dim(summed, (chip + step) % chips, 0, False)
            back.append(hop(block, chips, share, step) if step else block)
        back = jnp.stack(back)
        kept = lax.dynamic_index_in_dim(back, core, 1, False)
        return [
            kept,
            swap(lax.dynamic_index_in_dim(back, 1 - core, 1, False), "sp", 1),
            summed,
        ]

    own_shape = jax.ShapeDtypeStruct(residual_input.shape, jnp.bfloat16)
    parts_e = project(even, None)
    parts_o = project(odd, parts_e[2])
    stream, normed = pl.pallas_call(
        norm_kernel,
        in_specs=[smem()] + vmem(7),
        out_specs=vmem(2),
        out_shape=[own_shape, own_shape],
        scratch_shapes=[pltpu.VMEM(residual_input.shape, jnp.float32)],
        name="norm",
    )(
        spot,
        *parts_e[:2],
        *parts_o[:2],
        residual_input,
        cell_norm_gain.reshape(1, -1),
        expert_before_gain.reshape(1, -1),
    )

    def down_rows(bits):
        width = expert_down_weight.shape[1] // sides
        return lax.dynamic_slice_in_dim(expert_down_weight[0], (side ^ bits) * width, width, 0)

    down_weights = lax.optimization_barrier([down_rows(bits) for bits in range(sides)])

    def around(array, first):
        pieces = [array]
        bits = first
        for _ in range(sides.bit_length() - 1):
            pieces = pieces + [swap(piece, "tp", bits) for piece in pieces]
            bits = bits * 2 if bits * 2 < sides else 1
        order = [0]
        bits = first
        for _ in range(sides.bit_length() - 1):
            order = order + [place ^ bits for place in order]
            bits = bits * 2 if bits * 2 < sides else 1
        return [pieces[order.index(place)] for place in range(sides)]

    sequence = list(range(1, chips, 2)) + list(range(0, chips, 2))
    steps_of = [tuple(sequence[at : at + 2]) for at in range(0, chips, 2)]
    arrived = {0: normed}
    gathered = {}
    for order, step in enumerate([0] + [step for step in sequence if step]):
        if step:
            arrived[step] = hop(normed, chips, share, step)
        gathered[step] = around(arrived[step], sides // 2 if order % 2 else 1)
    spread_pieces = [[piece for step in steps for piece in gathered[step]] for steps in steps_of]
    width = normed.shape[1]
    hidden_parts = []
    earlier = None
    for steps, pieces in zip(steps_of, spread_pieces):
        if earlier is not None:
            earlier, pieces = lax.optimization_barrier((earlier, pieces))
        own_rows, other_rows = pl.pallas_call(
            partial(select_kernel, steps, chips),
            in_specs=[smem()] + vmem(1 + len(pieces)),
            out_specs=vmem(2),
            out_shape=[jax.ShapeDtypeStruct((2 * capacity, width), jnp.bfloat16)] * 2,
        )(spot, all_routes, *pieces)
        picked = swap(other_rows, "sp", 1)
        rows_in = jnp.concatenate([own_rows, picked], axis=0)
        gate_proj = jnp.dot(rows_in, expert_gate_weight[0], preferred_element_type=jnp.float32)
        up_proj = jnp.dot(rows_in, expert_up_weight[0], preferred_element_type=jnp.float32)
        earlier = (jax.nn.silu(gate_proj) * up_proj).astype(jnp.bfloat16)
        hidden_parts.append(earlier)
    returned = None
    for order, (steps, hidden) in enumerate(zip(steps_of, hidden_parts)):
        expert_out = None
        if order + 1 == len(steps_of) and sides == 4:
            far = swap(hidden, "tp", 3)
            spread_hidden = [hidden, swap(hidden, "tp", 1), swap(hidden, "tp", 2), far]
        else:
            spread_hidden = around(hidden, sides // 2 if order % 2 else 1)
        for bits, piece in enumerate(spread_hidden):
            term = jnp.dot(piece, down_weights[bits], preferred_element_type=jnp.float32)
            expert_out = term if expert_out is None else expert_out + term
        expert_out = expert_out.astype(jnp.bfloat16)
        other_out = swap(expert_out[2 * capacity :], "sp", 1)
        summed = pl.pallas_call(
            partial(combine_kernel, steps, chips),
            in_specs=[smem()] + vmem(4),
            out_specs=vmem(2),
            out_shape=[jax.ShapeDtypeStruct((segment, expert_out.shape[1]), jnp.bfloat16)] * 2,
        )(spot, all_routes, all_weights, expert_out, other_out)
        for array, step in zip(summed, steps):
            back = (hop(array, chips, share, -step) if step else array).astype(jnp.float32)
            returned = back if returned is None else returned + back
    returned = returned.astype(jnp.bfloat16).reshape(sides, 2 * short, -1)
    parts = []
    for bits in range(sides):
        piece = lax.dynamic_index_in_dim(returned, side ^ bits, 0, False)
        parts.append(swap(piece, "tp", bits) if bits else piece)
    return pl.pallas_call(
        last_kernel,
        in_specs=[smem()] + vmem(2 + sides),
        out_specs=vmem(1)[0],
        out_shape=own_shape,
        scratch_shapes=[pltpu.VMEM(residual_input.shape, jnp.float32)],
        name="last",
    )(spot, stream, expert_after_gain.reshape(1, -1), *parts)


def per_device(*arrays):
    queries = arrays[0]
    sources, sides = lax.axis_size("sp"), lax.axis_size("tp")
    head_count = queries.shape[1] // DQK
    pairs = sources == 2 * head_count and head_count % 2 == 0
    powers = sides & (sides - 1) == 0
    if pairs and powers and queries.shape[0] == BLOCK and queries.shape[0] % (32 * sides) == 0:
        return by_heads(*arrays)
    return by_states(*arrays)


def solution(mesh):
    placed = (
        P("sp", "tp"),
        P("sp", "tp"),
        P("sp", "tp"),
        P("sp", "tp"),
        P("sp", "tp"),
        P("sp", "tp"),
        P("sp", "tp"),
        P("tp", "sp"),
        P(("sp", "tp"), None),
        P(),
        P(),
        P(),
        P("sp", None),
        P("sp", None),
        P("sp", None, "tp"),
        P("sp", None, "tp"),
        P("sp", None, "tp"),
    )
    return jax.shard_map(
        per_device, mesh=mesh, in_specs=placed, out_specs=P(("sp", "tp"), None), check_vma=False
    )
```
